128 devices in a mesh: sp: 16 (over z, y), tp: 8 (over x, core).
Axes of the slice: x: 4, y: 4, z: 4, core: 2. Of those that a mesh axis runs over, the one named last changes fastest.
Arguments:
- tokens: bfloat16 [4, 8192, 1024], P(None, ('sp', 'tp')), may hold values from -6 to 6
- norm_gain: float32 [1024], replicated, may hold values from 0.1 to 1.9
- x_weight: bfloat16 [1024, 1024], P('sp', 'tp'), may hold values from -0.1875 to 0.1875
- z_weight: bfloat16 [1024, 1024], P('sp', 'tp'), may hold values from -0.1875 to 0.1875
- b_weight: bfloat16 [1024, 1024], P('sp', 'tp'), may hold values from -0.1875 to 0.1875
- c_weight: bfloat16 [1024, 1024], P('sp', 'tp'), may hold values from -0.1875 to 0.1875
- dt_weight: bfloat16 [1024, 16], P('sp', 'tp'), may hold values from -0.1875 to 0.1875
- x_conv: float32 [4, 1024], P(None, 'tp'), may hold values from -3 to 3
- b_conv: float32 [4, 1024], P(None, 'tp'), may hold values from -3 to 3
- c_conv: float32 [4, 1024], P(None, 'tp'), may hold values from -3 to 3
- dt_bias: float32 [16], P('tp'), may hold values from -1 to 1
- decay_rate: float32 [16], P('tp'), may hold values from 0.15 to 3.5
- out_gain: float32 [1024], P('tp'), may hold values from 0.1 to 1.9
- out_weight: bfloat16 [1024, 1024], P('tp', 'sp'), may hold values from -0.1875 to 0.1875
Outputs:
- mixed: bfloat16 [4, 8192, 1024], P(None, ('sp', 'tp'))
The draws below stay inside these ranges and needn't reach their ends.
All inputs are finite; a program needn't handle non-finite values.
Results may differ from the reference program's by a relative error of at most 0.02.
Values may be sent and summed in bfloat16 or wider, within the bound.
No kernel may reach another device: no remote copies, remote signals or barrier semaphores. Data moves between devices by JAX's collectives and lax.ppermute only.
A program may use at most 64 MiB of HBM per device.

```python
import math
import jax
import jax.numpy as jnp
from jax import lax

D = 1024
HEADS = 16
HEAD_P = 64
STATE = 128
GROUPS = 8
CONV = 4
BLOCK = 32
SEQS = 4
INNER = 1024
LENGTH = 8192


def shard_levels(own_key, shape, split, low, largest):
    def one(dim, shards_of):
        heights = jax.random.uniform(jax.random.fold_in(jax.random.fold_in(own_key, 6), dim), (shards_of,), jnp.float32, low / len(split), largest / len(split))
        return jnp.repeat(jnp.exp(heights), shape[dim] // shards_of).reshape((-1,) + (1,) * (len(shape) - dim - 1))

    gain = one(*split[0])
    for cut in split[1:]:
        gain = gain * one(*cut)
    return gain


def centred(rng, dims, deviation, most, split=(), kind=jnp.bfloat16):
    array = jax.random.normal(rng, dims, jnp.float32) * deviation
    if len(split) > 0:
        array = shard_levels(rng, dims, split, -0.22, 0.18) * array
    return jnp.clip(array, min=-most, max=most).astype(kind)


def setup_inputs(seed: int = 0) -> dict:
    arg_keys = jax.random.split(jax.random.key(seed), 15)
    tokens = centred(arg_keys[0], (SEQS, LENGTH, D), 1.0, 6.0, ((1, 128),))
    norm_gain = jnp.clip(1.0 + 0.18 * jax.random.normal(arg_keys[1], (D,), jnp.float32), 0.1, 1.9)
    x_weight = centred(arg_keys[2], (D, INNER), D ** -0.5, 0.1875, ((0, 16), (1, 8)))
    z_weight = centred(arg_keys[3], (D, INNER), D ** -0.5, 0.1875, ((0, 16), (1, 8)))
    b_weight = centred(arg_keys[4], (D, GROUPS * STATE), D ** -0.5, 0.1875, ((0, 16), (1, 8)))
    c_weight = centred(arg_keys[5], (D, GROUPS * STATE), D ** -0.5, 0.1875, ((0, 16), (1, 8)))
    dt_weight = centred(arg_keys[6], (D, HEADS), D ** -0.5, 0.1875, ((0, 16), (1, 8)))
    x_conv = centred(arg_keys[7], (CONV, INNER), CONV ** -0.5, 3.0, ((1, 8),), jnp.float32)
    b_conv = centred(arg_keys[8], (CONV, GROUPS * STATE), CONV ** -0.5, 3.0, ((1, 8),), jnp.float32)
    c_conv = centred(arg_keys[9], (CONV, GROUPS * STATE), CONV ** -0.5, 3.0, ((1, 8),), jnp.float32)
    dt_bias = jnp.clip(jax.random.uniform(arg_keys[10], (HEADS,), jnp.float32, -1.0, 1.0) * shard_levels(arg_keys[10], (HEADS,), ((0, 8),), -0.4, 0.0), -1.0, 1.0)
    decay_rate = jnp.clip(jnp.exp(math.log(3.5) - 3.149883 * jax.random.uniform(arg_keys[11], (HEADS,), jnp.float32) ** shard_levels(arg_keys[11], (HEADS,), ((0, 8),), -0.2, 0.2)), 0.15, 3.5)
    out_gain = jnp.clip(1.0 + 0.18 * jax.random.normal(arg_keys[12], (INNER,), jnp.float32), 0.1, 1.9)
    out_weight = centred(arg_keys[13], (INNER, D), INNER ** -0.5, 0.1875, ((0, 8), (1, 16)))
    return dict(tokens=tokens, norm_gain=norm_gain, x_weight=x_weight, z_weight=z_weight, b_weight=b_weight, c_weight=c_weight, dt_weight=dt_weight, x_conv=x_conv, b_conv=b_conv, c_conv=c_conv, dt_bias=dt_bias, decay_rate=decay_rate, out_gain=out_gain, out_weight=out_weight)


epsilon = 1e-05
precise = lax.Precision.HIGHEST

def short_conv(projected, taps):
    tap_count = taps.shape[0]
    source = projected.astype(jnp.float32)
    padded = jnp.pad(source, ((0, 0), (tap_count - 1, 0), (0, 0)))
    span_len = source.shape[1]
    running = jnp.zeros_like(source)
    for offset in range(tap_count):
        running = running + taps[offset] * padded[:, offset:offset + span_len]
    return jax.nn.silu(running)

def block_pass(inputs_dt, logdecay, b_state, c_state, per_group):
    seq_count, span_len, head_count, head_width = inputs_dt.shape
    groups, state_width = (b_state.shape[2], b_state.shape[3])
    blocks = span_len // BLOCK
    x_blocks = inputs_dt.reshape(seq_count, blocks, BLOCK, groups, per_group, head_width)
    b_blocks = b_state.reshape(seq_count, blocks, BLOCK, groups, state_width)
    c_blocks = c_state.reshape(seq_count, blocks, BLOCK, groups, state_width)
    log_blocks = logdecay.reshape(seq_count, blocks, BLOCK, groups, per_group)
    within = jnp.moveaxis(jnp.cumsum(log_blocks, axis=2), 2, -1)
    scores = jnp.einsum('sclgn,scmgn->scglm', c_blocks, b_blocks, precision=precise)
    lower_mask = jnp.tril(jnp.ones((BLOCK, BLOCK), dtype=bool))
    log_gaps = jnp.where(lower_mask, within[..., :, None] - within[..., None, :], -jnp.inf)
    weights = scores[:, :, :, None] * jnp.exp(log_gaps)
    diagonal_part = jnp.einsum('scghlm,scmghp->sclghp', weights, x_blocks, precision=precise)
    end_decay = jnp.moveaxis(jnp.exp(within[..., -1:] - within), -1, 2)
    block_states = jnp.einsum('sclgn,sclghp->scghpn', b_blocks, x_blocks * end_decay[..., None], precision=precise)
    block_decay = jnp.exp(within[..., -1])

    def advance(running_state, inputs):
        fresh_state, shrink = inputs
        return (running_state * shrink[..., None, None] + fresh_state, running_state)
    start_state = jnp.zeros((seq_count, groups, per_group, head_width, state_width), jnp.float32)
    final_state, entering = lax.scan(advance, start_state, (jnp.moveaxis(block_states, 1, 0), jnp.moveaxis(block_decay, 1, 0)))
    entering = jnp.moveaxis(entering, 0, 1)
    start_decay = jnp.moveaxis(jnp.exp(within), -1, 2)
    carried_part = jnp.einsum('sclgn,scghpn->sclghp', c_blocks, entering, precision=precise) * start_decay[..., None]
    return ((diagonal_part + carried_part).reshape(seq_count, span_len, head_count, head_width), final_state)

def reference(tokens, norm_gain, x_weight, z_weight, b_weight, c_weight, dt_weight, x_conv, b_conv, c_conv, dt_bias, decay_rate, out_gain, out_weight):
    source = tokens.astype(jnp.float32)
    normed = (source * lax.rsqrt(lax.optimization_barrier(jnp.mean(source * source, axis=-1, keepdims=True)) + epsilon) * norm_gain).astype(jnp.bfloat16)
    flattened = normed.reshape(SEQS * LENGTH, D)

    def project(weight):
        product = jnp.dot(flattened, weight, preferred_element_type=jnp.float32)
        return product.astype(jnp.bfloat16).reshape(SEQS, LENGTH, weight.shape[1])
    x_conv_out = short_conv(project(x_weight), x_conv).reshape(SEQS, LENGTH, HEADS, HEAD_P)
    b_state = short_conv(project(b_weight), b_conv).reshape(SEQS, LENGTH, GROUPS, STATE)
    c_state = short_conv(project(c_weight), c_conv).reshape(SEQS, LENGTH, GROUPS, STATE)
    z_proj = project(z_weight)
    step_dt = jax.nn.softplus(project(dt_weight).astype(jnp.float32) + dt_bias)
    logdecay = -(step_dt * decay_rate) / LENGTH
    y_all, final_state = block_pass(x_conv_out * step_dt[..., None], logdecay, b_state, c_state, HEADS // GROUPS)
    gate_act = jax.nn.silu(z_proj.astype(jnp.float32))
    gated = (y_all.reshape(SEQS, LENGTH, INNER) * gate_act).reshape(SEQS, LENGTH, GROUPS, INNER // GROUPS)
    gated = gated * lax.rsqrt(lax.optimization_barrier(jnp.mean(gated * gated, axis=-1, keepdims=True)) + epsilon)
    gated = (gated.reshape(SEQS, LENGTH, INNER) * out_gain).astype(jnp.bfloat16)
    mixed = jnp.dot(gated.reshape(SEQS * LENGTH, INNER), out_weight, preferred_element_type=jnp.float32)
    return mixed.astype(jnp.bfloat16).reshape(SEQS, LENGTH, D)
```

```python
import functools

import jax
import jax.numpy as jnp
from jax import lax
from jax.experimental import pallas as pl
from jax.experimental.pallas import tpu as pltpu
from jax.sharding import Mesh
from jax.sharding import PartitionSpec as P


LENGTH = 8192
SEQS = 4
SPAN = 512
PIECE = 64
T = 64
HALO = 16
EPS = 1e-05
AXES = ("z", "y", "x", "c")
SP = ("z", "y")
TP = ("x", "c")
bf16 = jnp.bfloat16
f32 = jnp.float32
VM = pl.BlockSpec(memory_space=pltpu.VMEM)
SM = pl.BlockSpec(memory_space=pltpu.SMEM)
PARAMS = pltpu.CompilerParams(vmem_limit_bytes=56 * 1024 * 1024)


def call(body, outs, ins, scratch=(), flops=0):
    return pl.pallas_call(
        body,
        out_shape=outs,
        in_specs=[SM] + [VM] * (len(ins) - 1),
        out_specs=jax.tree.map(lambda _: VM, outs),
        scratch_shapes=list(scratch),
        compiler_params=PARAMS,
        cost_estimate=pl.CostEstimate(flops=flops, bytes_accessed=1 << 20, transcendentals=0),
    )(*ins)


def shift(value, axis, d):
    n = lax.axis_size(axis)
    return lax.ppermute(value, axis, [(i, (i + d) % n) for i in range(n)])


def onward(value, axis, d):
    n = lax.axis_size(axis)
    return lax.ppermute(value, axis, [(i, i + d) for i in range(n - d)])


def silu(v):
    return v / (1.0 + jnp.exp(-v))


def dot(a, b, dims=((1,), (0,))):
    return lax.dot_general(a, b, (dims, ((), ())), preferred_element_type=f32)


def order_in(idx, b0, b1, b2, b3, out):
    z, y = idx[0], idx[1]
    for dz, b in enumerate((b0, b1, b2, b3)):
        for dy in range(4):
            at = lax.rem(z - dz + 4, 4) * 4 + lax.rem(y - dy + 4, 4)
            out[pl.ds(pl.multiple_of(at * 64, 64), 64), :] = b[dy * 64 : dy * 64 + 64, :]


def project_tail(idx, *refs):
    pieces, w, out, rows = refs[:14], refs[14], refs[15], refs[16]
    x, c = idx[2], idx[3]
    away = lax.rem(x - 3 + 4, 4)
    own, other = pieces[:7], pieces[7:]
    for of_c, group in ((1, own), (0, other)):
        for d in range(4):

            @pl.when(jnp.logical_and(c == of_c, away == d))
            def _(group=group, d=d):
                if d == 0:
                    rows[...] = group[0][:, PIECE - HALO :, :]
                else:
                    first, second = {1: (1, 2), 3: (3, 4), 2: (5, 6)}[d]
                    rows[0:2] = group[first][:, PIECE - HALO :, :]
                    rows[2:4] = group[second][:, PIECE - HALO :, :]

    v = rows[...].reshape(SEQS * HALO, 1024)
    vf = v.astype(f32)
    r = lax.rsqrt(jnp.mean(vf * vf, axis=1, keepdims=True) + EPS)
    out[...] = (dot(v, w[:, 0:384]) * r).astype(bf16).reshape(SEQS, HALO, 384)


def softplus(v):
    return jnp.maximum(v, 0.0) + jnp.log1p(jnp.exp(-jnp.abs(v)))


def span_state(idx, *refs):
    pieces, (w, halo, taps, dtb, rate) = refs[:14], refs[14:19]
    pack, u_out, b_out, l_out, c_raw, z_raw, rows, scale, ext = refs[19:]
    x, c = idx[2], idx[3]
    for swapped in range(2):
        group = pieces[7 * swapped : 7 * swapped + 7]
        for d in range(4):
            half = lax.rem(c + swapped, 2)
            at = pl.multiple_of((lax.rem(x - d + 4, 4) * 2 + half) * PIECE, PIECE)
            if d == 0:
                parts = ((0, 4, group[0]),)
            else:
                first, second = {1: (1, 2), 3: (3, 4), 2: (5, 6)}[d]
                parts = ((0, 2, group[first]), (2, 4, group[second]))
            for lo, hi, ref in parts:
                for s in range(lo, hi):
                    v = ref[s - lo]
                    vf = v.astype(f32)
                    r = lax.rsqrt(jnp.mean(vf * vf, axis=1, keepdims=True) + EPS)
                    rows[s, pl.ds(at, PIECE), :] = v
                    scale[s, pl.ds(at, PIECE), :] = jnp.broadcast_to(r, (PIECE, 128))
    row = lax.broadcasted_iota(jnp.int32, (T, 2 * T), 0)
    col = lax.broadcasted_iota(jnp.int32, (T, 2 * T), 1)
    tri = (lax.rem(col, T) <= row).astype(bf16)
    for s in range(SEQS):
        prod = dot(rows[s], w[...])
        r = scale[s]
        for k in range(2):
            ext[HALO:, k * 128 : k * 128 + 128] = prod[:, k * 128 : k * 128 + 128] * r
        c_raw[s] = (prod[:, 256:384] * r).astype(bf16)
        z_raw[s] = (prod[:, 384:512] * r).astype(bf16)
        ext[0:HALO, :] = halo[s, :, 0:256].astype(f32)
        dt = softplus(prod[:, 512:640] * r + dtb[...])
        ld = -(dt * rate[...]) / LENGTH
        hi = ld.astype(bf16)
        lo = (ld - hi.astype(f32)).astype(bf16)
        total = jnp.zeros((1, 128), f32)
        for k in range(SPAN // T):
            at = slice(k * T, k * T + T)
            both = jnp.concatenate([hi[at], lo[at]], axis=0)
            lc = dot(tri, both) + total
            l_out[s, at, :] = lc
            total = lc[T - 1 : T, :]
        conv = jnp.zeros((SPAN, 256), f32)
        for k in range(4):
            conv = conv + taps[k : k + 1, 0:256] * ext[HALO - 3 + k : HALO - 3 + k + SPAN, :]
        conv = silu(conv)
        u = conv[:, 0:128] * dt
        b = conv[:, 128:256].astype(bf16)
        u_out[s] = u.astype(bf16)
        b_out[s] = b
        late = (u * jnp.exp(total - l_out[s])).astype(bf16)
        pack[s, 0:128, :] = dot(b, late, ((0,), (0,))).astype(bf16)
        t_hi = total.astype(bf16)
        t_lo = (total - t_hi.astype(f32)).astype(bf16)
        which = lax.broadcasted_iota(jnp.int32, (16, 128), 0)
        both = jnp.where(which == 0, t_hi.astype(f32), jnp.where(which == 1, t_lo.astype(f32), 0.0))
        pack[s, 128:144, :] = both.astype(bf16)


def span_own(idx, u, b, l, c_raw, z_raw, halo, taps, y_out, c_out, z_out, ext):
    row = lax.broadcasted_iota(jnp.int32, (T, 128), 0)
    col = lax.rem(lax.broadcasted_iota(jnp.int32, (T, 128), 1), T)
    seen = col <= row
    up = (row <= col).astype(f32)
    left = lax.broadcasted_iota(jnp.int32, (T, 128), 1) < T
    for s in range(SEQS):
        ext[0:HALO, :] = halo[s, :, 256:384].astype(f32)
        ext[HALO:, :] = c_raw[s].astype(f32)
        conv = jnp.zeros((SPAN, 128), f32)
        for k in range(4):
            conv = conv + taps[k : k + 1, 256:384] * ext[HALO - 3 + k : HALO - 3 + k + SPAN, :]
        c_out[s] = silu(conv).astype(bf16)
        z_out[s] = silu(z_raw[s].astype(f32)).astype(bf16)
        state = jnp.zeros((128, 128), f32)
        start = jnp.zeros((1, 128), f32)
        for k in range(SPAN // T):
            at = slice(k * T, k * T + T)
            lc = l[s, at, :]
            uc = u[s, at, :]
            bc = b[s, at, :]
            cc = c_out[s, at, :]
            step = lc - jnp.concatenate([start, lc[0 : T - 1, :]], axis=0)
            l_row = start + jnp.sum(step * up, axis=0, keepdims=True)
            pairs = dot(cc, jnp.concatenate([bc, bc], axis=0), ((1,), (1,)))
            gap = jnp.exp(jnp.where(seen, lc - l_row, -jnp.inf))
            m = (pairs * gap).astype(bf16)
            zero = jnp.zeros_like(uc)
            blocks = jnp.concatenate(
                [jnp.where(left, uc, zero), jnp.where(left, zero, uc)], axis=0
            )
            y = dot(m, blocks)
            if k > 0:
                y = y + dot(cc, state.astype(bf16)) * jnp.exp(lc - start)
            y_out[s, at, :] = y
            end = lc[T - 1 : T, :]
            if k + 1 < SPAN // T:
                late = (uc.astype(f32) * jnp.exp(end - lc)).astype(bf16)
                state = state * jnp.exp(end - start) + dot(bc, late, ((0,), (0,)))
            start = end


def combine_y(idx, p0, p1, p2, p3, whole, before, l_before):
    y = idx[1]
    packs = (p0, p1, p2, p3)
    at = [lax.rem(y - d + 4, 4) for d in range(4)]
    for s in range(SEQS):
        logs = [p[s, 128:129, :].astype(f32) + p[s, 129:130, :].astype(f32) for p in packs]
        zero = jnp.zeros_like(logs[0])
        total = logs[0] + logs[1] + logs[2] + logs[3]
        early = zero
        for d in range(1, 4):
            early = early + jnp.where(at[d] < y, logs[d], zero)
        all_sum = jnp.zeros((128, 128), f32)
        early_sum = jnp.zeros((128, 128), f32)
        for d in range(4):
            after = zero
            after_here = zero
            for e in range(4):
                if e != d:
                    after = after + jnp.where(at[e] > at[d], logs[e], zero)
                    between = jnp.logical_and(at[e] > at[d], at[e] < y)
                    after_here = after_here + jnp.where(between, logs[e], zero)
            v = packs[d][s, 0:128, :].astype(f32)
            all_sum = all_sum + v * jnp.exp(after)
            if d > 0:
                early_sum = early_sum + v * jnp.where(at[d] < y, jnp.exp(after_here), zero)
        whole[s, 0:128, :] = all_sum.astype(bf16)
        before[s] = early_sum
        l_before[s] = jnp.broadcast_to(early, (8, 128))
        t_hi = total.astype(bf16)
        t_lo = (total - t_hi.astype(f32)).astype(bf16)
        which = lax.broadcasted_iota(jnp.int32, (16, 128), 0)
        both = jnp.where(which == 0, t_hi.astype(f32), jnp.where(which == 1, t_lo.astype(f32), 0.0))
        whole[s, 128:144, :] = both.astype(bf16)


def finish(idx, p1, p2, p3, before, l_before, y_own, cc, zs, l, gain, out):
    for s in range(SEQS):
        logs = [p[s, 128:129, :].astype(f32) + p[s, 129:130, :].astype(f32) for p in (p1, p2, p3)]
        state = p1[s, 0:128, :].astype(f32)
        state = state + p2[s, 0:128, :].astype(f32) * jnp.exp(logs[0])
        state = state + p3[s, 0:128, :].astype(f32) * jnp.exp(logs[0] + logs[1])
        state = state * jnp.exp(l_before[s, 0:1, :]) + before[s]
        y = y_own[s] + dot(cc[s], state.astype(bf16)) * jnp.exp(l[s])
        g = y * zs[s].astype(f32)
        g = g * lax.rsqrt(jnp.mean(g * g, axis=1, keepdims=True) + EPS) * gain[...]
        g = g.astype(bf16)
        for k in range(SPAN // PIECE):
            out[k, s] = g[k * PIECE : k * PIECE + PIECE, :]


def order_out(idx, b0, b1, b2, b3, out):
    order_in(idx, b0, b1, b2, b3, out)


def project_out(idx, g, *refs):
    w, out = refs[:10], refs[10]
    x, c = idx[2], idx[3]
    acc = None
    for swapped in range(2):
        own, left, right, far_a, far_b = w[5 * swapped : 5 * swapped + 5]
        half = lax.rem(c + swapped, 2)
        for d, parts in ((0, (own,)), (1, (left,)), (3, (right,)), (2, (far_a, far_b))):
            v = g[lax.rem(x - d + 4, 4) * 2 + half]
            weight = jnp.concatenate([p[...] for p in parts], axis=0)
            part = dot(v, weight, ((1,), (1,)))
            acc = part if acc is None else acc + part
    out[...] = acc.astype(bf16)


def struct(shape, kind=bf16):
    return jax.ShapeDtypeStruct(shape, kind)


def local(
    tokens,
    norm_gain,
    x_weight,
    z_weight,
    b_weight,
    c_weight,
    dt_weight,
    x_conv,
    b_conv,
    c_conv,
    dt_bias,
    decay_rate,
    out_gain,
    out_weight,
):
    idx = jnp.stack([lax.axis_index(a) for a in AXES]).astype(jnp.int32)
    sp = lax.axis_index(SP)
    first, second = tokens[0:2], tokens[2:4]
    left_a = shift(first, "x", 1)
    right_b = shift(second, "x", -1)
    left_b = shift(second, "x", 1)
    right_a = shift(first, "x", -1)
    far_a = shift(left_a, "x", 1)
    far_b = shift(right_b, "x", -1)
    here = (tokens, left_a, left_b, right_a, right_b, far_a, far_b)
    pieces = here + tuple(shift(v, "c", 1) for v in here)

    gain = lax.dynamic_slice_in_dim(norm_gain, sp * 64, 64)[:, None]
    wide_dt = jnp.repeat(dt_weight, 64, axis=1)
    w_own = jnp.concatenate([x_weight, b_weight, c_weight, z_weight, wide_dt], axis=1)
    w_own = (w_own.astype(f32) * gain).astype(bf16)
    w_y = jnp.concatenate([w_own] + [shift(w_own, "y", d) for d in (1, 2, 3)], axis=0)
    w_parts = [w_y] + [shift(w_y, "z", d) for d in (1, 2, 3)]
    w_in = call(order_in, struct((1024, 640)), [idx, *w_parts])

    o_own = out_weight.T
    o_y = jnp.concatenate([o_own] + [shift(o_own, "y", d) for d in (1, 2, 3)], axis=0)
    o_parts = [o_y] + [shift(o_y, "z", d) for d in (1, 2, 3)]
    o_here = call(order_out, struct((1024, 128)), [idx, *o_parts])
    o_left = shift(o_here, "x", 1)
    o_right = shift(o_here, "x", -1)
    o_far_a = shift(o_left[:512], "x", 1)
    o_far_b = shift(o_right[512:], "x", -1)
    outs = (o_here, o_left, o_right, o_far_a, o_far_b)
    outs = outs + tuple(shift(v, "c", 1) for v in outs)

    taps = jnp.concatenate([x_conv, b_conv, c_conv], axis=1)
    dtb = jnp.repeat(dt_bias, 64)[None]
    rate = jnp.repeat(decay_rate, 64)[None]

    tail = call(
        project_tail,
        struct((SEQS, HALO, 384)),
        [idx, *pieces, w_in],
        [pltpu.VMEM((SEQS, HALO, 1024), bf16)],
    )
    halo = lax.ppermute(tail, SP, [(i, i + 1) for i in range(15)])
    pack_s = struct((SEQS, 144, 128))
    rows_s = struct((SEQS, SPAN, 128))
    wide_s = struct((SEQS, SPAN, 128), f32)
    pack, u, b, l, c_raw, z_raw = call(
        span_state,
        (pack_s, rows_s, rows_s, wide_s, rows_s, rows_s),
        [idx, *pieces, w_in, halo, taps, dtb, rate],
        [
            pltpu.VMEM((SEQS, SPAN, 1024), bf16),
            pltpu.VMEM((SEQS, SPAN, 128), f32),
            pltpu.VMEM((HALO + SPAN, 256), f32),
        ],
    )
    packs = [pack] + [shift(pack, "y", d) for d in (1, 2, 3)]
    y_own, cc, zs = call(
        span_own,
        (wide_s, rows_s, rows_s),
        [idx, u, b, l, c_raw, z_raw, halo, taps],
        [pltpu.VMEM((HALO + SPAN, 128), f32)],
        flops=1 << 32,
    )
    whole, before, l_before = call(
        combine_y,
        (pack_s, struct((SEQS, 128, 128), f32), struct((SEQS, 8, 128), f32)),
        [idx, *packs],
    )
    earlier = [onward(whole, "z", d) for d in (1, 2, 3)]
    gated = call(
        finish,
        struct((8, SEQS, PIECE, 128)),
        [idx, *earlier, before, l_before, y_own, cc, zs, l, out_gain[None]],
    )
    swapped = lax.all_to_all(gated, TP, 0, 0, tiled=True).reshape(8, 256, 128)
    out = call(project_out, struct((256, 1024)), [idx, swapped, *outs])
    return out.reshape(SEQS, PIECE, 1024)


def solution(mesh):
    torus = Mesh(mesh.devices.reshape(4, 4, 4, 2), AXES)
    return jax.shard_map(
        local,
        mesh=torus,
        in_specs=(
            P(None, AXES, None),
            P(),
            P(SP, TP),
            P(SP, TP),
            P(SP, TP),
            P(SP, TP),
            P(SP, TP),
            P(None, TP),
            P(None, TP),
            P(None, TP),
            P(TP),
            P(TP),
            P(TP),
            P(TP, SP),
        ),
        out_specs=P(None, AXES, None),
        check_vma=False,
    )
```

```python
import jax
import jax.numpy as jnp
from jax import lax
from jax.experimental import pallas as pl
from jax.experimental.pallas import tpu as pltpu
from jax.sharding import Mesh
from jax.sharding import PartitionSpec as P


LENGTH = 8192
SEQS = 2
SPAN = 1024
PIECE = 64
PIECES = 16
SPANS = 8
T = 64
HALO = 16
EPS = 1e-05
AXES = ("z", "yh", "yl", "x", "c")
SP = ("z", "yh", "yl")
TP = ("x", "c")
LINE = ("z", "yh")
GROUP = ("yl", "x", "c")
bf16 = jnp.bfloat16
f32 = jnp.float32
VM = pl.BlockSpec(memory_space=pltpu.VMEM)
SM = pl.BlockSpec(memory_space=pltpu.SMEM)


def call(body, outs, ins, scratch=(), mib=16, flops=0):
    return pl.pallas_call(
        body,
        out_shape=outs,
        in_specs=[SM] + [VM] * (len(ins) - 1),
        out_specs=jax.tree.map(lambda _: VM, outs),
        scratch_shapes=list(scratch),
        compiler_params=pltpu.CompilerParams(vmem_limit_bytes=mib * 1024 * 1024),
        cost_estimate=pl.CostEstimate(flops=flops, bytes_accessed=1 << 20, transcendentals=0),
        name=body.__name__,
    )(*ins)


def shift(value, axis, d):
    n = lax.axis_size(axis)
    return lax.ppermute(value, axis, [(i, (i + d) % n) for i in range(n)])


def to_all(value, axes):
    n = lax.axis_size(axes)
    many = jnp.broadcast_to(value[None], (n,) + value.shape)
    return lax.all_to_all(many, axes, 0, 0, tiled=True)


def silu(v):
    return v / (1.0 + jnp.exp(-v))


def softplus(v):
    return jnp.maximum(v, 0.0) + jnp.log1p(jnp.exp(-jnp.abs(v)))


def dot(a, b, dims=((1,), (0,))):
    return lax.dot_general(a, b, (dims, ((), ())), preferred_element_type=f32)


def project(ref, w):
    v = ref[...].reshape(SEQS * PIECE, 1024)
    vf = v.astype(f32)
    r = lax.rsqrt(jnp.mean(vf * vf, axis=1, keepdims=True) + EPS)
    return (dot(v, w) * r).astype(bf16).reshape(SEQS, PIECE, 640)


def project_near(idx, *refs):
    pieces, w, out = refs[:12], refs[12], refs[13]
    rows = jnp.concatenate([p[...].reshape(SEQS * PIECE, 1024) for p in pieces], axis=0)
    vf = rows.astype(f32)
    r = lax.rsqrt(jnp.mean(vf * vf, axis=1, keepdims=True) + EPS)
    out[...] = (dot(rows, w[...]) * r).astype(bf16).reshape(12, SEQS, PIECE, 640)


def slots(idx):
    yl, x, c = idx[2], idx[3], idx[4]
    near, far = [], []
    for core in (c, 1 - c):
        for half in (yl, 1 - yl):
            for d in (0, 1, 3, 2):
                at = ((half * 4 + lax.rem(x - d + 4, 4)) * 2 + core) * PIECE
                (far if d == 2 else near).append(pl.multiple_of(at, PIECE))
    return near, far


def project_far(idx, *refs):
    pieces, w, done = refs[:4], refs[4], refs[5]
    xb, cr, zr, dr, tail = refs[6:]
    near, far = slots(idx)
    rows = jnp.concatenate([p[...].reshape(SEQS * PIECE, 1024) for p in pieces], axis=0)
    vf = rows.astype(f32)
    r = lax.rsqrt(jnp.mean(vf * vf, axis=1, keepdims=True) + EPS)
    last = (dot(rows, w[...]) * r).astype(bf16).reshape(4, SEQS, PIECE, 640)
    for at, value in list(zip(near, [done[k] for k in range(12)])) + list(zip(far, [last[k] for k in range(4)])):
        for s in range(SEQS):
            xb[s, pl.ds(at, PIECE), :] = value[s, :, 0:256]
            cr[s, pl.ds(at, PIECE), :] = value[s, :, 256:384]
            zr[s, pl.ds(at, PIECE), :] = value[s, :, 384:512]
            dr[s, pl.ds(at, PIECE), :] = value[s, :, 512:640]
    tail[:, :, 0:256] = xb[:, SPAN - HALO :, :]
    tail[:, :, 256:384] = cr[:, SPAN - HALO :, :]


def convolve(ext, taps, lanes, first, count):
    out = None
    for k in range(4):
        at = HALO - 3 + k + first
        part = taps[k : k + 1, lanes] * ext[at : at + count, :]
        out = part if out is None else out + part
    return silu(out)


def span_state(idx, xb, dr, taps, dtb, rate, u_out, b_out, l_out, d_out, s_out, ext):
    row = lax.broadcasted_iota(jnp.int32, (T, 2 * T), 0)
    col = lax.broadcasted_iota(jnp.int32, (T, 2 * T), 1)
    tri = (lax.rem(col, T) <= row).astype(bf16)
    for s in range(SEQS):
        ext[HALO:, :] = xb[s].astype(f32)
        dt = softplus(dr[s].astype(f32) + dtb[...])
        ld = -(dt * rate[...]) / LENGTH
        hi = ld.astype(bf16)
        lo = (ld - hi.astype(f32)).astype(bf16)
        total = jnp.zeros((1, 128), f32)
        for k in range(SPAN // T):
            at = slice(k * T, k * T + T)
            lc = dot(tri, jnp.concatenate([hi[at], lo[at]], axis=0)) + total
            l_out[s, at, :] = lc
            total = lc[T - 1 : T, :]
        d_out[s] = dt[0:T]
        conv = convolve(ext, taps, slice(0, 256), T, SPAN - T)
        u = conv[:, 0:128] * dt[T:]
        b = conv[:, 128:256].astype(bf16)
        u_out[s, T:, :] = u.astype(bf16)
        b_out[s, T:, :] = b
        late = (u * jnp.exp(total - l_out[s, T:, :])).astype(bf16)
        s_out[s] = dot(b, late, ((0,), (0,)))


def span_first(idx, xb, halo, taps, l, dt, part, u_out, b_out, pack, ext):
    for s in range(SEQS):
        ext[0:HALO, :] = halo[s, :, 0:256].astype(f32)
        ext[HALO:, :] = xb[s, 0:T, :].astype(f32)
        conv = convolve(ext, taps, slice(0, 256), 0, T)
        total = l[s, SPAN - 1 : SPAN, :]
        u = conv[:, 0:128] * dt[s]
        b = conv[:, 128:256].astype(bf16)
        u_out[s] = u.astype(bf16)
        b_out[s] = b
        late = (u * jnp.exp(total - l[s, 0:T, :])).astype(bf16)
        pack[s, 0:128, :] = (part[s] + dot(b, late, ((0,), (0,)))).astype(bf16)
        t_hi = total.astype(bf16).astype(f32)
        which = lax.broadcasted_iota(jnp.int32, (16, 128), 0)
        both = jnp.where(which == 0, t_hi, jnp.where(which == 1, total - t_hi, 0.0))
        pack[s, 128:144, :] = both.astype(bf16)


def span_own(idx, u, b, u0, b0, l, cr, zr, halo, taps, y_out, c_out, z_out, ext):
    row = lax.broadcasted_iota(jnp.int32, (T, 128), 0)
    col = lax.rem(lax.broadcasted_iota(jnp.int32, (T, 128), 1), T)
    seen = col <= row
    up = (row <= col).astype(f32)
    left = lax.broadcasted_iota(jnp.int32, (T, 128), 1) < T
    for s in range(SEQS):
        ext[0:HALO, :] = halo[s, :, 256:384].astype(f32)
        ext[HALO:, :] = cr[s].astype(f32)
        c_out[s] = convolve(ext, taps, slice(256, 384), 0, SPAN).astype(bf16)
        z_out[s] = silu(zr[s].astype(f32)).astype(bf16)
        state = jnp.zeros((128, 128), f32)
        start = jnp.zeros((1, 128), f32)
        for k in range(SPAN // T):
            at = slice(k * T, k * T + T)
            lc = l[s, at, :]
            uc = u0[s] if k == 0 else u[s, at, :]
            bc = b0[s] if k == 0 else b[s, at, :]
            cc = c_out[s, at, :]
            step = lc - jnp.concatenate([start, lc[0 : T - 1, :]], axis=0)
            l_row = start + jnp.sum(step * up, axis=0, keepdims=True)
            pairs = dot(cc, jnp.concatenate([bc, bc], axis=0), ((1,), (1,)))
            gap = jnp.exp(jnp.where(seen, lc - l_row, -jnp.inf))
            m = (pairs * gap).astype(bf16)
            zero = jnp.zeros_like(uc)
            blocks = jnp.concatenate([jnp.where(left, uc, zero), jnp.where(left, zero, uc)], axis=0)
            y = dot(m, blocks)
            if k > 0:
                y = y + dot(cc, state.astype(bf16)) * jnp.exp(lc - start)
            y_out[s, at, :] = y
            end = lc[T - 1 : T, :]
            if k + 1 < SPAN // T:
                late = (uc.astype(f32) * jnp.exp(end - lc)).astype(bf16)
                state = state * jnp.exp(end - start) + dot(bc, late, ((0,), (0,)))
            start = end


def finish(idx, packs, y_own, cc, zs, l, gain, out):
    me = idx[0] * 2 + idx[1]
    for s in range(SEQS):
        state = jnp.zeros((128, 128), f32)
        for j in range(SPANS - 1):
            log = packs[j, s, 128:129, :].astype(f32) + packs[j, s, 129:130, :].astype(f32)
            then = state * jnp.exp(log) + packs[j, s, 0:128, :].astype(f32)
            state = jnp.where(j < me, then, state)
        y = y_own[s] + dot(cc[s], state.astype(bf16)) * jnp.exp(l[s])
        g = y * zs[s].astype(f32)
        g = g * lax.rsqrt(jnp.mean(g * g, axis=1, keepdims=True) + EPS) * gain[...]
        g = g.astype(bf16)
        for k in range(PIECES):
            out[k, s] = g[k * PIECE : k * PIECE + PIECE, :]


def order_out(idx, own, other, out):
    c = idx[4]
    for x in range(4):
        for ref, core in ((own, c), (other, 1 - c)):
            at = pl.multiple_of((2 * x + core) * 128, 128)
            out[pl.ds(at, 128), :] = ref[x].astype(f32).T.astype(bf16)


def project_out(idx, g, w, out):
    for k in range(2):
        rows = jnp.concatenate([g[8 * k + j].reshape(SEQS * PIECE, 128) for j in range(8)], axis=1)
        out[128 * k : 128 * k + 128, :] = dot(rows, w[...]).astype(bf16)


def struct(shape, kind=bf16):
    return jax.ShapeDtypeStruct(shape, kind)


def local(
    tokens,
    norm_gain,
    x_weight,
    z_weight,
    b_weight,
    c_weight,
    dt_weight,
    x_conv,
    b_conv,
    c_conv,
    dt_bias,
    decay_rate,
    out_gain,
    out_weight,
):
    idx = jnp.stack([lax.axis_index(a) for a in AXES]).astype(jnp.int32)
    sp = lax.axis_index(SP)
    even = lax.axis_index("yl") == 0
    keep = jnp.where(even, tokens[0:2], tokens[2:4])
    give = jnp.where(even, tokens[2:4], tokens[0:2])
    got = shift(give, "yl", 1)
    left_a = shift(keep, "x", 1)
    right_a = shift(keep, "x", -1)
    left_b = shift(got, "x", 1)
    right_b = shift(got, "x", -1)
    far_a = shift(left_a, "x", 1)
    far_b = shift(right_b, "x", -1)
    near = (keep, left_a, right_a, got, left_b, right_b)
    near = near + tuple(shift(v, "c", 1) for v in near)
    far = (far_a, far_b)
    far = far + tuple(shift(v, "c", 1) for v in far)

    gain = lax.dynamic_slice_in_dim(norm_gain, sp * 64, 64)[:, None]
    wide_dt = jnp.repeat(dt_weight, 64, axis=1)
    w_own = jnp.concatenate([x_weight, b_weight, c_weight, z_weight, wide_dt], axis=1)
    w_own = (w_own.astype(f32) * gain).astype(bf16)
    w_in = to_all(w_own, SP).reshape(1024, 640)

    o_here = to_all(out_weight.T, SP).reshape(1024, 128)
    o_line = to_all(o_here, "x")
    w_out = call(order_out, struct((1024, 1024)), [idx, o_line, shift(o_line, "c", 1)])

    taps = jnp.concatenate([x_conv, b_conv, c_conv], axis=1)
    dtb = jnp.repeat(dt_bias, 64)[None]
    rate = jnp.repeat(decay_rate, 64)[None]

    half = struct((SEQS, SPAN, 128))
    wide = struct((SEQS, SPAN, 128), f32)
    first = struct((SEQS, T, 128))
    done = call(project_near, struct((12, SEQS, PIECE, 640)), [idx, *near, w_in])
    xb, cr, zr, dr, tail = call(
        project_far,
        (struct((SEQS, SPAN, 256)), half, half, half, struct((SEQS, HALO, 384))),
        [idx, *far, w_in, done],
    )
    halo = lax.ppermute(tail, LINE, [(i, i + 1) for i in range(SPANS - 1)])
    u, b, l, dt0, part = call(
        span_state,
        (half, half, wide, struct((SEQS, T, 128), f32), struct((SEQS, 128, 128), f32)),
        [idx, xb, dr, taps, dtb, rate],
        [pltpu.VMEM((HALO + SPAN, 256), f32)],
        flops=1 << 32,
    )
    u0, b0, pack = call(
        span_first,
        (first, first, struct((SEQS, 144, 128))),
        [idx, xb, halo, taps, l, dt0, part],
        [pltpu.VMEM((HALO + T, 256), f32)],
    )
    packs = to_all(pack, LINE)
    y_own, cc, zs = call(
        span_own,
        (wide, half, half),
        [idx, u, b, u0, b0, l, cr, zr, halo, taps],
        [pltpu.VMEM((HALO + SPAN, 128), f32)],
        flops=1 << 32,
    )
    gated = call(
        finish,
        struct((PIECES, SEQS, PIECE, 128)),
        [idx, packs, y_own, cc, zs, l, out_gain[None]],
    )
    back = lax.all_to_all(gated, GROUP, 0, 0, tiled=True)
    out = call(project_out, struct((256, 1024)), [idx, back, w_out])
    return out.reshape(2 * SEQS, PIECE, 1024)


def solution(mesh):
    torus = Mesh(mesh.devices.reshape(4, 2, 2, 4, 2), AXES)
    return jax.shard_map(
        local,
        mesh=torus,
        in_specs=(
            P(None, AXES, None),
            P(),
            P(SP, TP),
            P(SP, TP),
            P(SP, TP),
            P(SP, TP),
            P(SP, TP),
            P(None, TP),
            P(None, TP),
            P(None, TP),
            P(TP),
            P(TP),
            P(TP),
            P(TP, SP),
        ),
        out_specs=P(None, AXES, None),
        check_vma=False,
    )
```

```python
import jax
import jax.numpy as jnp
from jax import lax
from jax.experimental import pallas as pl
from jax.experimental.pallas import tpu as pltpu
from jax.sharding import Mesh
from jax.sharding import PartitionSpec as P


LENGTH = 8192
HEAD_P = 64
SEQS = 2
SPAN = 1024
PIECE = 64
PIECES = 16
SPANS = 8
T = 64
HALO = 16
EPS = 1e-05
AXES = ("z", "yh", "yl", "x", "c")
SP = ("z", "yh", "yl")
TP = ("x", "c")
LINE = ("z", "yh")
GROUP = ("yl", "x", "c")
bf16 = jnp.bfloat16
f32 = jnp.float32
VM = pl.BlockSpec(memory_space=pltpu.VMEM)
SM = pl.BlockSpec(memory_space=pltpu.SMEM)


HB = pl.BlockSpec(memory_space=pltpu.HBM)
DMA = pltpu.SemaphoreType.DMA


def call(body, outs, ins, scratch=(), mib=16, us=2, scalars=0, hbm=()):
    ins = [pltpu.with_memory_space_constraint(v, pltpu.HBM) if k in hbm else v for k, v in enumerate(ins)]
    return pl.pallas_call(
        body,
        out_shape=outs,
        in_specs=[SM if k < scalars else HB if k in hbm else VM for k in range(len(ins))],
        out_specs=tuple(VM if isinstance(o, jax.ShapeDtypeStruct) else HB for o in outs),
        scratch_shapes=list(scratch),
        compiler_params=pltpu.CompilerParams(vmem_limit_bytes=mib * 1024 * 1024),
        cost_estimate=pl.CostEstimate(
            flops=us * 1000000000, bytes_accessed=1 << 20, transcendentals=0
        ),
    )(*ins)


def fetch(pairs, sems):
    moves = [pltpu.make_async_copy(a, b, sems.at[k]) for k, (a, b) in enumerate(pairs)]
    for m in moves:
        m.start()
    return moves


def place():
    return [lax.axis_index(a) for a in AXES]


def shift(value, axis, d):
    n = lax.axis_size(axis)
    return lax.ppermute(value, axis, [(i, (i + d) % n) for i in range(n)])


def exchange(value, axes):
    return lax.all_to_all(value, axes, 0, 0, tiled=True)


def silu(v):
    return v / (1.0 + jnp.exp(-v))


def softplus(v):
    return jnp.maximum(v, 0.0) + jnp.log1p(jnp.exp(-jnp.abs(v)))


def dot(a, b, dims=((1,), (0,))):
    return lax.dot_general(a, b, (dims, ((), ())), preferred_element_type=f32)


def prepare(*refs):
    ins, (w_out, o_out), held, (turned, sems) = refs[:7], refs[7:9], refs[9:16], refs[16:]
    moves = fetch(list(zip(ins, held)), sems)
    for m in moves:
        m.wait()
    xw, bw, cw, zw, dw, gain, ow = held
    z, yh, yl, _, _ = place()
    sp = z * 4 + yh * 2 + yl
    row = gain[pl.ds(lax.div(sp, 2), 1), :]
    first = lax.rem(sp, 2) == 0
    row = jnp.where(first, row[:, 0:64], row[:, 64:128])
    row = jnp.concatenate([row, row], axis=1)
    g = jnp.broadcast_to(row, (128, 128)).T[0:64]
    dt = dw[...].astype(f32)
    dt = jnp.concatenate([dt[0:1], dt[1:2]], axis=1) * row
    dt = jnp.broadcast_to(dt, (8, 128)).astype(bf16)
    ws = [(v[...].astype(f32) * g).astype(bf16) for v in (xw, bw, cw, zw)]
    o = ow[...]
    for k in range(16):
        for j in range(4):
            w_out[k, 0:64, 128 * j : 128 * j + 128] = ws[j]
        w_out[k, 64:72, 0:128] = dt
        w_out[k, 64:72, 128:512] = jnp.zeros((8, 384), bf16)
        o_out[k] = o


def order_in(parts, w):
    lane = lax.broadcasted_iota(jnp.int32, (64, 128), 1)
    for k in range(16):
        w[64 * k : 64 * k + 64, 0:512] = parts[k, 0:64, :]
        row = parts[k, 64:72, 0:128].astype(f32)[0:1]
        both = jnp.broadcast_to(row, (128, 128)).T
        w[64 * k : 64 * k + 64, 512:640] = jnp.where(lane < 64, both[0:64], both[64:128]).astype(bf16)


def project_near(*refs):
    pieces, w, out = refs[:12], refs[12], refs[13]
    rows = jnp.concatenate([p[...].reshape(SEQS * PIECE, 1024) for p in pieces], axis=0)
    vf = rows.astype(f32)
    r = lax.rsqrt(jnp.mean(vf * vf, axis=1, keepdims=True) + EPS)
    out[...] = (dot(rows, w[...]) * r).astype(bf16).reshape(12, SEQS, PIECE, 640)


def slots():
    _, _, yl, x, c = place()
    near, far = [], []
    for core in (c, 1 - c):
        for half in (yl, 1 - yl):
            for d in (0, 1, 3, 2):
                at = ((half * 4 + lax.rem(x - d + 4, 4)) * 2 + core) * PIECE
                (far if d == 2 else near).append(pl.multiple_of(at, PIECE))
    return near, far


def project_far(*refs):
    pieces, w, done = refs[:4], refs[4], refs[5]
    xb, cr, zr, dr, tail, x0 = refs[6:]
    near, far = slots()
    rows = jnp.concatenate([p[...].reshape(SEQS * PIECE, 1024) for p in pieces], axis=0)
    vf = rows.astype(f32)
    r = lax.rsqrt(jnp.mean(vf * vf, axis=1, keepdims=True) + EPS)
    last = (dot(rows, w[...]) * r).astype(bf16).reshape(4, SEQS, PIECE, 640)
    for at, value in list(zip(near, [done[k] for k in range(12)])) + list(zip(far, [last[k] for k in range(4)])):
        for s in range(SEQS):
            xb[s, pl.ds(at, PIECE), :] = value[s, :, 0:256]
            cr[s, pl.ds(at, PIECE), :] = value[s, :, 256:384]
            zr[s, pl.ds(at, PIECE), :] = value[s, :, 384:512]
            dr[s, pl.ds(at, PIECE), :] = value[s, :, 512:640]
    x0[...] = xb[:, 0:T, :]
    tail[:, :, 0:256] = xb[:, SPAN - HALO :, :]
    tail[:, :, 256:384] = cr[:, SPAN - HALO :, :]


def convolve(ext, taps, lanes, first, count):
    out = None
    for k in range(4):
        at = HALO - 3 + k + first
        part = taps[k : k + 1, :] * ext[at : at + count, lanes]
        out = part if out is None else out + part
    return silu(out)


def span_state(bias, rates, xb, dr, zr, x_taps, b_taps, u_out, b_out, l_out, e_out, d_out, s_out, z_out, ext, l_all, u_v, b_v, sem):
    away = fetch([(zr, z_out)], sem.at[pl.ds(0, 1)])
    head = lax.broadcasted_iota(jnp.int32, (1, 128), 1) < HEAD_P
    dtb = jnp.where(head, bias[0], bias[1])
    rate = jnp.where(head, rates[0], rates[1])
    row = lax.broadcasted_iota(jnp.int32, (T, 2 * T), 0)
    col = lax.broadcasted_iota(jnp.int32, (T, 2 * T), 1)
    tri = (lax.rem(col, T) <= row).astype(bf16)
    for s in range(SEQS):
        ext[HALO:, :] = xb[s].astype(f32)
        dt = softplus(dr[s].astype(f32) + dtb)
        ld = -(dt * rate) / LENGTH
        hi = ld.astype(bf16)
        lo = (ld - hi.astype(f32)).astype(bf16)
        total = jnp.zeros((1, 128), f32)
        for k in range(SPAN // T):
            at = slice(k * T, k * T + T)
            lc = dot(tri, jnp.concatenate([hi[at], lo[at]], axis=0))
            l_out[s, at, :] = lc.astype(bf16)
            l_all[at, :] = lc + total
            total = lc[T - 1 : T, :] + total
            e_out[s, k : k + 1, :] = total
        d_out[s] = dt[0:T]
        u = convolve(ext, x_taps, slice(0, 128), T, SPAN - T) * dt[T:]
        b = convolve(ext, b_taps, slice(128, 256), T, SPAN - T).astype(bf16)
        u_v[s, T:, :] = u.astype(bf16)
        b_v[s, T:, :] = b
        late_rows = pl.ds(T, SPAN - T)
        ready = [(u_v.at[s, late_rows, :], u_out.at[s, late_rows, :]), (b_v.at[s, late_rows, :], b_out.at[s, late_rows, :])]
        away += fetch(ready, sem.at[pl.ds(1 + 2 * s, 2)])
        late = (u * jnp.exp(total - l_all[T:, :])).astype(bf16)
        s_out[s] = dot(b, late, ((0,), (0,)))
    for m in away:
        m.wait()


def span_first(x0, halo, x_taps, b_taps, l, ends, dt, part, u_out, b_out, pack, ext):
    for s in range(SEQS):
        ext[0:HALO, :] = halo[s, :, 0:256].astype(f32)
        ext[HALO:, :] = x0[s].astype(f32)
        total = ends[s, PIECES - 1 : PIECES, :]
        u = convolve(ext, x_taps, slice(0, 128), 0, T) * dt[s]
        b = convolve(ext, b_taps, slice(128, 256), 0, T).astype(bf16)
        u_out[s] = u.astype(bf16)
        b_out[s] = b
        late = (u * jnp.exp(total - l[s, 0:T, :].astype(f32))).astype(bf16)
        state = (part[s] + dot(b, late, ((0,), (0,)))).astype(bf16)
        t_hi = total.astype(bf16).astype(f32)
        which = lax.broadcasted_iota(jnp.int32, (16, 128), 0)
        both = jnp.where(which == 0, t_hi, jnp.where(which == 1, total - t_hi, 0.0))
        both = both.astype(bf16)
        for k in range(SPANS):
            pack[k, s, 0:128, :] = state
            pack[k, s, 128:144, :] = both


def span_own(u, b, u0, b0, l, ends, cr, zr, halo, taps, y_out, c_out, e_out, ext, uv, bv, zv, sem):
    come = []
    for s in range(SEQS):
        later = pl.ds(T, SPAN - T)
        moves = [(zr.at[s], zv.at[s])]
        moves += [(u.at[s, later, :], uv.at[s, later, :]), (b.at[s, later, :], bv.at[s, later, :])]
        come.append(fetch(moves, sem.at[pl.ds(3 * s, 3)]))
    row = lax.broadcasted_iota(jnp.int32, (T, 128), 0)
    col = lax.rem(lax.broadcasted_iota(jnp.int32, (T, 128), 1), T)
    seen = col <= row
    up = (row <= col).astype(f32)
    left = lax.broadcasted_iota(jnp.int32, (T, 128), 1) < T
    for s in range(SEQS):
        ext[0:HALO, :] = halo[s, :, 256:384].astype(f32)
        ext[HALO:, :] = cr[s].astype(f32)
        c_out[s] = convolve(ext, taps, slice(0, 128), 0, SPAN).astype(bf16)
        for m in come[s]:
            m.wait()
        state = jnp.zeros((128, 128), f32)
        for k in range(SPAN // T):
            at = slice(k * T, k * T + T)
            lc = l[s, at, :].astype(f32)
            uc = u0[s] if k == 0 else uv[s, at, :]
            bc = b0[s] if k == 0 else bv[s, at, :]
            cc = c_out[s, at, :]
            step = lc - jnp.concatenate([jnp.zeros((1, 128), f32), lc[0 : T - 1, :]], axis=0)
            l_row = jnp.sum(step * up, axis=0, keepdims=True)
            pairs = dot(cc, jnp.concatenate([bc, bc], axis=0), ((1,), (1,)))
            gap = jnp.exp(jnp.where(seen, lc - l_row, -jnp.inf))
            m = (pairs * gap).astype(bf16)
            zero = jnp.zeros_like(uc)
            blocks = jnp.concatenate([jnp.where(left, uc, zero), jnp.where(left, zero, uc)], axis=0)
            y = dot(m, blocks)
            gate = silu(zv[s, at, :].astype(f32))
            here = jnp.exp(lc)
            if k > 0:
                y = y + dot(cc, state.astype(bf16)) * here
                e_out[s, at, :] = (gate * here * jnp.exp(ends[s, k - 1 : k, :])).astype(bf16)
            else:
                e_out[s, at, :] = (gate * here).astype(bf16)
            y_out[s, at, :] = (y * gate).astype(bf16)
            end = lc[T - 1 : T, :]
            if k + 1 < SPAN // T:
                late = (uc.astype(f32) * jnp.exp(end - lc)).astype(bf16)
                state = state * jnp.exp(end) + dot(bc, late, ((0,), (0,)))


def finish(packs, y_own, cc, decay, gain, out):
    z, yh, _, _, _ = place()
    me = z * 2 + yh
    for s in range(SEQS):
        state = jnp.zeros((128, 128), f32)
        for j in range(SPANS - 1):
            log = packs[j, s, 128:129, :].astype(f32) + packs[j, s, 129:130, :].astype(f32)
            then = state * jnp.exp(log) + packs[j, s, 0:128, :].astype(f32)
            state = jnp.where(j < me, then, state)
        g = y_own[s].astype(f32) + dot(cc[s], state.astype(bf16)) * decay[s].astype(f32)
        g = g * lax.rsqrt(jnp.mean(g * g, axis=1, keepdims=True) + EPS) * gain[...]
        g = g.astype(bf16)
        for k in range(PIECES):
            out[k, s] = g[k * PIECE : k * PIECE + PIECE, :]


def order_out(*refs):
    ins, out, held, sems = refs[:10], refs[10], refs[11], refs[12]
    places = [(0, 1024), (1024, 1024), (2048, 1024), (3072, 512), (3584, 512)]
    places = places + [(4096 + a, n) for a, n in places]
    moves = fetch([(r, held.at[pl.ds(a, n), :]) for r, (a, n) in zip(ins, places)], sems)
    for m in moves:
        m.wait()
    _, _, _, x, c = place()
    for core in range(2):
        half = lax.rem(c + core, 2)
        for k, d in enumerate((0, 1, 3, 2)):
            at = pl.multiple_of((2 * lax.rem(x - d + 4, 4) + half) * 128, 128)
            first = 4096 * core + 1024 * k
            out[pl.ds(at, 128), :] = held[first : first + 1024, :].astype(f32).T.astype(bf16)


def project_out(g, w, out):
    for k in range(2):
        rows = jnp.concatenate([g[8 * k + j].reshape(SEQS * PIECE, 128) for j in range(8)], axis=1)
        out[128 * k : 128 * k + 128, :] = dot(rows, w[...]).astype(bf16)


def struct(shape, kind=bf16):
    return jax.ShapeDtypeStruct(shape, kind)


def local(
    tokens,
    norm_gain,
    x_weight,
    z_weight,
    b_weight,
    c_weight,
    dt_weight,
    x_conv,
    b_conv,
    c_conv,
    dt_bias,
    decay_rate,
    out_gain,
    out_weight,
):
    even = lax.axis_index("yl") == 0
    keep = jnp.where(even, tokens[0:2], tokens[2:4])
    give = jnp.where(even, tokens[2:4], tokens[0:2])
    got = shift(give, "yl", 1)
    left_a = shift(keep, "x", 1)
    right_a = shift(keep, "x", -1)
    left_b = shift(got, "x", 1)
    right_b = shift(got, "x", -1)
    far_a = shift(left_a, "x", 1)
    far_b = shift(right_b, "x", -1)
    near = (keep, left_a, right_a, got, left_b, right_b)
    near = near + tuple(shift(v, "c", 1) for v in near)
    far = (far_a, far_b)
    far = far + tuple(shift(v, "c", 1) for v in far)

    weights = [x_weight, b_weight, c_weight, z_weight]
    weights = weights + [dt_weight.T, norm_gain.reshape(8, 128), out_weight.T]
    w_own, o_own = call(
        prepare,
        (struct((16, 72, 512)), struct((16, 64, 128))),
        weights,
        [pltpu.VMEM(w.shape, w.dtype) for w in weights] + [pltpu.VMEM((128, 128), f32), DMA((7,))],
        hbm=range(7),
    )
    (w_in,) = call(order_in, (struct((1024, 640)),), [exchange(w_own, SP)])
    o_here = exchange(o_own, SP).reshape(1024, 128)
    o_left = shift(o_here, "x", 1)
    o_right = shift(o_here, "x", -1)
    o_far_a = shift(o_left[:512], "x", 1)
    o_far_b = shift(o_right[512:], "x", -1)
    outs = (o_here, o_left, o_right, o_far_a, o_far_b)
    outs = outs + tuple(shift(v, "c", 1) for v in outs)
    (w_out,) = call(
        order_out,
        (struct((1024, 1024)),),
        outs,
        [pltpu.VMEM((8192, 128), bf16), DMA((10,))],
        hbm=range(10),
    )

    half = struct((SEQS, SPAN, 128))
    first = struct((SEQS, T, 128))
    state = struct((SEQS, 128, 128), f32)
    far_s = pltpu.HBM(half.shape, bf16)
    ends_s = struct((SEQS, PIECES, 128), f32)
    (done,) = call(project_near, (struct((12, SEQS, PIECE, 640)),), [*near, w_in], us=4)
    xb, cr, zr, dr, tail, x0 = call(
        project_far,
        (
            struct((SEQS, SPAN, 256)),
            half,
            half,
            half,
            struct((SEQS, HALO, 384)),
            struct((SEQS, T, 256)),
        ),
        [*far, w_in, done],
    )
    halo = lax.ppermute(tail, LINE, [(i, i + 1) for i in range(SPANS - 1)])
    u, b, l, ends, dt0, part, z_far = call(
        span_state,
        (far_s, far_s, half, ends_s, struct((SEQS, T, 128), f32), state, far_s),
        [dt_bias, decay_rate, xb, dr, zr, x_conv, b_conv],
        [pltpu.VMEM((HALO + SPAN, 256), f32), pltpu.VMEM((SPAN, 128), f32), pltpu.VMEM(half.shape, bf16), pltpu.VMEM(half.shape, bf16), DMA((5,))],
        us=4,
        scalars=2,
    )
    u0, b0, packs = call(
        span_first,
        (first, first, struct((SPANS, SEQS, 144, 128))),
        [x0, halo, x_conv, b_conv, l, ends, dt0, part],
        [pltpu.VMEM((HALO + T, 256), f32)],
    )
    packs = exchange(packs, LINE)
    y_own, cc, decay = call(
        span_own,
        (half, half, half),
        [u, b, u0, b0, l, ends, cr, z_far, halo, c_conv],
        [pltpu.VMEM((HALO + SPAN, 128), f32)] + [pltpu.VMEM(half.shape, bf16)] * 3 + [DMA((6,))],
        us=6,
        hbm=(0, 1, 7),
    )
    (gated,) = call(
        finish,
        (struct((PIECES, SEQS, PIECE, 128)),),
        [packs, y_own, cc, decay, out_gain[None]],
    )
    back = exchange(gated, GROUP)
    (out,) = call(project_out, (struct((256, 1024)),), [back, w_out])
    return out.reshape(2 * SEQS, PIECE, 1024)


def solution(mesh):
    torus = Mesh(mesh.devices.reshape(4, 2, 2, 4, 2), AXES)
    return jax.shard_map(
        local,
        mesh=torus,
        in_specs=(
            P(None, AXES, None),
            P(),
            P(SP, TP),
            P(SP, TP),
            P(SP, TP),
            P(SP, TP),
            P(SP, TP),
            P(None, TP),
            P(None, TP),
            P(None, TP),
            P(TP),
            P(TP),
            P(TP),
            P(TP, SP),
        ),
        out_specs=P(None, AXES, None),
        check_vma=False,
    )
```

```python
import jax
import jax.numpy as jnp
from jax import lax
from jax.experimental import pallas as pl
from jax.experimental.pallas import tpu as pltpu
from jax.sharding import Mesh
from jax.sharding import PartitionSpec as P


LENGTH = 8192
HEAD_P = 64
SEQS = 2
SPAN = 1024
PIECE = 64
PIECES = 16
SPANS = 8
T = 64
HALO = 16
EPS = 1e-05
AXES = ("z", "yh", "yl", "x", "c")
SP = ("z", "yh", "yl")
TP = ("x", "c")
LINE = ("z", "yh")
GROUP = ("yl", "x", "c")
bf16 = jnp.bfloat16
f32 = jnp.float32
VM = pl.BlockSpec(memory_space=pltpu.VMEM)
SM = pl.BlockSpec(memory_space=pltpu.SMEM)


HB = pl.BlockSpec(memory_space=pltpu.HBM)
DMA = pltpu.SemaphoreType.DMA


def call(body, outs, ins, scratch=(), mib=16, us=2, scalars=0, hbm=()):
    ins = [pltpu.with_memory_space_constraint(v, pltpu.HBM) if k in hbm else v for k, v in enumerate(ins)]
    return pl.pallas_call(
        body,
        out_shape=outs,
        in_specs=[SM if k < scalars else HB if k in hbm else VM for k in range(len(ins))],
        out_specs=tuple(VM if isinstance(o, jax.ShapeDtypeStruct) else HB for o in outs),
        scratch_shapes=list(scratch),
        compiler_params=pltpu.CompilerParams(vmem_limit_bytes=mib * 1024 * 1024),
        cost_estimate=pl.CostEstimate(
            flops=us * 1000000000, bytes_accessed=1 << 20, transcendentals=0
        ),
    )(*ins)


def fetch(pairs, sems):
    moves = [pltpu.make_async_copy(a, b, sems.at[k]) for k, (a, b) in enumerate(pairs)]
    for m in moves:
        m.start()
    return moves


def place():
    return [lax.axis_index(a) for a in AXES]


def shift(value, axis, d):
    n = lax.axis_size(axis)
    return lax.ppermute(value, axis, [(i, (i + d) % n) for i in range(n)])


def onward(value, d):
    return lax.ppermute(value, LINE, [(i, i + d) for i in range(SPANS - d)])


def exchange(value, axes):
    return lax.all_to_all(value, axes, 0, 0, tiled=True)


def silu(v):
    return v / (1.0 + jnp.exp(-v))


def softplus(v):
    return jnp.maximum(v, 0.0) + jnp.log1p(jnp.exp(-jnp.abs(v)))


def dot(a, b, dims=((1,), (0,))):
    return lax.dot_general(a, b, (dims, ((), ())), preferred_element_type=f32)


def prepare(*refs):
    ins, (w_out, o_out), held, (turned, sems) = refs[:7], refs[7:9], refs[9:16], refs[16:]
    moves = fetch(list(zip(ins, held)), sems)
    for m in moves:
        m.wait()
    xw, bw, cw, zw, dw, gain, ow = held
    z, yh, yl, _, _ = place()
    sp = z * 4 + yh * 2 + yl
    row = gain[pl.ds(lax.div(sp, 2), 1), :]
    first = lax.rem(sp, 2) == 0
    row = jnp.where(first, row[:, 0:64], row[:, 64:128])
    row = jnp.concatenate([row, row], axis=1)
    g = jnp.broadcast_to(row, (128, 128)).T[0:64]
    dt = dw[...].astype(f32)
    dt = jnp.concatenate([dt[0:1], dt[1:2]], axis=1) * row
    dt = jnp.broadcast_to(dt, (8, 128)).astype(bf16)
    ws = [(v[...].astype(f32) * g).astype(bf16) for v in (xw, bw, cw, zw)]
    o = ow[...]
    for j in range(4):
        w_out[0:64, 128 * j : 128 * j + 128] = ws[j]
    w_out[64:72, 0:128] = dt
    w_out[64:72, 128:512] = jnp.zeros((8, 384), bf16)
    for k in range(16):
        o_out[k] = o


def gather_y(p0, p1, p2, p3, out):
    _, yh, yl, _, _ = place()
    for d, p in enumerate((p0, p1, p2, p3)):
        out[lax.rem(2 * yh + yl - d + 4, 4)] = p[...]


def order_in(p0, p1, p2, p3, w):
    lane = lax.broadcasted_iota(jnp.int32, (64, 128), 1)
    z = lax.axis_index("z")
    for d, p in enumerate((p0, p1, p2, p3)):
        first = lax.rem(z - d + 4, 4) * 256
        for k in range(4):
            at = pl.ds(pl.multiple_of(first + 64 * k, 64), 64)
            w[at, 0:512] = p[k, 0:64, :]
            row = p[k, 64:72, 0:128].astype(f32)[0:1]
            both = jnp.broadcast_to(row, (128, 128)).T
            w[at, 512:640] = jnp.where(lane < 64, both[0:64], both[64:128]).astype(bf16)


def projected(pieces, w):
    rows = jnp.concatenate([p[...].reshape(SEQS * PIECE, 1024) for p in pieces], axis=0)
    vf = rows.astype(f32)
    r = lax.rsqrt(jnp.mean(vf * vf, axis=1, keepdims=True) + EPS)
    return (dot(rows, w[...]) * r).astype(bf16).reshape(len(pieces), SEQS, PIECE, 640)


def project_near(*refs):
    pieces, w, out, held, sem = refs[:12], refs[12], refs[13], refs[14], refs[15]
    away = []
    for k in range(3):
        held[4 * k : 4 * k + 4] = projected(pieces[4 * k : 4 * k + 4], w)
        part = pl.ds(4 * k, 4)
        away += fetch([(held.at[part], out.at[part])], sem.at[pl.ds(k, 1)])
    for m in away:
        m.wait()


def slots():
    _, _, yl, x, c = place()
    near, far = [], []
    for core in (c, 1 - c):
        for half in (yl, 1 - yl):
            for d in (0, 1, 3, 2):
                at = ((half * 4 + lax.rem(x - d + 4, 4)) * 2 + core) * PIECE
                (far if d == 2 else near).append(pl.multiple_of(at, PIECE))
    return near, far


def project_far(*refs):
    pieces, w, done = refs[:4], refs[4], refs[5]
    xb, cr, zr, dr, tail, x0, zl, sem = refs[6:]
    near, far = slots()
    lanes = ((xb, 0, 256), (cr, 256, 128), (zr, 384, 128), (dr, 512, 128))
    moves = []
    for k, at in enumerate(near):
        for s in range(SEQS):
            for ref, lane, n in lanes:
                moves.append((done.at[k, s, :, pl.ds(lane, n)], ref.at[s, pl.ds(at, PIECE), :]))
    come = fetch(moves, sem)
    last = projected(pieces, w)
    zl[...] = last[:, :, :, 384:512]
    moves = [(zl.at[k, s], zr.at[s, pl.ds(at, PIECE), :]) for k, at in enumerate(far) for s in range(SEQS)]
    come += fetch(moves, sem.at[pl.ds(96, 8)])
    for k, at in enumerate(far):
        for s in range(SEQS):
            for ref, lane, n in lanes:
                if ref is not zr:
                    ref[s, pl.ds(at, PIECE), :] = last[k, s, :, lane : lane + n]
    for m in come:
        m.wait()
    x0[...] = xb[:, 0:T, :]
    tail[:, :, 0:256] = xb[:, SPAN - HALO :, :]
    tail[:, :, 256:384] = cr[:, SPAN - HALO :, :]


def convolve(ext, taps, lanes, first, count):
    out = None
    for k in range(4):
        at = HALO - 3 + k + first
        part = taps[k : k + 1, :] * ext[at : at + count, lanes]
        out = part if out is None else out + part
    return silu(out)


def span_state(bias, rates, xb, dr, x_taps, b_taps, u_out, b_out, l_out, e_out, d_out, s_out, ext, l_all, u_v, b_v, sem):
    away = []
    head = lax.broadcasted_iota(jnp.int32, (1, 128), 1) < HEAD_P
    dtb = jnp.where(head, bias[0], bias[1])
    rate = jnp.where(head, rates[0], rates[1])
    row = lax.broadcasted_iota(jnp.int32, (T, 2 * T), 0)
    col = lax.broadcasted_iota(jnp.int32, (T, 2 * T), 1)
    tri = (lax.rem(col, T) <= row).astype(bf16)
    for s in range(SEQS):
        ext[HALO:, :] = xb[s].astype(f32)
        dt = softplus(dr[s].astype(f32) + dtb)
        ld = -(dt * rate) / LENGTH
        hi = ld.astype(bf16)
        lo = (ld - hi.astype(f32)).astype(bf16)
        total = jnp.zeros((1, 128), f32)
        for k in range(SPAN // T):
            at = slice(k * T, k * T + T)
            lc = dot(tri, jnp.concatenate([hi[at], lo[at]], axis=0))
            l_out[s, at, :] = lc.astype(bf16)
            l_all[at, :] = lc + total
            total = lc[T - 1 : T, :] + total
            e_out[s, k : k + 1, :] = total
        d_out[s] = dt[0:T]
        u = convolve(ext, x_taps, slice(0, 128), T, SPAN - T) * dt[T:]
        b = convolve(ext, b_taps, slice(128, 256), T, SPAN - T).astype(bf16)
        u_v[s, T:, :] = u.astype(bf16)
        b_v[s, T:, :] = b
        late_rows = pl.ds(T, SPAN - T)
        ready = [(u_v.at[s, late_rows, :], u_out.at[s, late_rows, :]), (b_v.at[s, late_rows, :], b_out.at[s, late_rows, :])]
        away += fetch(ready, sem.at[pl.ds(2 * s, 2)])
        late = (u * jnp.exp(total - l_all[T:, :])).astype(bf16)
        s_out[s] = dot(b, late, ((0,), (0,)))
    for m in away:
        m.wait()


def span_first(x0, halo, x_taps, b_taps, l, ends, dt, part, u_out, b_out, pack, ext):
    for s in range(SEQS):
        ext[0:HALO, :] = halo[s, :, 0:256].astype(f32)
        ext[HALO:, :] = x0[s].astype(f32)
        total = ends[s, PIECES - 1 : PIECES, :]
        u = convolve(ext, x_taps, slice(0, 128), 0, T) * dt[s]
        b = convolve(ext, b_taps, slice(128, 256), 0, T).astype(bf16)
        u_out[s] = u.astype(bf16)
        b_out[s] = b
        late = (u * jnp.exp(total - l[s, 0:T, :].astype(f32))).astype(bf16)
        state = (part[s] + dot(b, late, ((0,), (0,)))).astype(bf16)
        t_hi = total.astype(bf16).astype(f32)
        which = lax.broadcasted_iota(jnp.int32, (16, 128), 0)
        both = jnp.where(which == 0, t_hi, jnp.where(which == 1, total - t_hi, 0.0))
        pack[s, 0:128, :] = state
        pack[s, 128:144, :] = both.astype(bf16)


def span_own(u, b, u0, b0, l, ends, cr, zr, halo, taps, y_out, c_out, e_out, ext, uv, bv, zv, sem):
    come = []
    for s in range(SEQS):
        later = pl.ds(T, SPAN - T)
        moves = [(zr.at[s], zv.at[s])]
        moves += [(u.at[s, later, :], uv.at[s, later, :]), (b.at[s, later, :], bv.at[s, later, :])]
        come.append(fetch(moves, sem.at[pl.ds(3 * s, 3)]))
    row = lax.broadcasted_iota(jnp.int32, (T, 128), 0)
    col = lax.rem(lax.broadcasted_iota(jnp.int32, (T, 128), 1), T)
    seen = col <= row
    up = (row <= col).astype(f32)
    left = lax.broadcasted_iota(jnp.int32, (T, 128), 1) < T
    for s in range(SEQS):
        ext[0:HALO, :] = halo[s, :, 256:384].astype(f32)
        ext[HALO:, :] = cr[s].astype(f32)
        c_out[s] = convolve(ext, taps, slice(0, 128), 0, SPAN).astype(bf16)
        for m in come[s]:
            m.wait()
        state = jnp.zeros((128, 128), f32)
        for k in range(SPAN // T):
            at = slice(k * T, k * T + T)
            lc = l[s, at, :].astype(f32)
            uc = u0[s] if k == 0 else uv[s, at, :]
            bc = b0[s] if k == 0 else bv[s, at, :]
            cc = c_out[s, at, :]
            step = lc - jnp.concatenate([jnp.zeros((1, 128), f32), lc[0 : T - 1, :]], axis=0)
            l_row = jnp.sum(step * up, axis=0, keepdims=True)
            pairs = dot(cc, jnp.concatenate([bc, bc], axis=0), ((1,), (1,)))
            gap = jnp.exp(jnp.where(seen, lc - l_row, -jnp.inf))
            m = (pairs * gap).astype(bf16)
            zero = jnp.zeros_like(uc)
            blocks = jnp.concatenate([jnp.where(left, uc, zero), jnp.where(left, zero, uc)], axis=0)
            y = dot(m, blocks)
            gate = silu(zv[s, at, :].astype(f32))
            here = jnp.exp(lc)
            if k > 0:
                y = y + dot(cc, state.astype(bf16)) * here
                e_out[s, at, :] = (gate * here * jnp.exp(ends[s, k - 1 : k, :])).astype(bf16)
            else:
                e_out[s, at, :] = (gate * here).astype(bf16)
            y_out[s, at, :] = (y * gate).astype(bf16)
            end = lc[T - 1 : T, :]
            if k + 1 < SPAN // T:
                late = (uc.astype(f32) * jnp.exp(end - lc)).astype(bf16)
                state = state * jnp.exp(end) + dot(bc, late, ((0,), (0,)))


def finish(*refs):
    packs, (y_own, cc, decay, gain, out) = refs[:7], refs[7:]
    for s in range(SEQS):
        state = packs[0][s, 0:128, :].astype(f32)
        log = jnp.zeros((1, 128), f32)
        for j in range(1, SPANS - 1):
            p = packs[j - 1]
            log = log + p[s, 128:129, :].astype(f32) + p[s, 129:130, :].astype(f32)
            state = state + packs[j][s, 0:128, :].astype(f32) * jnp.exp(log)
        g = y_own[s].astype(f32) + dot(cc[s], state.astype(bf16)) * decay[s].astype(f32)
        g = g * lax.rsqrt(jnp.mean(g * g, axis=1, keepdims=True) + EPS) * gain[...]
        g = g.astype(bf16)
        for k in range(PIECES):
            out[k, s] = g[k * PIECE : k * PIECE + PIECE, :]


def order_out(*refs):
    ins, out, held, sems = refs[:8], refs[8], refs[9], refs[10]
    moves = fetch([(r, held.at[k]) for k, r in enumerate(ins)], sems)
    _, _, _, x, c = place()
    for core in range(2):
        half = lax.rem(c + core, 2)
        for d in range(4):
            at = pl.multiple_of((2 * lax.rem(x - d + 4, 4) + half) * 128, 128)
            moves[4 * core + d].wait()
            out[pl.ds(at, 128), :] = held[4 * core + d].astype(f32).T.astype(bf16)


def project_out(g, w, out):
    for k in range(2):
        rows = jnp.concatenate([g[8 * k + j].reshape(SEQS * PIECE, 128) for j in range(8)], axis=1)
        out[128 * k : 128 * k + 128, :] = dot(rows, w[...]).astype(bf16)


def struct(shape, kind=bf16):
    return jax.ShapeDtypeStruct(shape, kind)


def local(
    tokens,
    norm_gain,
    x_weight,
    z_weight,
    b_weight,
    c_weight,
    dt_weight,
    x_conv,
    b_conv,
    c_conv,
    dt_bias,
    decay_rate,
    out_gain,
    out_weight,
):
    even = lax.axis_index("yl") == 0
    keep = jnp.where(even, tokens[0:2], tokens[2:4])
    give = jnp.where(even, tokens[2:4], tokens[0:2])
    got = shift(give, "yl", 1)
    left_a = shift(keep, "x", 1)
    right_a = shift(keep, "x", -1)
    left_b = shift(got, "x", 1)
    right_b = shift(got, "x", -1)
    far_a = shift(left_a, "x", 1)
    far_b = shift(right_b, "x", -1)
    near = (keep, left_a, right_a, got, left_b, right_b)
    near = near + tuple(shift(v, "c", 1) for v in near)
    far = (far_a, far_b)
    far = far + tuple(shift(v, "c", 1) for v in far)

    weights = [x_weight, b_weight, c_weight, z_weight]
    weights = weights + [dt_weight.T, norm_gain.reshape(8, 128), out_weight.T]
    w_own, o_own = call(
        prepare,
        (struct((72, 512)), struct((16, 64, 128))),
        weights,
        [pltpu.VMEM(w.shape, w.dtype) for w in weights] + [pltpu.VMEM((128, 128), f32), DMA((7,))],
        hbm=range(7),
    )
    y_parts = [w_own] + [shift(w_own, ("yh", "yl"), d) for d in (1, 2, 3)]
    (w_line,) = call(gather_y, (struct((4, 72, 512)),), y_parts)
    z_parts = [w_line] + [shift(w_line, "z", d) for d in (1, 2, 3)]
    (w_in,) = call(order_in, (struct((1024, 640)),), z_parts)
    o_here = exchange(o_own, SP).reshape(1024, 128)
    outs = [o_here] + [shift(o_here, "x", d) for d in (1, 2, 3)]
    outs = outs + [shift(v, "c", 1) for v in outs]
    (w_out,) = call(
        order_out,
        (struct((1024, 1024)),),
        outs,
        [pltpu.VMEM((8, 1024, 128), bf16), DMA((8,))],
        hbm=range(8),
    )

    half = struct((SEQS, SPAN, 128))
    first = struct((SEQS, T, 128))
    state = struct((SEQS, 128, 128), f32)
    far_s = pltpu.HBM(half.shape, bf16)
    ends_s = struct((SEQS, PIECES, 128), f32)
    pieces_s = (12, SEQS, PIECE, 640)
    (done,) = call(
        project_near,
        (pltpu.HBM(pieces_s, bf16),),
        [*near, w_in],
        [pltpu.VMEM(pieces_s, bf16), DMA((3,))],
        us=4,
    )
    xb, cr, zr, dr, tail, x0 = call(
        project_far,
        (
            struct((SEQS, SPAN, 256)),
            half,
            far_s,
            half,
            struct((SEQS, HALO, 384)),
            struct((SEQS, T, 256)),
        ),
        [*far, w_in, done],
        [pltpu.VMEM((4, SEQS, PIECE, 128), bf16), DMA((104,))],
        hbm=(5,),
    )
    halo = onward(tail, 1)
    u, b, l, ends, dt0, part = call(
        span_state,
        (far_s, far_s, half, ends_s, struct((SEQS, T, 128), f32), state),
        [dt_bias, decay_rate, xb, dr, x_conv, b_conv],
        [pltpu.VMEM((HALO + SPAN, 256), f32), pltpu.VMEM((SPAN, 128), f32), pltpu.VMEM(half.shape, bf16), pltpu.VMEM(half.shape, bf16), DMA((4,))],
        us=4,
        scalars=2,
    )
    u0, b0, pack = call(
        span_first,
        (first, first, struct((SEQS, 144, 128))),
        [x0, halo, x_conv, b_conv, l, ends, dt0, part],
        [pltpu.VMEM((HALO + T, 256), f32)],
    )
    packs = [onward(pack, d) for d in range(1, SPANS)]
    y_own, cc, decay = call(
        span_own,
        (half, half, half),
        [u, b, u0, b0, l, ends, cr, zr, halo, c_conv],
        [pltpu.VMEM((HALO + SPAN, 128), f32)] + [pltpu.VMEM(half.shape, bf16)] * 3 + [DMA((6,))],
        us=6,
        hbm=(0, 1, 7),
    )
    (gated,) = call(
        finish,
        (struct((PIECES, SEQS, PIECE, 128)),),
        [*packs, y_own, cc, decay, out_gain[None]],
    )
    back = exchange(gated, GROUP)
    (out,) = call(project_out, (struct((256, 1024)),), [back, w_out])
    return out.reshape(2 * SEQS, PIECE, 1024)


def solution(mesh):
    torus = Mesh(mesh.devices.reshape(4, 2, 2, 4, 2), AXES)
    return jax.shard_map(
        local,
        mesh=torus,
        in_specs=(
            P(None, AXES, None),
            P(),
            P(SP, TP),
            P(SP, TP),
            P(SP, TP),
            P(SP, TP),
            P(SP, TP),
            P(None, TP),
            P(None, TP),
            P(None, TP),
            P(TP),
            P(TP),
            P(TP),
            P(TP, SP),
        ),
        out_specs=P(None, AXES, None),
        check_vma=False,
    )
```

```python
import jax
import jax.numpy as jnp
from jax import lax
from jax.experimental import pallas as pl
from jax.experimental.pallas import tpu as pltpu
from jax.sharding import Mesh
from jax.sharding import PartitionSpec as P


LENGTH = 8192
HEAD_P = 64
SEQS = 2
SPAN = 1024
PIECE = 64
PIECES = 16
SPANS = 8
T = 64
HALO = 16
EPS = 1e-05
AXES = ("z", "yh", "yl", "x", "c")
SP = ("z", "yh", "yl")
TP = ("x", "c")
LINE = ("z", "yh")
GROUP = ("yl", "x", "c")
bf16 = jnp.bfloat16
f32 = jnp.float32
VM = pl.BlockSpec(memory_space=pltpu.VMEM)
SM = pl.BlockSpec(memory_space=pltpu.SMEM)


HB = pl.BlockSpec(memory_space=pltpu.HBM)
DMA = pltpu.SemaphoreType.DMA


def call(body, outs, ins, scratch=(), mib=16, us=2, scalars=0, hbm=()):
    ins = [pltpu.with_memory_space_constraint(v, pltpu.HBM) if k in hbm else v for k, v in enumerate(ins)]
    return pl.pallas_call(
        body,
        out_shape=outs,
        in_specs=[SM if k < scalars else HB if k in hbm else VM for k in range(len(ins))],
        out_specs=tuple(VM if isinstance(o, jax.ShapeDtypeStruct) else HB for o in outs),
        scratch_shapes=list(scratch),
        compiler_params=pltpu.CompilerParams(vmem_limit_bytes=mib * 1024 * 1024),
        cost_estimate=pl.CostEstimate(
            flops=us * 1000000000, bytes_accessed=1 << 20, transcendentals=0
        ),
    )(*ins)


def fetch(pairs, sems):
    moves = [pltpu.make_async_copy(a, b, sems.at[k]) for k, (a, b) in enumerate(pairs)]
    for m in moves:
        m.start()
    return moves


def place():
    return [lax.axis_index(a) for a in AXES]


def shift(value, axis, d):
    n = lax.axis_size(axis)
    return lax.ppermute(value, axis, [(i, (i + d) % n) for i in range(n)])


def exchange(value, axes):
    return lax.all_to_all(value, axes, 0, 0, tiled=True)


def silu(v):
    h = 0.5 * v
    return h + h * jnp.tanh(h)


def softplus(v):
    return jnp.maximum(v, 0.0) + jnp.log1p(jnp.exp(-jnp.abs(v)))


def dot(a, b, dims=((1,), (0,))):
    return lax.dot_general(a, b, (dims, ((), ())), preferred_element_type=f32)


def prepare(*refs):
    ins, (w_out, o_out), held, (turned, sems) = refs[:7], refs[7:9], refs[9:16], refs[16:]
    moves = fetch(list(zip(ins, held)), sems)
    for m in moves:
        m.wait()
    xw, bw, cw, zw, dw, gain, ow = held
    z, yh, yl, _, _ = place()
    sp = z * 4 + yh * 2 + yl
    row = gain[pl.ds(lax.div(sp, 2), 1), :]
    first = lax.rem(sp, 2) == 0
    row = jnp.where(first, row[:, 0:64], row[:, 64:128])
    row = jnp.concatenate([row, row], axis=1)
    g = jnp.broadcast_to(row, (128, 128)).T[0:64]
    dt = dw[...].astype(f32)
    dt = jnp.concatenate([dt[0:1], dt[1:2]], axis=1) * row
    dt = jnp.broadcast_to(dt, (8, 128)).astype(bf16)
    ws = [(v[...].astype(f32) * g).astype(bf16) for v in (xw, bw, cw, zw)]
    o = ow[...]
    for j in range(4):
        w_out[0:64, 128 * j : 128 * j + 128] = ws[j]
    w_out[64:72, 0:128] = dt
    w_out[64:72, 128:512] = jnp.zeros((8, 384), bf16)
    for k in range(16):
        o_out[k] = o


def gather_y(p0, p1, p2, p3, out):
    _, yh, yl, _, _ = place()
    for d, p in enumerate((p0, p1, p2, p3)):
        out[lax.rem(2 * yh + yl - d + 4, 4)] = p[...]


def order_in(p0, p1, p2, p3, w):
    lane = lax.broadcasted_iota(jnp.int32, (64, 128), 1)
    z = lax.axis_index("z")
    for d, p in enumerate((p0, p1, p2, p3)):
        first = lax.rem(z - d + 4, 4) * 256
        for k in range(4):
            at = pl.ds(pl.multiple_of(first + 64 * k, 64), 64)
            w[at, 0:512] = p[k, 0:64, :]
            row = p[k, 64:72, 0:128].astype(f32)[0:1]
            both = jnp.broadcast_to(row, (128, 128)).T
            w[at, 512:640] = jnp.where(lane < 64, both[0:64], both[64:128]).astype(bf16)


def projected(pieces, w):
    rows = jnp.concatenate([p[...].reshape(SEQS * PIECE, 1024) for p in pieces], axis=0)
    vf = rows.astype(f32)
    r = lax.rsqrt(jnp.mean(vf * vf, axis=1, keepdims=True) + EPS)
    return (dot(rows, w[...]) * r).astype(bf16).reshape(len(pieces), SEQS, PIECE, 640)


def slots():
    _, _, yl, x, c = place()
    near, far = [], []
    for core in (c, 1 - c):
        for half in (yl, 1 - yl):
            for d in (0, 1, 3, 2):
                at = ((half * 4 + lax.rem(x - d + 4, 4)) * 2 + core) * PIECE
                (far if d == 2 else near).append(pl.multiple_of(at, PIECE))
    return near, far


LANES = ((0, 256), (256, 128), (384, 128), (512, 128))


def project_near(*refs):
    pieces, w, outs, held, sem = refs[:12], refs[12], refs[13:17], refs[17:21], refs[21]
    near, _ = slots()
    away = []
    for k in range(3):
        part = projected(pieces[4 * k : 4 * k + 4], w)
        for j in range(4):
            at = pl.ds(near[4 * k + j], PIECE)
            for s in range(SEQS):
                moves = []
                for ref, out, (lane, n) in zip(held, outs, LANES):
                    ref[s, at, :] = part[j, s, :, lane : lane + n]
                    moves.append((ref.at[s, at, :], out.at[s, at, :]))
                away += fetch(moves, sem.at[pl.ds(len(away), 4)])
    for m in away:
        m.wait()


def project_far(*refs):
    pieces, w, ins = refs[:4], refs[4], refs[5:8]
    outs, z_far, tail, x0, sem = refs[8:11], refs[11], refs[12], refs[13], refs[14]
    _, far = slots()
    come = fetch([(a.at[s], b.at[s]) for a, b in zip(ins, outs) for s in range(SEQS)], sem)
    last = projected(pieces, w)
    z_far[...] = last[:, :, :, 384:512]
    for m in come:
        m.wait()
    for k, at in enumerate(far):
        for s in range(SEQS):
            for ref, (lane, n) in zip(outs, (LANES[0], LANES[1], LANES[3])):
                ref[s, pl.ds(at, PIECE), :] = last[k, s, :, lane : lane + n]
    xb, cr, _ = outs
    x0[...] = xb[:, 0:T, :]
    tail[:, :, 0:256] = xb[:, SPAN - HALO :, :]
    tail[:, :, 256:384] = cr[:, SPAN - HALO :, :]


def entering(halo, s, lane, end):
    z, yh, _, _, _ = place()
    v = halo[s, :, lane:end].astype(f32)
    return jnp.where(2 * z + yh == 0, jnp.zeros_like(v), v)


def convolve(ext, taps, lanes, first, count):
    out = None
    for k in range(4):
        at = HALO - 3 + k + first
        part = taps[k : k + 1, :] * ext[at : at + count, lanes]
        out = part if out is None else out + part
    return silu(out)


def span_state(bias, rates, xb, dr, x_taps, b_taps, u_out, b_out, l_out, e_out, d_out, l_first, s_out, ext, l_all, u_v, b_v, l_v, sem):
    away = []
    head = lax.broadcasted_iota(jnp.int32, (1, 128), 1) < HEAD_P
    dtb = jnp.where(head, bias[0], bias[1])
    rate = jnp.where(head, rates[0], rates[1])
    row = lax.broadcasted_iota(jnp.int32, (T, 2 * T), 0)
    col = lax.broadcasted_iota(jnp.int32, (T, 2 * T), 1)
    tri = (lax.rem(col, T) <= row).astype(bf16)
    for s in range(SEQS):
        ext[HALO:, :] = xb[s].astype(f32)
        dt = softplus(dr[s].astype(f32) + dtb)
        ld = -(dt * rate) / LENGTH
        hi = ld.astype(bf16)
        lo = (ld - hi.astype(f32)).astype(bf16)
        total = jnp.zeros((1, 128), f32)
        for k in range(SPAN // T):
            at = slice(k * T, k * T + T)
            lc = dot(tri, jnp.concatenate([hi[at], lo[at]], axis=0))
            l_v[s, at, :] = lc.astype(bf16)
            l_all[at, :] = lc + total
            total = lc[T - 1 : T, :] + total
            e_out[s, k : k + 1, :] = total
        d_out[s] = dt[0:T]
        l_first[s] = l_v[s, 0:T, :]
        away += fetch([(l_v.at[s], l_out.at[s])], sem.at[pl.ds(4 + s, 1)])
        u = convolve(ext, x_taps, slice(0, 128), T, SPAN - T) * dt[T:]
        b = convolve(ext, b_taps, slice(128, 256), T, SPAN - T).astype(bf16)
        u_v[s, T:, :] = u.astype(bf16)
        b_v[s, T:, :] = b
        late_rows = pl.ds(T, SPAN - T)
        ready = [(u_v.at[s, late_rows, :], u_out.at[s, late_rows, :]), (b_v.at[s, late_rows, :], b_out.at[s, late_rows, :])]
        away += fetch(ready, sem.at[pl.ds(2 * s, 2)])
        late = (u * jnp.exp(total - l_all[T:, :])).astype(bf16)
        s_out[s] = dot(b, late, ((0,), (0,)))
    for m in away:
        m.wait()


def span_first(x0, halo, x_taps, b_taps, l, ends, dt, part, u_out, b_out, pack, ext):
    for s in range(SEQS):
        ext[0:HALO, :] = entering(halo, s, 0, 256)
        ext[HALO:, :] = x0[s].astype(f32)
        total = ends[s, PIECES - 1 : PIECES, :]
        u = convolve(ext, x_taps, slice(0, 128), 0, T) * dt[s]
        b = convolve(ext, b_taps, slice(128, 256), 0, T).astype(bf16)
        u_out[s] = u.astype(bf16)
        b_out[s] = b
        late = (u * jnp.exp(total - l[s].astype(f32))).astype(bf16)
        state = (part[s] + dot(b, late, ((0,), (0,)))).astype(bf16)
        t_hi = total.astype(bf16).astype(f32)
        which = lax.broadcasted_iota(jnp.int32, (16, 128), 0)
        both = jnp.where(which == 0, t_hi, jnp.where(which == 1, total - t_hi, 0.0))
        both = both.astype(bf16)
        for k in range(SPANS):
            pack[k, s, 0:128, :] = state
            pack[k, s, 128:144, :] = both


def span_own(u, b, u0, b0, l, ends, cr, zr, z_far, halo, taps, y_out, c_out, e_out, ext, uv, bv, lv, zv, sem):
    come = []
    for s in range(SEQS):
        later = pl.ds(T, SPAN - T)
        moves = [(zr.at[s], zv.at[s]), (l.at[s], lv.at[s])]
        moves += [(u.at[s, later, :], uv.at[s, later, :]), (b.at[s, later, :], bv.at[s, later, :])]
        come.append(fetch(moves, sem.at[pl.ds(4 * s, 4)]))
    row = lax.broadcasted_iota(jnp.int32, (T, 128), 0)
    col = lax.rem(lax.broadcasted_iota(jnp.int32, (T, 128), 1), T)
    seen = col <= row
    up = (row <= col).astype(f32)
    left = lax.broadcasted_iota(jnp.int32, (T, 128), 1) < T
    for s in range(SEQS):
        ext[0:HALO, :] = entering(halo, s, 256, 384)
        ext[HALO:, :] = cr[s].astype(f32)
        c_out[s] = convolve(ext, taps, slice(0, 128), 0, SPAN).astype(bf16)
        for m in come[s]:
            m.wait()
        for k, at in enumerate(slots()[1]):
            zv[s, pl.ds(at, PIECE), :] = z_far[k, s]
        state = jnp.zeros((128, 128), f32)
        for k in range(SPAN // T):
            at = slice(k * T, k * T + T)
            lc = lv[s, at, :].astype(f32)
            uc = u0[s] if k == 0 else uv[s, at, :]
            bc = b0[s] if k == 0 else bv[s, at, :]
            cc = c_out[s, at, :]
            step = lc - jnp.concatenate([jnp.zeros((1, 128), f32), lc[0 : T - 1, :]], axis=0)
            l_row = jnp.sum(step * up, axis=0, keepdims=True)
            pairs = dot(cc, jnp.concatenate([bc, bc], axis=0), ((1,), (1,)))
            gap = jnp.exp(jnp.where(seen, lc - l_row, -jnp.inf))
            m = (pairs * gap).astype(bf16)
            zero = jnp.zeros_like(uc)
            blocks = jnp.concatenate([jnp.where(left, uc, zero), jnp.where(left, zero, uc)], axis=0)
            y = dot(m, blocks)
            gate = silu(zv[s, at, :].astype(f32))
            here = jnp.exp(lc)
            if k > 0:
                y = y + dot(cc, state.astype(bf16)) * here
                e_out[s, at, :] = (gate * here * jnp.exp(ends[s, k - 1 : k, :])).astype(bf16)
            else:
                e_out[s, at, :] = (gate * here).astype(bf16)
            y_out[s, at, :] = (y * gate).astype(bf16)
            end = lc[T - 1 : T, :]
            if k + 1 < SPAN // T:
                late = (uc.astype(f32) * jnp.exp(end - lc)).astype(bf16)
                state = state * jnp.exp(end) + dot(bc, late, ((0,), (0,)))


def finish(packs, y_own, cc, decay, gain, out):
    z, yh, _, _, _ = place()
    me = z * 2 + yh
    for s in range(SEQS):
        state = jnp.zeros((128, 128), f32)
        for j in range(SPANS - 1):
            log = packs[j, s, 128:129, :].astype(f32) + packs[j, s, 129:130, :].astype(f32)
            then = state * jnp.exp(log) + packs[j, s, 0:128, :].astype(f32)
            state = jnp.where(j < me, then, state)
        g = y_own[s].astype(f32) + dot(cc[s], state.astype(bf16)) * decay[s].astype(f32)
        g = g * lax.rsqrt(jnp.mean(g * g, axis=1, keepdims=True) + EPS) * gain[...]
        g = g.astype(bf16)
        for k in range(PIECES):
            out[k, s] = g[k * PIECE : k * PIECE + PIECE, :]


def order_out(*refs):
    ins, out, held, sems = refs[:8], refs[8], refs[9], refs[10]
    moves = fetch([(r, held.at[k]) for k, r in enumerate(ins)], sems)
    _, _, _, x, c = place()
    for core in range(2):
        half = lax.rem(c + core, 2)
        for d in range(4):
            at = pl.multiple_of((2 * lax.rem(x - d + 4, 4) + half) * 128, 128)
            moves[4 * core + d].wait()
            out[pl.ds(at, 128), :] = held[4 * core + d].astype(f32).T.astype(bf16)


def project_out(g, w, out):
    for k in range(2):
        rows = jnp.concatenate([g[8 * k + j].reshape(SEQS * PIECE, 128) for j in range(8)], axis=1)
        out[128 * k : 128 * k + 128, :] = dot(rows, w[...]).astype(bf16)


def struct(shape, kind=bf16):
    return jax.ShapeDtypeStruct(shape, kind)


def local(
    tokens,
    norm_gain,
    x_weight,
    z_weight,
    b_weight,
    c_weight,
    dt_weight,
    x_conv,
    b_conv,
    c_conv,
    dt_bias,
    decay_rate,
    out_gain,
    out_weight,
):
    even = lax.axis_index("yl") == 0
    keep = jnp.where(even, tokens[0:2], tokens[2:4])
    give = jnp.where(even, tokens[2:4], tokens[0:2])
    got = shift(give, "yl", 1)
    left_a = shift(keep, "x", 1)
    right_a = shift(keep, "x", -1)
    left_b = shift(got, "x", 1)
    right_b = shift(got, "x", -1)
    far_a = shift(left_a, "x", 1)
    far_b = shift(right_b, "x", -1)
    near = (keep, left_a, right_a, got, left_b, right_b)
    near = near + tuple(shift(v, "c", 1) for v in near)
    far = (far_a, far_b)
    far = far + tuple(shift(v, "c", 1) for v in far)

    weights = [x_weight, b_weight, c_weight, z_weight]
    weights = weights + [dt_weight.T, norm_gain.reshape(8, 128), out_weight.T]
    w_own, o_own = call(
        prepare,
        (struct((72, 512)), struct((16, 64, 128))),
        weights,
        [pltpu.VMEM(w.shape, w.dtype) for w in weights] + [pltpu.VMEM((128, 128), f32), DMA((7,))],
        hbm=range(7),
    )
    y_parts = [w_own] + [shift(w_own, ("yh", "yl"), d) for d in (1, 2, 3)]
    (w_line,) = call(gather_y, (struct((4, 72, 512)),), y_parts)
    z_parts = [w_line] + [shift(w_line, "z", d) for d in (1, 2, 3)]
    (w_in,) = call(order_in, (struct((1024, 640)),), z_parts)
    o_here = exchange(o_own, SP).reshape(1024, 128)
    outs = [o_here] + [shift(o_here, "x", d) for d in (1, 2, 3)]
    outs = outs + [shift(v, "c", 1) for v in outs]
    (w_out,) = call(
        order_out,
        (struct((1024, 1024)),),
        outs,
        [pltpu.VMEM((8, 1024, 128), bf16), DMA((8,))],
        hbm=range(8),
    )

    half = struct((SEQS, SPAN, 128))
    first = struct((SEQS, T, 128))
    state = struct((SEQS, 128, 128), f32)
    far_s = pltpu.HBM(half.shape, bf16)
    ends_s = struct((SEQS, PIECES, 128), f32)
    xb_s = (SEQS, SPAN, 256)
    far_xb, far_cr, zr, far_dr = call(
        project_near,
        (pltpu.HBM(xb_s, bf16), far_s, far_s, far_s),
        [*near, w_in],
        [pltpu.VMEM(xb_s, bf16)] + [pltpu.VMEM(half.shape, bf16)] * 3 + [DMA((96,))],
        us=4,
    )
    xb, cr, dr, z_far, tail, x0 = call(
        project_far,
        (
            struct(xb_s),
            half,
            half,
            struct((4, SEQS, PIECE, 128)),
            struct((SEQS, HALO, 384)),
            struct((SEQS, T, 256)),
        ),
        [*far, w_in, far_xb, far_cr, far_dr],
        [DMA((6,))],
        hbm=(5, 6, 7),
    )
    halo = shift(tail, LINE, 1)
    u, b, l, ends, dt0, l0, part = call(
        span_state,
        (far_s, far_s, far_s, ends_s, struct((SEQS, T, 128), f32), first, state),
        [dt_bias, decay_rate, xb, dr, x_conv, b_conv],
        [pltpu.VMEM((HALO + SPAN, 256), f32), pltpu.VMEM((SPAN, 128), f32)] + [pltpu.VMEM(half.shape, bf16)] * 3 + [DMA((6,))],
        us=4,
        scalars=2,
    )
    u0, b0, pack = call(
        span_first,
        (first, first, struct((SPANS, SEQS, 144, 128))),
        [x0, halo, x_conv, b_conv, l0, ends, dt0, part],
        [pltpu.VMEM((HALO + T, 256), f32)],
    )
    packs = exchange(pack, LINE)
    y_own, cc, decay = call(
        span_own,
        (half, half, half),
        [u, b, u0, b0, l, ends, cr, zr, z_far, halo, c_conv],
        [pltpu.VMEM((HALO + SPAN, 128), f32)] + [pltpu.VMEM(half.shape, bf16)] * 4 + [DMA((8,))],
        us=6,
        hbm=(0, 1, 4, 7),
    )
    (gated,) = call(
        finish,
        (struct((PIECES, SEQS, PIECE, 128)),),
        [packs, y_own, cc, decay, out_gain[None]],
    )
    back = exchange(gated, GROUP)
    (out,) = call(project_out, (struct((256, 1024)),), [back, w_out])
    return out.reshape(2 * SEQS, PIECE, 1024)


def solution(mesh):
    torus = Mesh(mesh.devices.reshape(4, 2, 2, 4, 2), AXES)
    return jax.shard_map(
        local,
        mesh=torus,
        in_specs=(
            P(None, AXES, None),
            P(),
            P(SP, TP),
            P(SP, TP),
            P(SP, TP),
            P(SP, TP),
            P(SP, TP),
            P(None, TP),
            P(None, TP),
            P(None, TP),
            P(TP),
            P(TP),
            P(TP),
            P(TP, SP),
        ),
        out_specs=P(None, AXES, None),
        check_vma=False,
    )
```

```python
import jax
import jax.numpy as jnp
from jax import lax
from jax.experimental import pallas as pl
from jax.experimental.pallas import tpu as pltpu
from jax.sharding import Mesh
from jax.sharding import PartitionSpec as P


LENGTH = 8192
HEAD_P = 64
SEQS = 2
SPAN = 1024
PIECE = 64
PIECES = 16
SPANS = 8
T = 64
HALO = 16
EPS = 1e-05
AXES = ("z", "yh", "yl", "x", "c")
SP = ("z", "yh", "yl")
TP = ("x", "c")
LINE = ("z", "yh")
GROUP = ("yl", "x", "c")
bf16 = jnp.bfloat16
f32 = jnp.float32
VM = pl.BlockSpec(memory_space=pltpu.VMEM)
SM = pl.BlockSpec(memory_space=pltpu.SMEM)


HB = pl.BlockSpec(memory_space=pltpu.HBM)
DMA = pltpu.SemaphoreType.DMA


def call(body, outs, ins, scratch=(), mib=16, us=2, scalars=0, hbm=()):
    ins = [pltpu.with_memory_space_constraint(v, pltpu.HBM) if k in hbm else v for k, v in enumerate(ins)]
    return pl.pallas_call(
        body,
        out_shape=outs,
        in_specs=[SM if k < scalars else HB if k in hbm else VM for k in range(len(ins))],
        out_specs=tuple(VM if isinstance(o, jax.ShapeDtypeStruct) else HB for o in outs),
        scratch_shapes=list(scratch),
        compiler_params=pltpu.CompilerParams(vmem_limit_bytes=mib * 1024 * 1024),
        cost_estimate=pl.CostEstimate(
            flops=us * 1000000000, bytes_accessed=1 << 20, transcendentals=0
        ),
    )(*ins)


def fetch(pairs, sems):
    moves = [pltpu.make_async_copy(a, b, sems.at[k]) for k, (a, b) in enumerate(pairs)]
    for m in moves:
        m.start()
    return moves


def place():
    return [lax.axis_index(a) for a in AXES]


def shift(value, axis, d):
    n = lax.axis_size(axis)
    return lax.ppermute(value, axis, [(i, (i + d) % n) for i in range(n)])


def exchange(value, axes):
    return lax.all_to_all(value, axes, 0, 0, tiled=True)


def silu(v):
    h = 0.5 * v
    return h + h * jnp.tanh(h)


def softplus(v):
    return jnp.maximum(v, 0.0) + jnp.log1p(jnp.exp(-jnp.abs(v)))


def dot(a, b, dims=((1,), (0,))):
    return lax.dot_general(a, b, (dims, ((), ())), preferred_element_type=f32)


def prepare(*refs):
    ins, (w_out, o_out), held, (turned, sems) = refs[:7], refs[7:9], refs[9:16], refs[16:]
    moves = fetch(list(zip(ins, held)), sems)
    for m in moves:
        m.wait()
    xw, bw, cw, zw, dw, gain, ow = held
    z, yh, yl, _, _ = place()
    sp = z * 4 + yh * 2 + yl
    row = gain[pl.ds(lax.div(sp, 2), 1), :]
    first = lax.rem(sp, 2) == 0
    row = jnp.where(first, row[:, 0:64], row[:, 64:128])
    row = jnp.concatenate([row, row], axis=1)
    g = jnp.broadcast_to(row, (128, 128)).T[0:64]
    dt = dw[...].astype(f32)
    dt = jnp.concatenate([dt[0:1], dt[1:2]], axis=1) * row
    dt = jnp.broadcast_to(dt, (8, 128)).astype(bf16)
    ws = [(v[...].astype(f32) * g).astype(bf16) for v in (xw, bw, cw, zw)]
    o = ow[...]
    for j in range(4):
        w_out[0:64, 128 * j : 128 * j + 128] = ws[j]
    w_out[64:72, 0:128] = dt
    w_out[64:72, 128:512] = jnp.zeros((8, 384), bf16)
    for k in range(16):
        o_out[k] = o


def gather_y(p0, p1, p2, p3, out):
    _, yh, yl, _, _ = place()
    for d, p in enumerate((p0, p1, p2, p3)):
        out[lax.rem(2 * yh + yl - d + 4, 4)] = p[...]


def order_in(p0, p1, p2, p3, w):
    lane = lax.broadcasted_iota(jnp.int32, (64, 128), 1)
    z = lax.axis_index("z")
    for d, p in enumerate((p0, p1, p2, p3)):
        first = lax.rem(z - d + 4, 4) * 256
        for k in range(4):
            at = pl.ds(pl.multiple_of(first + 64 * k, 64), 64)
            w[at, 0:512] = p[k, 0:64, :]
            row = p[k, 64:72, 0:128].astype(f32)[0:1]
            both = jnp.broadcast_to(row, (128, 128)).T
            w[at, 512:640] = jnp.where(lane < 64, both[0:64], both[64:128]).astype(bf16)


def projected(pieces, w):
    rows = jnp.concatenate([p[...].reshape(SEQS * PIECE, 1024) for p in pieces], axis=0)
    vf = rows.astype(f32)
    r = lax.rsqrt(jnp.mean(vf * vf, axis=1, keepdims=True) + EPS)
    return (dot(rows, w[...]) * r).astype(bf16).reshape(len(pieces), SEQS, PIECE, 640)


def slots():
    _, _, yl, x, c = place()
    near, far = [], []
    for core in (c, 1 - c):
        for half in (yl, 1 - yl):
            for d in (0, 1, 3, 2):
                at = ((half * 4 + lax.rem(x - d + 4, 4)) * 2 + core) * PIECE
                (far if d == 2 else near).append(pl.multiple_of(at, PIECE))
    return near, far


def project_all(*refs):
    pieces, w = refs[:16], refs[16]
    xb, far_c, dr, zr, tail, x0, cr, zv, sem = refs[17:]
    near, far = slots()
    places = near + far
    away = []
    for k in range(4):
        part = projected(pieces[4 * k : 4 * k + 4], w)
        for j in range(4):
            at = pl.ds(places[4 * k + j], PIECE)
            for s in range(SEQS):
                for ref, lane, n in ((xb, 0, 256), (cr, 256, 128), (zv, 384, 128), (dr, 512, 128)):
                    ref[s, at, :] = part[j, s, :, lane : lane + n]
                moves = [(cr.at[s, at, :], far_c.at[s, at, :]), (zv.at[s, at, :], zr.at[s, at, :])]
                away += fetch(moves, sem.at[pl.ds(len(away), 2)])
    x0[...] = xb[:, 0:T, :]
    tail[:, :, 0:256] = xb[:, SPAN - HALO :, :]
    tail[:, :, 256:384] = cr[:, SPAN - HALO :, :]
    for m in away:
        m.wait()


def entering(halo, s, lane, end):
    z, yh, _, _, _ = place()
    v = halo[s, :, lane:end].astype(f32)
    return jnp.where(2 * z + yh == 0, jnp.zeros_like(v), v)


def convolve(ext, taps, lanes, first, count):
    out = None
    for k in range(4):
        at = HALO - 3 + k + first
        part = taps[k : k + 1, :] * ext[at : at + count, lanes]
        out = part if out is None else out + part
    return silu(out)


def halves(v):
    hi = v.astype(bf16)
    return [hi, (v - hi.astype(f32)).astype(bf16)]


def spread(rows, groups):
    count = max(groups) + 1
    source = lax.broadcasted_iota(jnp.int32, (8 * len(rows), 128 * count), 0)
    lane = lax.broadcasted_iota(jnp.int32, (8 * len(rows), 128 * count), 1)
    hit = None
    for k, g in enumerate(groups):
        want = lane // HEAD_P - 2 * g + 8 * k
        mine = jnp.logical_and(lane // 128 == g, source == want)
        hit = mine if hit is None else jnp.logical_or(hit, mine)
    return dot(jnp.concatenate(rows, axis=0), hit.astype(f32).astype(bf16), ((0,), (0,)))


def whole(lines):
    return jnp.concatenate([lines[8 * b : 8 * b + 8] for b in range(SPAN // 128)], axis=1)


def offsets(lines):
    total, ahead = jnp.zeros((8, 1), f32), []
    for k in range(SPAN // T):
        ahead.append(total)
        end = (k % 2) * T + T - 1
        total = total + lines[8 * (k // 2) : 8 * (k // 2) + 8, end : end + 1]
    return ahead, total


def absolute(lines, ahead):
    first = lax.broadcasted_iota(jnp.int32, (8, 128), 1) < T
    parts = []
    for b in range(SPAN // 128):
        parts.append(lines[8 * b : 8 * b + 8] + jnp.where(first, ahead[2 * b], ahead[2 * b + 1]))
    return jnp.concatenate(parts, axis=1)


def span_state(bias, rates, xb, dr, x_taps, b_taps, u_out, b_out, l_out, d_out, t_out, s_out, ext, u_v, b_v, sem):
    row = lax.broadcasted_iota(jnp.int32, (8, 128), 0)
    lane = lax.broadcasted_iota(jnp.int32, (8, 128), 1)
    pick = jnp.logical_and(row < 2, lane == row * HEAD_P).astype(f32).astype(bf16)
    row = lax.broadcasted_iota(jnp.int32, (8, 1), 0)
    dtb = jnp.where(row == 0, bias[0], jnp.where(row == 1, bias[1], 0.0))
    rate = jnp.where(row == 0, rates[0], jnp.where(row == 1, rates[1], 0.0))
    row = lax.broadcasted_iota(jnp.int32, (128, 128), 0)
    col = lax.broadcasted_iota(jnp.int32, (128, 128), 1)
    sums = jnp.logical_and(row <= col, row // T == col // T).astype(f32).astype(bf16)
    away = []
    for s in range(SEQS):
        ext[HALO:, :] = xb[s].astype(f32)
        dt = softplus(dot(pick, dr[s], ((1,), (1,))) + dtb)
        ld = -(dt * rate) / LENGTH
        ld = jnp.concatenate([ld[:, 128 * b : 128 * b + 128] for b in range(SPAN // 128)], axis=0)
        both = dot(jnp.concatenate(halves(ld), axis=0), sums)
        lines = both[0:64] + both[64:128]
        l_out[s] = lines
        ahead, total = offsets(lines)
        late = dt * jnp.exp(total - absolute(lines, ahead))
        wide = spread(halves(dt) + halves(late), (0, 0, 1, 1))
        d_out[s] = wide[0:T]
        head = lax.broadcasted_iota(jnp.int32, (1, 128), 1) < HEAD_P
        t_out[s] = jnp.broadcast_to(jnp.where(head, total[0:1], total[1:2]), (8, 128))
        x = convolve(ext, x_taps, slice(0, 128), T, SPAN - T)
        u_v[s, T:, :] = (x * wide[T:, 0:128]).astype(bf16)
        b = convolve(ext, b_taps, slice(128, 256), T, SPAN - T).astype(bf16)
        b_v[s, T:, :] = b
        at = pl.ds(T, SPAN - T)
        ready = [(u_v.at[s, at, :], u_out.at[s, at, :]), (b_v.at[s, at, :], b_out.at[s, at, :])]
        away += fetch(ready, sem.at[pl.ds(2 * s, 2)])
        s_out[s] = dot(b, (x * wide[T:, 128:256]).astype(bf16), ((0,), (0,)))
    for m in away:
        m.wait()


def span_first(x0, halo, x_taps, b_taps, dt, totals, part, u_out, b_out, pack, ext):
    for s in range(SEQS):
        ext[0:HALO, :] = entering(halo, s, 0, 256)
        ext[HALO:, :] = x0[s].astype(f32)
        total = totals[s, 0:1, :]
        x = convolve(ext, x_taps, slice(0, 128), 0, T)
        b = convolve(ext, b_taps, slice(128, 256), 0, T).astype(bf16)
        u_out[s] = (x * dt[s, :, 0:128]).astype(bf16)
        b_out[s] = b
        late = (x * dt[s, :, 128:256]).astype(bf16)
        state = (part[s] + dot(b, late, ((0,), (0,)))).astype(bf16)
        t_hi = total.astype(bf16).astype(f32)
        which = lax.broadcasted_iota(jnp.int32, (16, 128), 0)
        both = jnp.where(which == 0, t_hi, jnp.where(which == 1, total - t_hi, 0.0))
        both = both.astype(bf16)
        for k in range(SPANS):
            pack[k, s, 0:128, :] = state
            pack[k, s, 128:144, :] = both


def span_own(u, b, u0, b0, l, cr, zr, halo, taps, y_out, c_out, e_out, ext, cv, uv, bv, zv, wide, sem):
    come = []
    for s in range(SEQS):
        later = pl.ds(T, SPAN - T)
        moves = [(cr.at[s], cv.at[s]), (zr.at[s], zv.at[s])]
        moves += [(u.at[s, later, :], uv.at[s, later, :]), (b.at[s, later, :], bv.at[s, later, :])]
        come.append(fetch(moves, sem.at[pl.ds(4 * s, 4)]))
    row = lax.broadcasted_iota(jnp.int32, (T, 128), 0)
    col = lax.rem(lax.broadcasted_iota(jnp.int32, (T, 128), 1), T)
    seen = col <= row
    left = lax.broadcasted_iota(jnp.int32, (T, 128), 1) < T
    first = lax.broadcasted_iota(jnp.int32, (8, 128), 1) < T
    for s in range(SEQS):
        lines = l[s]
        ahead, _ = offsets(lines)
        ends = []
        for k in range(SPAN // 128):
            v = lines[8 * k : 8 * k + 8]
            ends.append(jnp.where(first, v[:, T - 1 : T], v[:, 2 * T - 1 : 2 * T]) - v)
        flat = whole(lines)
        rows = halves(flat) + [jnp.exp(flat).astype(bf16)]
        rows = rows + [jnp.exp(jnp.concatenate(ends, axis=1)).astype(bf16)]
        rows = rows + [jnp.exp(absolute(lines, ahead)).astype(bf16)]
        wide[s] = spread(rows, (0, 0, 1, 2, 3))
    for s in range(SEQS):
        come[s][0].wait()
        ext[0:HALO, :] = entering(halo, s, 256, 384)
        ext[HALO:, :] = cv[s].astype(f32)
        c_out[s] = convolve(ext, taps, slice(0, 128), 0, SPAN).astype(bf16)
    for moves in come:
        for m in moves[1:]:
            m.wait()
    states = [None] * SEQS
    for k in range(SPAN // T):
        at = slice(k * T, k * T + T)
        for s in range(SEQS):
            uc = u0[s] if k == 0 else uv[s, at, :]
            bc = b0[s] if k == 0 else bv[s, at, :]
            cc = c_out[s, at, :]
            half = slice((k % 2) * T, (k % 2) * T + T)
            at_8 = 8 * (k // 2)
            l_row = jnp.concatenate([l[s, at_8 : at_8 + 1, half], l[s, at_8 + 1 : at_8 + 2, half]], axis=1)
            pairs = dot(cc, jnp.concatenate([bc, bc], axis=0), ((1,), (1,)))
            gap = jnp.exp(jnp.where(seen, wide[s, at, 0:128] - l_row, -jnp.inf))
            m = (pairs * gap).astype(bf16)
            zero = jnp.zeros_like(uc)
            blocks = jnp.concatenate([jnp.where(left, uc, zero), jnp.where(left, zero, uc)], axis=0)
            y = dot(m, blocks)
            gate = silu(zv[s, at, :].astype(f32))
            here = wide[s, at, 128:256]
            if k > 0:
                y = y + dot(cc, states[s].astype(bf16)) * here
            e_out[s, at, :] = (gate * wide[s, at, 384:512]).astype(bf16)
            y_out[s, at, :] = (y * gate).astype(bf16)
            if k + 1 < SPAN // T:
                late = (uc.astype(f32) * wide[s, at, 256:384]).astype(bf16)
                fresh = dot(bc, late, ((0,), (0,)))
                states[s] = fresh if k == 0 else states[s] * here[T - 1 : T, :] + fresh


def finish(packs, y_own, cc, decay, gain, out):
    z, yh, _, _, _ = place()
    me = z * 2 + yh
    for s in range(SEQS):
        state = jnp.zeros((128, 128), f32)
        for j in range(SPANS - 1):
            log = packs[j, s, 128:129, :].astype(f32) + packs[j, s, 129:130, :].astype(f32)
            then = state * jnp.exp(log) + packs[j, s, 0:128, :].astype(f32)
            state = jnp.where(j < me, then, state)
        g = y_own[s].astype(f32) + dot(cc[s], state.astype(bf16)) * decay[s].astype(f32)
        g = g * lax.rsqrt(jnp.mean(g * g, axis=1, keepdims=True) + EPS) * gain[...]
        g = g.astype(bf16)
        for k in range(PIECES):
            out[k, s] = g[k * PIECE : k * PIECE + PIECE, :]


def order_out(*refs):
    ins, out, held, sems = refs[:8], refs[8], refs[9], refs[10]
    moves = fetch([(r, held.at[k]) for k, r in enumerate(ins)], sems)
    _, _, _, x, c = place()
    for core in range(2):
        half = lax.rem(c + core, 2)
        for d in range(4):
            at = pl.multiple_of((2 * lax.rem(x - d + 4, 4) + half) * 128, 128)
            moves[4 * core + d].wait()
            out[pl.ds(at, 128), :] = held[4 * core + d].astype(f32).T.astype(bf16)


def project_out(g, w, out):
    for k in range(2):
        rows = jnp.concatenate([g[8 * k + j].reshape(SEQS * PIECE, 128) for j in range(8)], axis=1)
        out[128 * k : 128 * k + 128, :] = dot(rows, w[...]).astype(bf16)


def struct(shape, kind=bf16):
    return jax.ShapeDtypeStruct(shape, kind)


def local(
    tokens,
    norm_gain,
    x_weight,
    z_weight,
    b_weight,
    c_weight,
    dt_weight,
    x_conv,
    b_conv,
    c_conv,
    dt_bias,
    decay_rate,
    out_gain,
    out_weight,
):
    even = lax.axis_index("yl") == 0
    keep = jnp.where(even, tokens[0:2], tokens[2:4])
    give = jnp.where(even, tokens[2:4], tokens[0:2])
    got = shift(give, "yl", 1)
    left_a = shift(keep, "x", 1)
    right_a = shift(keep, "x", -1)
    left_b = shift(got, "x", 1)
    right_b = shift(got, "x", -1)
    far_a = shift(left_a, "x", 1)
    far_b = shift(right_b, "x", -1)
    near = (keep, left_a, right_a, got, left_b, right_b)
    near = near + tuple(shift(v, "c", 1) for v in near)
    far = (far_a, far_b)
    far = far + tuple(shift(v, "c", 1) for v in far)

    weights = [x_weight, b_weight, c_weight, z_weight]
    weights = weights + [dt_weight.T, norm_gain.reshape(8, 128), out_weight.T]
    w_own, o_own = call(
        prepare,
        (struct((72, 512)), struct((16, 64, 128))),
        weights,
        [pltpu.VMEM(w.shape, w.dtype) for w in weights] + [pltpu.VMEM((128, 128), f32), DMA((7,))],
        hbm=range(7),
    )
    y_parts = [w_own] + [shift(w_own, ("yh", "yl"), d) for d in (1, 2, 3)]
    (w_line,) = call(gather_y, (struct((4, 72, 512)),), y_parts)
    z_parts = [w_line] + [shift(w_line, "z", d) for d in (1, 2, 3)]
    (w_in,) = call(order_in, (struct((1024, 640)),), z_parts)
    o_here = exchange(o_own, SP).reshape(1024, 128)
    outs = [o_here] + [shift(o_here, "x", d) for d in (1, 2, 3)]
    outs = outs + [shift(v, "c", 1) for v in outs]
    (w_out,) = call(
        order_out,
        (struct((1024, 1024)),),
        outs,
        [pltpu.VMEM((8, 1024, 128), bf16), DMA((8,))],
        hbm=range(8),
    )

    half = struct((SEQS, SPAN, 128))
    first = struct((SEQS, T, 128))
    state = struct((SEQS, 128, 128), f32)
    far_s = pltpu.HBM(half.shape, bf16)
    lines = struct((SEQS, 64, 128), f32)
    totals_s = struct((SEQS, 8, 128), f32)
    first_s = struct((SEQS, T, 256), f32)
    xb, cr, dr, zr, tail, x0 = call(
        project_all,
        (
            struct((SEQS, SPAN, 256)),
            far_s,
            half,
            far_s,
            struct((SEQS, HALO, 384)),
            struct((SEQS, T, 256)),
        ),
        [*near, *far, w_in],
        [pltpu.VMEM(half.shape, bf16), pltpu.VMEM(half.shape, bf16), DMA((64,))],
        us=5,
    )
    halo = shift(tail, LINE, 1)
    u, b, l, dt0, totals, part = call(
        span_state,
        (far_s, far_s, lines, first_s, totals_s, state),
        [dt_bias, decay_rate, xb, dr, x_conv, b_conv],
        [pltpu.VMEM((HALO + SPAN, 256), f32)] + [pltpu.VMEM(half.shape, bf16)] * 2 + [DMA((4,))],
        us=4,
        scalars=2,
    )
    u0, b0, pack = call(
        span_first,
        (first, first, struct((SPANS, SEQS, 144, 128))),
        [x0, halo, x_conv, b_conv, dt0, totals, part],
        [pltpu.VMEM((HALO + T, 256), f32)],
    )
    packs = exchange(pack, LINE)
    y_own, cc, decay = call(
        span_own,
        (half, half, half),
        [u, b, u0, b0, l, cr, zr, halo, c_conv],
        [pltpu.VMEM((HALO + SPAN, 128), f32)]
        + [pltpu.VMEM(half.shape, bf16)] * 4
        + [pltpu.VMEM((SEQS, SPAN, 512), f32), DMA((8,))],
        us=6,
        hbm=(0, 1, 5, 6),
    )
    (gated,) = call(
        finish,
        (struct((PIECES, SEQS, PIECE, 128)),),
        [packs, y_own, cc, decay, out_gain[None]],
    )
    back = exchange(gated, GROUP)
    (out,) = call(project_out, (struct((256, 1024)),), [back, w_out])
    return out.reshape(2 * SEQS, PIECE, 1024)


def solution(mesh):
    torus = Mesh(mesh.devices.reshape(4, 2, 2, 4, 2), AXES)
    return jax.shard_map(
        local,
        mesh=torus,
        in_specs=(
            P(None, AXES, None),
            P(),
            P(SP, TP),
            P(SP, TP),
            P(SP, TP),
            P(SP, TP),
            P(SP, TP),
            P(None, TP),
            P(None, TP),
            P(None, TP),
            P(TP),
            P(TP),
            P(TP),
            P(TP, SP),
        ),
        out_specs=P(None, AXES, None),
        check_vma=False,
    )
```

```python
import jax
import jax.numpy as jnp
from jax import lax
from jax.experimental import pallas as pl
from jax.experimental.pallas import tpu as pltpu
from jax.sharding import Mesh
from jax.sharding import PartitionSpec as P


LENGTH = 8192
HEAD_P = 64
SEQS = 2
SPAN = 1024
PIECE = 64
PIECES = 16
SPANS = 8
T = 64
HALO = 16
EPS = 1e-05
AXES = ("z", "yh", "yl", "x", "c")
SP = ("z", "yh", "yl")
TP = ("x", "c")
LINE = ("z", "yh")
GROUP = ("yl", "x", "c")
bf16 = jnp.bfloat16
f32 = jnp.float32
VM = pl.BlockSpec(memory_space=pltpu.VMEM)
SM = pl.BlockSpec(memory_space=pltpu.SMEM)


HB = pl.BlockSpec(memory_space=pltpu.HBM)
DMA = pltpu.SemaphoreType.DMA


def call(body, outs, ins, scratch=(), mib=16, us=2, scalars=0, hbm=()):
    ins = [pltpu.with_memory_space_constraint(v, pltpu.HBM) if k in hbm else v for k, v in enumerate(ins)]
    return pl.pallas_call(
        body,
        out_shape=outs,
        in_specs=[SM if k < scalars else HB if k in hbm else VM for k in range(len(ins))],
        out_specs=tuple(VM if isinstance(o, jax.ShapeDtypeStruct) else HB for o in outs),
        scratch_shapes=list(scratch),
        compiler_params=pltpu.CompilerParams(vmem_limit_bytes=mib * 1024 * 1024),
        cost_estimate=pl.CostEstimate(
            flops=us * 1000000000, bytes_accessed=1 << 20, transcendentals=0
        ),
    )(*ins)


def fetch(pairs, sems):
    moves = [pltpu.make_async_copy(a, b, sems.at[k]) for k, (a, b) in enumerate(pairs)]
    for m in moves:
        m.start()
    return moves


def place():
    return [lax.axis_index(a) for a in AXES]


def shift(value, axis, d):
    n = lax.axis_size(axis)
    return lax.ppermute(value, axis, [(i, (i + d) % n) for i in range(n)])


def exchange(value, axes):
    return lax.all_to_all(value, axes, 0, 0, tiled=True)


def silu(v):
    h = 0.5 * v
    return h + h * jnp.tanh(h)


def softplus(v):
    return jnp.maximum(v, 0.0) + jnp.log1p(jnp.exp(-jnp.abs(v)))


def dot(a, b, dims=((1,), (0,))):
    return lax.dot_general(a, b, (dims, ((), ())), preferred_element_type=f32)


def prepare(*refs):
    ins, (w_out, o_out), held, (turned, sems) = refs[:7], refs[7:9], refs[9:16], refs[16:]
    moves = fetch(list(zip(ins, held)), sems)
    for m in moves:
        m.wait()
    xw, bw, cw, zw, dw, gain, ow = held
    z, yh, yl, _, _ = place()
    sp = z * 4 + yh * 2 + yl
    row = gain[pl.ds(lax.div(sp, 2), 1), :]
    first = lax.rem(sp, 2) == 0
    row = jnp.where(first, row[:, 0:64], row[:, 64:128])
    row = jnp.concatenate([row, row], axis=1)
    g = jnp.broadcast_to(row, (128, 128)).T[0:64]
    dt = dw[...].astype(f32)
    dt = jnp.concatenate([dt[0:1], dt[1:2]], axis=1) * row
    dt = jnp.broadcast_to(dt, (8, 128)).astype(bf16)
    ws = [(v[...].astype(f32) * g).astype(bf16) for v in (xw, bw, cw, zw)]
    o = ow[...]
    for j in range(4):
        w_out[0:64, 128 * j : 128 * j + 128] = ws[j]
    w_out[64:72, 0:128] = dt
    w_out[64:72, 128:512] = jnp.zeros((8, 384), bf16)
    for k in range(16):
        o_out[k] = o


def gather_y(p0, p1, p2, p3, out):
    _, yh, yl, _, _ = place()
    for d, p in enumerate((p0, p1, p2, p3)):
        out[lax.rem(2 * yh + yl - d + 4, 4)] = p[...]


def order_in(p0, p1, p2, p3, w, steps):
    z = lax.axis_index("z")
    for d, p in enumerate((p0, p1, p2, p3)):
        first = lax.rem(z - d + 4, 4) * 256
        for k in range(4):
            w[pl.ds(pl.multiple_of(first + 64 * k, 64), 64), :] = p[k, 0:64, :]
        at = pl.ds(pl.multiple_of(first, 256), 256)
        rows = [p[k, 64:72, 0:128].astype(f32)[0:1] for k in range(4)]
        for h in range(2):
            row = jnp.concatenate([v[:, 64 * h : 64 * h + 64] for v in rows], axis=1)
            steps[16 * h : 16 * h + 16, at] = jnp.broadcast_to(row, (16, 256)).astype(bf16)


def slots():
    _, _, yl, x, c = place()
    return [
        (half * 4 + lax.rem(x - d + 4, 4)) * 2 + core
        for core in (c, 1 - c)
        for half, d in ((yl, 0), (yl, 1), (yl, 3), (1 - yl, 0), (1 - yl, 1), (1 - yl, 3), (yl, 2), (1 - yl, 2))
    ]


def project_all(*refs):
    here, there, (w, steps) = refs[:8], refs[8:16], refs[16:18]
    xb, cr, zr, dt_out, tail, x0, held, sem = refs[18:]
    come = fetch([(a, held.at[k]) for k, a in enumerate(there[0:6])], sem)
    places = slots()
    lane = lax.broadcasted_iota(jnp.int32, (128, 128), 1)
    for k in range(2):
        if k == 1:
            for m in come:
                m.wait()
        pieces = [v[...] for v in here]
        if k == 1:
            pieces = [held[j] for j in range(6)] + [v[...] for v in there[6:8]]
        rows = jnp.concatenate([p.reshape(SEQS * PIECE, 1024) for p in pieces], axis=0)
        wide = rows.astype(f32)
        r = lax.rsqrt(jnp.mean(wide * wide, axis=1, keepdims=True) + EPS)
        part = (dot(rows, w[...]) * r).astype(bf16).reshape(8, SEQS, PIECE, 512)
        d0, d1 = (
            jnp.sum(wide * jnp.concatenate([steps[16 * h : 16 * h + 16, :]] * 64, axis=0).astype(f32), axis=1, keepdims=True) * r
            for h in range(2)
        )
        for j in range(8):
            slot = places[8 * k + j]
            at = pl.ds(pl.multiple_of(slot * PIECE, PIECE), PIECE)
            for s in range(SEQS):
                for ref, lo, n in ((xb, 0, 256), (cr, 256, 128), (zr, 384, 128)):
                    ref[s, at, :] = part[j, s, :, lo : lo + n]
            one = slice(128 * j, 128 * j + 128)
            turned = jnp.where(lane < 64, d0[one], d1[one]).T
            both = jnp.concatenate([turned[0:1], turned[64:65]], axis=0)
            for s in range(SEQS):
                dt_out[s, slot] = both[:, 64 * s : 64 * s + 64]
    x0[...] = xb[:, 0:T, :]
    tail[:, :, 0:256] = xb[:, SPAN - HALO :, :]
    tail[:, :, 256:384] = cr[:, SPAN - HALO :, :]


def entering(halo, s, lane, end):
    z, yh, _, _, _ = place()
    v = halo[s, :, lane:end].astype(f32)
    return jnp.where(2 * z + yh == 0, jnp.zeros_like(v), v)


def convolve(rows, taps):
    part = (0.5 * taps[0:1, :]) * rows
    for k in range(1, 4):
        part = (0.5 * taps[k : k + 1, :]) * rows + pltpu.roll(part, 1, 0)
    half = part[HALO:]
    return half + half * jnp.tanh(half)


def halves(v):
    hi = v.astype(bf16)
    return [hi, (v - hi.astype(f32)).astype(bf16)]


def spread(rows, groups):
    count = max(groups) + 1
    source = lax.broadcasted_iota(jnp.int32, (8 * len(rows), 128 * count), 0)
    lane = lax.broadcasted_iota(jnp.int32, (8 * len(rows), 128 * count), 1)
    hit = None
    for k, g in enumerate(groups):
        want = lane // HEAD_P - 2 * g + 8 * k
        mine = jnp.logical_and(lane // 128 == g, source == want)
        hit = mine if hit is None else jnp.logical_or(hit, mine)
    return dot(jnp.concatenate(rows, axis=0), hit.astype(f32).astype(bf16), ((0,), (0,)))


def offsets(lines):
    total, ahead = jnp.zeros((8, 1), f32), []
    for k in range(SPAN // T):
        ahead.append(total)
        end = (k % 2) * T + T - 1
        total = total + lines[8 * (k // 2) : 8 * (k // 2) + 8, end : end + 1]
    return ahead, total


def absolute(lines, ahead):
    first = lax.broadcasted_iota(jnp.int32, (8, 128), 1) < T
    parts = []
    for b in range(SPAN // 128):
        parts.append(lines[8 * b : 8 * b + 8] + jnp.where(first, ahead[2 * b], ahead[2 * b + 1]))
    return jnp.concatenate(parts, axis=0)


def span_state(
    bias, rates, xb, cr, zr, raw, x_taps, b_taps,
    u_out, b_out, c_out, z_out, l_out, d_out, t_out, s_out,
    u_v, b_v, late_v, wide, sem,
):
    away = fetch([(cr, c_out), (zr, z_out)], sem.at[pl.ds(0, 2)])
    row = lax.rem(lax.broadcasted_iota(jnp.int32, (64, 1), 0), 8)
    dtb = jnp.where(row == 0, bias[0], jnp.where(row == 1, bias[1], 0.0))
    rate = jnp.where(row == 0, rates[0], jnp.where(row == 1, rates[1], 0.0))
    row = lax.broadcasted_iota(jnp.int32, (128, 128), 0)
    col = lax.broadcasted_iota(jnp.int32, (128, 128), 1)
    sums = jnp.logical_and(row <= col, row // T == col // T).astype(f32).astype(bf16)
    none = jnp.zeros((6, 128), f32)
    for s in range(SEQS):
        steps = []
        for b in range(SPAN // 128):
            steps += [jnp.concatenate([raw[s, 2 * b], raw[s, 2 * b + 1]], axis=1), none]
        dt = softplus(jnp.concatenate(steps, axis=0) + dtb)
        ld = -(dt * rate) / LENGTH
        both = dot(jnp.concatenate(halves(ld), axis=0), sums)
        lines = both[0:64] + both[64:128]
        l_out[s] = lines
        ahead, total = offsets(lines)
        total_all = jnp.concatenate([total] * 8, axis=0)
        late = dt * jnp.exp(total_all - absolute(lines, ahead))
        rows = halves(dt) + halves(late)
        for b in range(SPAN // 128):
            block = [v[8 * b : 8 * b + 8] for v in rows]
            wide[128 * b : 128 * b + 128, :] = spread(block, (0, 0, 1, 1))
        d_out[s] = wide[0:T]
        head = lax.broadcasted_iota(jnp.int32, (1, 128), 1) < HEAD_P
        t_out[s] = jnp.broadcast_to(jnp.where(head, total[0:1], total[1:2]), (8, 128))
        for first in range(T, SPAN, 128):
            last = min(first + 128, SPAN)
            rows = xb[s, first - HALO : last, :].astype(f32)
            x = convolve(rows[:, 0:128], x_taps)
            u_v[s, first:last, :] = (x * wide[first:last, 0:128]).astype(bf16)
            late_v[first:last, :] = (x * wide[first:last, 128:256]).astype(bf16)
            b_v[s, first:last, :] = convolve(rows[:, 128:256], b_taps).astype(bf16)
        at = pl.ds(T, SPAN - T)
        ready = [(u_v.at[s, at, :], u_out.at[s, at, :]), (b_v.at[s, at, :], b_out.at[s, at, :])]
        away += fetch(ready, sem.at[pl.ds(2 + 2 * s, 2)])
        s_out[s] = dot(b_v[s, T:, :], late_v[T:, :], ((0,), (0,)))
    for m in away:
        m.wait()


def span_first(x0, halo, x_taps, b_taps, dt, totals, part, u_out, b_out, pack):
    for s in range(SEQS):
        rows = jnp.concatenate([entering(halo, s, 0, 256), x0[s].astype(f32)], axis=0)
        total = totals[s, 0:1, :]
        x = convolve(rows[:, 0:128], x_taps)
        b = convolve(rows[:, 128:256], b_taps).astype(bf16)
        u_out[s] = (x * dt[s, :, 0:128]).astype(bf16)
        b_out[s] = b
        late = (x * dt[s, :, 128:256]).astype(bf16)
        state = (part[s] + dot(b, late, ((0,), (0,)))).astype(bf16)
        t_hi = total.astype(bf16).astype(f32)
        which = lax.broadcasted_iota(jnp.int32, (16, 128), 0)
        both = jnp.where(which == 0, t_hi, jnp.where(which == 1, total - t_hi, 0.0))
        both = both.astype(bf16)
        for k in range(SPANS):
            pack[k, s, 0:128, :] = state
            pack[k, s, 128:144, :] = both


def span_own(u, b, u0, b0, l, cr, zr, halo, taps, y_out, c_out, e_out, cv, uv, bv, zv, wide, sem):
    come = []
    for s in range(SEQS):
        later = pl.ds(T, SPAN - T)
        moves = [(cr.at[s], cv.at[s]), (zr.at[s], zv.at[s])]
        moves += [(u.at[s, later, :], uv.at[s, later, :]), (b.at[s, later, :], bv.at[s, later, :])]
        come.append(fetch(moves, sem.at[pl.ds(4 * s, 4)]))
    row = lax.broadcasted_iota(jnp.int32, (T, 128), 0)
    col = lax.rem(lax.broadcasted_iota(jnp.int32, (T, 128), 1), T)
    seen = col <= row
    left = lax.broadcasted_iota(jnp.int32, (T, 128), 1) < T
    first = lax.broadcasted_iota(jnp.int32, (8, 128), 1) < T
    for s in range(SEQS):
        lines = l[s]
        ahead, _ = offsets(lines)
        past = absolute(lines, ahead)
        for k in range(SPAN // 128):
            v = lines[8 * k : 8 * k + 8]
            rest = jnp.where(first, v[:, T - 1 : T], v[:, 2 * T - 1 : 2 * T]) - v
            rows = halves(v)
            rows += [jnp.exp(r).astype(bf16) for r in (v, rest, past[8 * k : 8 * k + 8])]
            wide[s, 128 * k : 128 * k + 128, :] = spread(rows, (0, 0, 1, 2, 3))
    for s in range(SEQS):
        come[s][0].wait()
        for k in range(0, SPAN, 128):
            if k == 0:
                rows = jnp.concatenate([entering(halo, s, 256, 384), cv[s, 0:128, :].astype(f32)], axis=0)
            else:
                rows = cv[s, k - HALO : k + 128, :].astype(f32)
            c_out[s, k : k + 128, :] = convolve(rows, taps).astype(bf16)
    for moves in come:
        for m in moves[1:]:
            m.wait()
    states = [None] * SEQS
    for k in range(SPAN // T):
        at = slice(k * T, k * T + T)
        for s in range(SEQS):
            uc = u0[s] if k == 0 else uv[s, at, :]
            bc = b0[s] if k == 0 else bv[s, at, :]
            cc = c_out[s, at, :]
            half = slice((k % 2) * T, (k % 2) * T + T)
            at_8 = 8 * (k // 2)
            l_row = jnp.concatenate([l[s, at_8 : at_8 + 1, half], l[s, at_8 + 1 : at_8 + 2, half]], axis=1)
            pairs = dot(cc, jnp.concatenate([bc, bc], axis=0), ((1,), (1,)))
            gap = jnp.exp(jnp.where(seen, wide[s, at, 0:128] - l_row, -jnp.inf))
            m = (pairs * gap).astype(bf16)
            zero = jnp.zeros_like(uc)
            blocks = jnp.concatenate([jnp.where(left, uc, zero), jnp.where(left, zero, uc)], axis=0)
            y = dot(m, blocks)
            gate = silu(zv[s, at, :].astype(f32))
            here = wide[s, at, 128:256]
            if k > 0:
                y = y + dot(cc, states[s].astype(bf16)) * here
            e_out[s, at, :] = (gate * wide[s, at, 384:512]).astype(bf16)
            y_out[s, at, :] = (y * gate).astype(bf16)
            if k + 1 < SPAN // T:
                late = (uc.astype(f32) * wide[s, at, 256:384]).astype(bf16)
                fresh = dot(bc, late, ((0,), (0,)))
                states[s] = fresh if k == 0 else states[s] * here[T - 1 : T, :] + fresh


def finish(packs, y_own, cc, decay, gain, out):
    z, yh, _, _, _ = place()
    me = z * 2 + yh
    for s in range(SEQS):
        state = jnp.zeros((128, 128), f32)
        for j in range(SPANS - 1):
            log = packs[j, s, 128:129, :].astype(f32) + packs[j, s, 129:130, :].astype(f32)
            then = state * jnp.exp(log) + packs[j, s, 0:128, :].astype(f32)
            state = jnp.where(j < me, then, state)
        g = y_own[s].astype(f32) + dot(cc[s], state.astype(bf16)) * decay[s].astype(f32)
        g = g * lax.rsqrt(jnp.mean(g * g, axis=1, keepdims=True) + EPS) * gain[...]
        g = g.astype(bf16)
        for k in range(PIECES):
            out[k, s] = g[k * PIECE : k * PIECE + PIECE, :]


def order_out(*refs):
    ins, out, held, sems = refs[:8], refs[8], refs[9], refs[10]
    moves = fetch([(r, held.at[k]) for k, r in enumerate(ins)], sems)
    _, _, _, x, c = place()
    for core in range(2):
        half = lax.rem(c + core, 2)
        for d in range(4):
            at = pl.multiple_of((2 * lax.rem(x - d + 4, 4) + half) * 128, 128)
            moves[4 * core + d].wait()
            out[pl.ds(at, 128), :] = held[4 * core + d].astype(f32).T.astype(bf16)


def project_out(g, w, out):
    for k in range(2):
        rows = jnp.concatenate([g[8 * k + j].reshape(SEQS * PIECE, 128) for j in range(8)], axis=1)
        out[128 * k : 128 * k + 128, :] = dot(rows, w[...]).astype(bf16)


def struct(shape, kind=bf16):
    return jax.ShapeDtypeStruct(shape, kind)


def local(
    tokens,
    norm_gain,
    x_weight,
    z_weight,
    b_weight,
    c_weight,
    dt_weight,
    x_conv,
    b_conv,
    c_conv,
    dt_bias,
    decay_rate,
    out_gain,
    out_weight,
):
    even = lax.axis_index("yl") == 0
    keep = jnp.where(even, tokens[0:2], tokens[2:4])
    give = jnp.where(even, tokens[2:4], tokens[0:2])
    got = shift(give, "yl", 1)
    left_a = shift(keep, "x", 1)
    right_a = shift(keep, "x", -1)
    left_b = shift(got, "x", 1)
    right_b = shift(got, "x", -1)
    far_a = shift(left_a, "x", 1)
    far_b = shift(right_b, "x", -1)
    here = (keep, left_a, right_a, got, left_b, right_b, far_a, far_b)
    there = tuple(shift(v, "c", 1) for v in here)

    weights = [x_weight, b_weight, c_weight, z_weight]
    weights = weights + [dt_weight.T, norm_gain.reshape(8, 128), out_weight.T]
    w_own, o_own = call(
        prepare,
        (struct((72, 512)), struct((16, 64, 128))),
        weights,
        [pltpu.VMEM(w.shape, w.dtype) for w in weights] + [pltpu.VMEM((128, 128), f32), DMA((7,))],
        hbm=range(7),
    )
    y_parts = [w_own] + [shift(w_own, ("yh", "yl"), d) for d in (1, 2, 3)]
    (w_line,) = call(gather_y, (struct((4, 72, 512)),), y_parts)
    z_parts = [w_line] + [shift(w_line, "z", d) for d in (1, 2, 3)]
    w_in, steps = call(order_in, (struct((1024, 512)), struct((32, 1024))), z_parts)
    o_here = exchange(o_own, SP).reshape(1024, 128)
    outs = [o_here] + [shift(o_here, "x", d) for d in (1, 2, 3)]
    outs = outs + [shift(v, "c", 1) for v in outs]
    (w_out,) = call(
        order_out,
        (struct((1024, 1024)),),
        outs,
        [pltpu.VMEM((8, 1024, 128), bf16), DMA((8,))],
        hbm=range(1, 8),
    )

    half = struct((SEQS, SPAN, 128))
    first = struct((SEQS, T, 128))
    state = struct((SEQS, 128, 128), f32)
    far_s = pltpu.HBM(half.shape, bf16)
    lines = struct((SEQS, 64, 128), f32)
    totals_s = struct((SEQS, 8, 128), f32)
    first_s = struct((SEQS, T, 256), f32)
    xb, cr, zr, raw, tail, x0 = call(
        project_all,
        (
            struct((SEQS, SPAN, 256)),
            half,
            half,
            struct((SEQS, PIECES, 2, PIECE), f32),
            struct((SEQS, HALO, 384)),
            struct((SEQS, T, 256)),
        ),
        [*here, *there, w_in, steps],
        [pltpu.VMEM((6, SEQS, PIECE, 1024), bf16), DMA((6,))],
        us=5,
        hbm=range(8, 14),
    )
    halo = shift(tail, LINE, 1)
    u, b, far_c, far_z, l, dt0, totals, part = call(
        span_state,
        (far_s, far_s, far_s, far_s, lines, first_s, totals_s, state),
        [dt_bias, decay_rate, xb, cr, zr, raw, x_conv, b_conv],
        [pltpu.VMEM(half.shape, bf16)] * 2
        + [pltpu.VMEM((SPAN, 128), bf16), pltpu.VMEM((SPAN, 256), f32), DMA((6,))],
        us=4,
        scalars=2,
    )
    u0, b0, pack = call(
        span_first,
        (first, first, struct((SPANS, SEQS, 144, 128))),
        [x0, halo, x_conv, b_conv, dt0, totals, part],
    )
    packs = exchange(pack, LINE)
    y_own, cc, decay = call(
        span_own,
        (half, half, half),
        [u, b, u0, b0, l, far_c, far_z, halo, c_conv],
        [pltpu.VMEM(half.shape, bf16)] * 4
        + [pltpu.VMEM((SEQS, SPAN, 512), f32), DMA((8,))],
        us=6,
        hbm=(0, 1, 5, 6),
    )
    (gated,) = call(
        finish,
        (struct((PIECES, SEQS, PIECE, 128)),),
        [packs, y_own, cc, decay, out_gain[None]],
    )
    back = exchange(gated, GROUP)
    (out,) = call(project_out, (struct((256, 1024)),), [back, w_out])
    return out.reshape(2 * SEQS, PIECE, 1024)


def solution(mesh):
    torus = Mesh(mesh.devices.reshape(4, 2, 2, 4, 2), AXES)
    return jax.shard_map(
        local,
        mesh=torus,
        in_specs=(
            P(None, AXES, None),
            P(),
            P(SP, TP),
            P(SP, TP),
            P(SP, TP),
            P(SP, TP),
            P(SP, TP),
            P(None, TP),
            P(None, TP),
            P(None, TP),
            P(TP),
            P(TP),
            P(TP),
            P(TP, SP),
        ),
        out_specs=P(None, AXES, None),
        check_vma=False,
    )
```

```python
import jax
import jax.numpy as jnp
from jax import lax
from jax.experimental import pallas as pl
from jax.experimental.pallas import tpu as pltpu
from jax.sharding import Mesh
from jax.sharding import PartitionSpec as P


LENGTH = 8192
HEAD_P = 64
SEQS = 2
SPAN = 1024
PIECE = 64
PIECES = 16
SPANS = 8
T = 64
HALO = 16
EPS = 1e-05
AXES = ("z", "yh", "yl", "x", "c")
SP = ("z", "yh", "yl")
TP = ("x", "c")
LINE = ("z", "yh")
GROUP = ("yl", "x", "c")
bf16 = jnp.bfloat16
f32 = jnp.float32
VM = pl.BlockSpec(memory_space=pltpu.VMEM)
SM = pl.BlockSpec(memory_space=pltpu.SMEM)


HB = pl.BlockSpec(memory_space=pltpu.HBM)
DMA = pltpu.SemaphoreType.DMA


def call(body, outs, ins, scratch=(), mib=16, us=2, scalars=0, hbm=()):
    ins = [pltpu.with_memory_space_constraint(v, pltpu.HBM) if k in hbm else v for k, v in enumerate(ins)]
    return pl.pallas_call(
        body,
        out_shape=outs,
        in_specs=[SM if k < scalars else HB if k in hbm else VM for k in range(len(ins))],
        out_specs=tuple(VM if isinstance(o, jax.ShapeDtypeStruct) else HB for o in outs),
        scratch_shapes=list(scratch),
        compiler_params=pltpu.CompilerParams(vmem_limit_bytes=mib * 1024 * 1024),
        cost_estimate=pl.CostEstimate(
            flops=us * 1000000000, bytes_accessed=1 << 20, transcendentals=0
        ),
    )(*ins)


def fetch(pairs, sems):
    moves = [pltpu.make_async_copy(a, b, sems.at[k]) for k, (a, b) in enumerate(pairs)]
    for m in moves:
        m.start()
    return moves


def place():
    return [lax.axis_index(a) for a in AXES]


def shift(value, axis, d):
    n = lax.axis_size(axis)
    return lax.ppermute(value, axis, [(i, (i + d) % n) for i in range(n)])


def exchange(value, axes):
    return lax.all_to_all(value, axes, 0, 0, tiled=True)


def silu(v):
    h = 0.5 * v
    return h + h * jnp.tanh(h)


def softplus(v):
    return jnp.maximum(v, 0.0) + jnp.log1p(jnp.exp(-jnp.abs(v)))


def dot(a, b, dims=((1,), (0,))):
    return lax.dot_general(a, b, (dims, ((), ())), preferred_element_type=f32)


def prepare(*refs):
    ins, w_out, held, sems = refs[:7], refs[7], refs[8:15], refs[15]
    moves = fetch(list(zip(ins, held)), sems)
    for m in moves:
        m.wait()
    xw, bw, cw, zw, dw, gain, ow = held
    z, yh, yl, _, _ = place()
    sp = z * 4 + yh * 2 + yl
    row = gain[pl.ds(lax.div(sp, 2), 1), :]
    first = lax.rem(sp, 2) == 0
    row = jnp.where(first, row[:, 0:64], row[:, 64:128])
    row = jnp.concatenate([row, row], axis=1)
    g = jnp.broadcast_to(row, (128, 128)).T[0:64]
    dt = dw[...].astype(f32)
    dt = jnp.concatenate([dt[0:1], dt[1:2]], axis=1) * row
    dt = jnp.broadcast_to(dt, (8, 128)).astype(bf16)
    ws = [(v[...].astype(f32) * g).astype(bf16) for v in (xw, bw, cw, zw)]
    o = ow[...]
    for j in range(4):
        w_out[0:64, 128 * j : 128 * j + 128] = ws[j]
    w_out[64:72, 0:128] = dt
    w_out[64:72, 128:512] = jnp.zeros((8, 384), bf16)
    for j in range(4):
        w_out[72:88, 128 * j : 128 * j + 128] = o[16 * j : 16 * j + 16]


def gather_y(p0, p1, p2, p3, out, o_out):
    _, yh, yl, _, _ = place()
    for d, p in enumerate((p0, p1, p2, p3)):
        at = lax.rem(2 * yh + yl - d + 4, 4)
        out[at] = p[0:72, :]
        for j in range(4):
            o_out[at, 16 * j : 16 * j + 16, :] = p[72:88, 128 * j : 128 * j + 128]


def order_in(p0, p1, p2, p3, w, steps):
    z = lax.axis_index("z")
    for d, p in enumerate((p0, p1, p2, p3)):
        first = lax.rem(z - d + 4, 4) * 256
        for k in range(4):
            w[pl.ds(pl.multiple_of(first + 64 * k, 64), 64), :] = p[k, 0:64, :]
        at = pl.ds(pl.multiple_of(first, 256), 256)
        rows = [p[k, 64:72, 0:128].astype(f32)[0:1] for k in range(4)]
        for h in range(2):
            row = jnp.concatenate([v[:, 64 * h : 64 * h + 64] for v in rows], axis=1)
            steps[16 * h : 16 * h + 16, at] = jnp.broadcast_to(row, (16, 256)).astype(bf16)


def slots():
    _, _, yl, x, c = place()
    return [
        (half * 4 + lax.rem(x - d + 4, 4)) * 2 + core
        for core in (c, 1 - c)
        for half, d in ((yl, 0), (yl, 1), (yl, 3), (1 - yl, 0), (1 - yl, 1), (1 - yl, 3), (yl, 2), (1 - yl, 2))
    ]


def project_all(*refs):
    here, there, (w, steps), o_parts = refs[:8], refs[8:16], refs[16:18], refs[18:22]
    xb, cr, zr, dt_out, tail, x0, o_out, sem = refs[22:]
    z = lax.axis_index("z")
    moves = []
    for d, p in enumerate(o_parts):
        for k in range(4):
            at = pl.multiple_of(lax.rem(z - d + 4, 4) * 256 + 64 * k, 64)
            moves.append((p.at[k], o_out.at[pl.ds(at, 64), :]))
    away = fetch(moves, sem)
    places = slots()
    lane = lax.broadcasted_iota(jnp.int32, (128, 128), 1)
    for k in range(2):
        pieces = [v[...] for v in (here, there)[k]]
        rows = jnp.concatenate([p.reshape(SEQS * PIECE, 1024) for p in pieces], axis=0)
        wide = rows.astype(f32)
        r = lax.rsqrt(jnp.mean(wide * wide, axis=1, keepdims=True) + EPS)
        part = (dot(rows, w[...]) * r).astype(bf16).reshape(8, SEQS, PIECE, 512)
        d0, d1 = (
            jnp.sum(wide * jnp.concatenate([steps[16 * h : 16 * h + 16, :]] * 64, axis=0).astype(f32), axis=1, keepdims=True) * r
            for h in range(2)
        )
        for j in range(8):
            slot = places[8 * k + j]
            at = pl.ds(pl.multiple_of(slot * PIECE, PIECE), PIECE)
            for s in range(SEQS):
                for ref, lo, n in ((xb, 0, 256), (cr, 256, 128), (zr, 384, 128)):
                    ref[s, at, :] = part[j, s, :, lo : lo + n]
            one = slice(128 * j, 128 * j + 128)
            turned = jnp.where(lane < 64, d0[one], d1[one]).T
            both = jnp.concatenate([turned[0:1], turned[64:65]], axis=0)
            for s in range(SEQS):
                dt_out[s, slot] = both[:, 64 * s : 64 * s + 64]
    x0[...] = xb[:, 0:T, :]
    tail[:, :, 0:256] = xb[:, SPAN - HALO :, :]
    tail[:, :, 256:384] = cr[:, SPAN - HALO :, :]
    for m in away:
        m.wait()


def entering(halo, s, lane, end):
    z, yh, _, _, _ = place()
    v = halo[s, :, lane:end].astype(f32)
    return jnp.where(2 * z + yh == 0, jnp.zeros_like(v), v)


def convolve(rows, taps):
    part = (0.5 * taps[0:1, :]) * rows
    for k in range(1, 4):
        part = (0.5 * taps[k : k + 1, :]) * rows + pltpu.roll(part, 1, 0)
    half = part[HALO:]
    return half + half * jnp.tanh(half)


def halves(v):
    hi = v.astype(bf16)
    return [hi, (v - hi.astype(f32)).astype(bf16)]


def spread(rows, groups):
    count = max(groups) + 1
    source = lax.broadcasted_iota(jnp.int32, (8 * len(rows), 128 * count), 0)
    lane = lax.broadcasted_iota(jnp.int32, (8 * len(rows), 128 * count), 1)
    hit = None
    for k, g in enumerate(groups):
        want = lane // HEAD_P - 2 * g + 8 * k
        mine = jnp.logical_and(lane // 128 == g, source == want)
        hit = mine if hit is None else jnp.logical_or(hit, mine)
    return dot(jnp.concatenate(rows, axis=0), hit.astype(f32).astype(bf16), ((0,), (0,)))


def offsets(lines):
    total, ahead = jnp.zeros((8, 1), f32), []
    for k in range(SPAN // T):
        ahead.append(total)
        end = (k % 2) * T + T - 1
        total = total + lines[8 * (k // 2) : 8 * (k // 2) + 8, end : end + 1]
    return ahead, total


def absolute(lines, ahead):
    first = lax.broadcasted_iota(jnp.int32, (8, 128), 1) < T
    parts = []
    for b in range(SPAN // 128):
        parts.append(lines[8 * b : 8 * b + 8] + jnp.where(first, ahead[2 * b], ahead[2 * b + 1]))
    return jnp.concatenate(parts, axis=0)


def span_state(
    bias, rates, xb, cr, zr, raw, x_taps, b_taps,
    u_out, b_out, c_out, z_out, l_out, d_out, t_out, s_out,
    u_v, b_v, late_v, wide, sem,
):
    away = fetch([(cr, c_out), (zr, z_out)], sem.at[pl.ds(0, 2)])
    row = lax.rem(lax.broadcasted_iota(jnp.int32, (64, 1), 0), 8)
    dtb = jnp.where(row == 0, bias[0], jnp.where(row == 1, bias[1], 0.0))
    rate = jnp.where(row == 0, rates[0], jnp.where(row == 1, rates[1], 0.0))
    row = lax.broadcasted_iota(jnp.int32, (128, 128), 0)
    col = lax.broadcasted_iota(jnp.int32, (128, 128), 1)
    sums = jnp.logical_and(row <= col, row // T == col // T).astype(f32).astype(bf16)
    none = jnp.zeros((6, 128), f32)
    for s in range(SEQS):
        steps = []
        for b in range(SPAN // 128):
            steps += [jnp.concatenate([raw[s, 2 * b], raw[s, 2 * b + 1]], axis=1), none]
        dt = softplus(jnp.concatenate(steps, axis=0) + dtb)
        ld = -(dt * rate) / LENGTH
        both = dot(jnp.concatenate(halves(ld), axis=0), sums)
        lines = both[0:64] + both[64:128]
        l_out[s] = lines
        ahead, total = offsets(lines)
        total_all = jnp.concatenate([total] * 8, axis=0)
        late = dt * jnp.exp(total_all - absolute(lines, ahead))
        rows = halves(dt) + halves(late)
        for b in range(SPAN // 128):
            block = [v[8 * b : 8 * b + 8] for v in rows]
            wide[128 * b : 128 * b + 128, :] = spread(block, (0, 0, 1, 1))
        d_out[s] = wide[0:T]
        head = lax.broadcasted_iota(jnp.int32, (1, 128), 1) < HEAD_P
        t_out[s] = jnp.broadcast_to(jnp.where(head, total[0:1], total[1:2]), (8, 128))
        for first in range(T, SPAN, 128):
            last = min(first + 128, SPAN)
            rows = xb[s, first - HALO : last, :].astype(f32)
            x = convolve(rows[:, 0:128], x_taps)
            u_v[s, first:last, :] = (x * wide[first:last, 0:128]).astype(bf16)
            late_v[first:last, :] = (x * wide[first:last, 128:256]).astype(bf16)
            b_v[s, first:last, :] = convolve(rows[:, 128:256], b_taps).astype(bf16)
        at = pl.ds(T, SPAN - T)
        ready = [(u_v.at[s, at, :], u_out.at[s, at, :]), (b_v.at[s, at, :], b_out.at[s, at, :])]
        away += fetch(ready, sem.at[pl.ds(2 + 2 * s, 2)])
        s_out[s] = dot(b_v[s, T:, :], late_v[T:, :], ((0,), (0,)))
    for m in away:
        m.wait()


def span_first(x0, halo, x_taps, b_taps, dt, totals, part, u_out, b_out, pack):
    for s in range(SEQS):
        rows = jnp.concatenate([entering(halo, s, 0, 256), x0[s].astype(f32)], axis=0)
        total = totals[s, 0:1, :]
        x = convolve(rows[:, 0:128], x_taps)
        b = convolve(rows[:, 128:256], b_taps).astype(bf16)
        u_out[s] = (x * dt[s, :, 0:128]).astype(bf16)
        b_out[s] = b
        late = (x * dt[s, :, 128:256]).astype(bf16)
        state = (part[s] + dot(b, late, ((0,), (0,)))).astype(bf16)
        t_hi = total.astype(bf16).astype(f32)
        which = lax.broadcasted_iota(jnp.int32, (16, 128), 0)
        both = jnp.where(which == 0, t_hi, jnp.where(which == 1, total - t_hi, 0.0))
        both = both.astype(bf16)
        for k in range(SPANS):
            pack[k, s, 0:128, :] = state
            pack[k, s, 128:144, :] = both


def span_own(u, b, u0, b0, l, cr, zr, halo, taps, y_out, c_out, e_out, cv, uv, bv, zv, mv, sv, wide, sem):
    come = []
    for s in range(SEQS):
        later = pl.ds(T, SPAN - T)
        moves = [(cr.at[s], cv.at[s]), (zr.at[s], zv.at[s])]
        moves += [(u.at[s, later, :], uv.at[s, later, :]), (b.at[s, later, :], bv.at[s, later, :])]
        come.append(fetch(moves, sem.at[pl.ds(4 * s, 4)]))
    row = lax.broadcasted_iota(jnp.int32, (T, 128), 0)
    col = lax.rem(lax.broadcasted_iota(jnp.int32, (T, 128), 1), T)
    seen = col <= row
    left = lax.broadcasted_iota(jnp.int32, (T, 128), 1) < T
    first = lax.broadcasted_iota(jnp.int32, (8, 128), 1) < T
    for s in range(SEQS):
        lines = l[s]
        ahead, _ = offsets(lines)
        past = absolute(lines, ahead)
        for k in range(SPAN // 128):
            v = lines[8 * k : 8 * k + 8]
            rest = jnp.where(first, v[:, T - 1 : T], v[:, 2 * T - 1 : 2 * T]) - v
            rows = halves(v)
            rows += [jnp.exp(r).astype(bf16) for r in (v, rest, past[8 * k : 8 * k + 8])]
            wide[s, 128 * k : 128 * k + 128, :] = spread(rows, (0, 0, 1, 2, 3))
    for s in range(SEQS):
        come[s][0].wait()
        for k in range(0, SPAN, 128):
            if k == 0:
                rows = jnp.concatenate([entering(halo, s, 256, 384), cv[s, 0:128, :].astype(f32)], axis=0)
            else:
                rows = cv[s, k - HALO : k + 128, :].astype(f32)
            c_out[s, k : k + 128, :] = convolve(rows, taps).astype(bf16)
    for moves in come:
        for m in moves[1:]:
            m.wait()
    chunks = [(s, k, slice(k * T, k * T + T)) for k in range(SPAN // T) for s in range(SEQS)]

    def rows(first, later, s, k, at):
        return first[s] if k == 0 else later[s, at, :]

    for s, k, at in chunks:
        bc = rows(b0, bv, s, k, at)
        half = slice((k % 2) * T, (k % 2) * T + T)
        at_8 = 8 * (k // 2)
        l_row = jnp.concatenate([l[s, at_8 : at_8 + 1, half], l[s, at_8 + 1 : at_8 + 2, half]], axis=1)
        pairs = dot(c_out[s, at, :], jnp.concatenate([bc, bc], axis=0), ((1,), (1,)))
        gap = jnp.exp(jnp.where(seen, wide[s, at, 0:128] - l_row, -jnp.inf))
        mv[s, at, :] = (pairs * gap).astype(bf16)
    states = [jnp.zeros((128, 128), f32)] * SEQS
    for s, k, at in chunks[: -SEQS]:
        late = (rows(u0, uv, s, k, at).astype(f32) * wide[s, at, 256:384]).astype(bf16)
        fresh = dot(rows(b0, bv, s, k, at), late, ((0,), (0,)))
        states[s] = states[s] * wide[s, k * T + T - 1 : k * T + T, 128:256] + fresh
        sv[s, k + 1] = states[s].astype(bf16)
    for s, k, at in chunks:
        uc = rows(u0, uv, s, k, at)
        zero = jnp.zeros_like(uc)
        blocks = jnp.concatenate([jnp.where(left, uc, zero), jnp.where(left, zero, uc)], axis=0)
        y = dot(mv[s, at, :], blocks)
        if k > 0:
            y = y + dot(c_out[s, at, :], sv[s, k]) * wide[s, at, 128:256]
        gate = silu(zv[s, at, :].astype(f32))
        e_out[s, at, :] = (gate * wide[s, at, 384:512]).astype(bf16)
        y_out[s, at, :] = (y * gate).astype(bf16)


def finish(packs, y_own, cc, decay, gain, out):
    z, yh, _, _, _ = place()
    me = z * 2 + yh
    for s in range(SEQS):
        state = jnp.zeros((128, 128), f32)
        for j in range(SPANS - 1):
            log = packs[j, s, 128:129, :].astype(f32) + packs[j, s, 129:130, :].astype(f32)
            then = state * jnp.exp(log) + packs[j, s, 0:128, :].astype(f32)
            state = jnp.where(j < me, then, state)
        g = y_own[s].astype(f32) + dot(cc[s], state.astype(bf16)) * decay[s].astype(f32)
        g = g * lax.rsqrt(jnp.mean(g * g, axis=1, keepdims=True) + EPS) * gain[...]
        g = g.astype(bf16)
        for k in range(PIECES):
            out[k, s] = g[k * PIECE : k * PIECE + PIECE, :]


def order_out(*refs):
    ins, out, held, sems = refs[:8], refs[8], refs[9], refs[10]
    moves = fetch([(r, held.at[k]) for k, r in enumerate(ins)], sems)
    _, _, _, x, c = place()
    for core in range(2):
        half = lax.rem(c + core, 2)
        for d in range(4):
            at = pl.multiple_of((2 * lax.rem(x - d + 4, 4) + half) * 128, 128)
            moves[4 * core + d].wait()
            out[pl.ds(at, 128), :] = held[4 * core + d].astype(f32).T.astype(bf16)


def project_out(g, w, out):
    for k in range(2):
        rows = jnp.concatenate([g[8 * k + j].reshape(SEQS * PIECE, 128) for j in range(8)], axis=1)
        out[128 * k : 128 * k + 128, :] = dot(rows, w[...]).astype(bf16)


def struct(shape, kind=bf16):
    return jax.ShapeDtypeStruct(shape, kind)


def local(
    tokens,
    norm_gain,
    x_weight,
    z_weight,
    b_weight,
    c_weight,
    dt_weight,
    x_conv,
    b_conv,
    c_conv,
    dt_bias,
    decay_rate,
    out_gain,
    out_weight,
):
    even = lax.axis_index("yl") == 0
    keep = jnp.where(even, tokens[0:2], tokens[2:4])
    give = jnp.where(even, tokens[2:4], tokens[0:2])
    got = shift(give, "yl", 1)
    left_a = shift(keep, "x", 1)
    right_a = shift(keep, "x", -1)
    left_b = shift(got, "x", 1)
    right_b = shift(got, "x", -1)
    far_a = shift(left_a, "x", 1)
    far_b = shift(right_b, "x", -1)
    here = (keep, left_a, right_a, got, left_b, right_b, far_a, far_b)
    there = tuple(shift(v, "c", 1) for v in here)

    weights = [x_weight, b_weight, c_weight, z_weight]
    weights = weights + [dt_weight.T, norm_gain.reshape(8, 128), out_weight.T]
    (w_own,) = call(
        prepare,
        (struct((88, 512)),),
        weights,
        [pltpu.VMEM(w.shape, w.dtype) for w in weights] + [DMA((7,))],
        hbm=range(7),
    )
    y_parts = [w_own] + [shift(w_own, ("yh", "yl"), d) for d in (1, 2, 3)]
    w_line, o_line = call(gather_y, (struct((4, 72, 512)), struct((4, 64, 128))), y_parts)
    z_parts = [w_line] + [shift(w_line, "z", d) for d in (1, 2, 3)]
    w_in, steps = call(order_in, (struct((1024, 512)), struct((32, 1024))), z_parts)
    o_parts = [o_line] + [shift(o_line, "z", d) for d in (1, 2, 3)]

    half = struct((SEQS, SPAN, 128))
    first = struct((SEQS, T, 128))
    state = struct((SEQS, 128, 128), f32)
    far_s = pltpu.HBM(half.shape, bf16)
    lines = struct((SEQS, 64, 128), f32)
    totals_s = struct((SEQS, 8, 128), f32)
    first_s = struct((SEQS, T, 256), f32)
    xb, cr, zr, raw, tail, x0, o_here = call(
        project_all,
        (
            struct((SEQS, SPAN, 256)),
            half,
            half,
            struct((SEQS, PIECES, 2, PIECE), f32),
            struct((SEQS, HALO, 384)),
            struct((SEQS, T, 256)),
            pltpu.HBM((1024, 128), bf16),
        ),
        [*here, *there, w_in, steps, *o_parts],
        [DMA((16,))],
        us=5,
    )
    outs = [o_here] + [shift(o_here, "x", d) for d in (1, 2, 3)]
    outs = outs + [shift(v, "c", 1) for v in outs]
    (w_out,) = call(
        order_out,
        (struct((1024, 1024)),),
        outs,
        [pltpu.VMEM((8, 1024, 128), bf16), DMA((8,))],
        hbm=range(8),
    )
    halo = shift(tail, LINE, 1)
    u, b, far_c, far_z, l, dt0, totals, part = call(
        span_state,
        (far_s, far_s, far_s, far_s, lines, first_s, totals_s, state),
        [dt_bias, decay_rate, xb, cr, zr, raw, x_conv, b_conv],
        [pltpu.VMEM(half.shape, bf16)] * 2
        + [pltpu.VMEM((SPAN, 128), bf16), pltpu.VMEM((SPAN, 256), f32), DMA((6,))],
        us=4,
        scalars=2,
    )
    u0, b0, pack = call(
        span_first,
        (first, first, struct((SPANS, SEQS, 144, 128))),
        [x0, halo, x_conv, b_conv, dt0, totals, part],
    )
    packs = exchange(pack, LINE)
    y_own, cc, decay = call(
        span_own,
        (half, half, half),
        [u, b, u0, b0, l, far_c, far_z, halo, c_conv],
        [pltpu.VMEM(half.shape, bf16)] * 5
        + [pltpu.VMEM((SEQS, PIECES, 128, 128), bf16), pltpu.VMEM((SEQS, SPAN, 512), f32), DMA((8,))],
        us=6,
        hbm=(0, 1, 5, 6),
    )
    (gated,) = call(
        finish,
        (struct((PIECES, SEQS, PIECE, 128)),),
        [packs, y_own, cc, decay, out_gain[None]],
    )
    back = exchange(gated, GROUP)
    (out,) = call(project_out, (struct((256, 1024)),), [back, w_out])
    return out.reshape(2 * SEQS, PIECE, 1024)


def solution(mesh):
    torus = Mesh(mesh.devices.reshape(4, 2, 2, 4, 2), AXES)
    return jax.shard_map(
        local,
        mesh=torus,
        in_specs=(
            P(None, AXES, None),
            P(),
            P(SP, TP),
            P(SP, TP),
            P(SP, TP),
            P(SP, TP),
            P(SP, TP),
            P(None, TP),
            P(None, TP),
            P(None, TP),
            P(TP),
            P(TP),
            P(TP),
            P(TP, SP),
        ),
        out_specs=P(None, AXES, None),
        check_vma=False,
    )
```

```python
import jax
import jax.numpy as jnp
from jax import lax
from jax.experimental import pallas as pl
from jax.experimental.pallas import tpu as pltpu
from jax.sharding import Mesh
from jax.sharding import PartitionSpec as P


LENGTH = 8192
HEAD_P = 64
SEQS = 2
SPAN = 1024
PIECE = 64
PIECES = 16
T = 64
HALO = 16
EPS = 1e-05
AXES = ("z", "yh", "yl", "x", "c")
SP = ("z", "yh", "yl")
TP = ("x", "c")
LINE = ("z", "yh")
GROUP = ("yl", "x", "c")
bf16 = jnp.bfloat16
f32 = jnp.float32
VM = pl.BlockSpec(memory_space=pltpu.VMEM)
SM = pl.BlockSpec(memory_space=pltpu.SMEM)


HB = pl.BlockSpec(memory_space=pltpu.HBM)
DMA = pltpu.SemaphoreType.DMA


def call(body, outs, ins, scratch=(), mib=16, us=2, scalars=0, hbm=()):
    ins = [pltpu.with_memory_space_constraint(v, pltpu.HBM) if k in hbm else v for k, v in enumerate(ins)]
    return pl.pallas_call(
        body,
        out_shape=outs,
        in_specs=[SM if k < scalars else HB if k in hbm else VM for k in range(len(ins))],
        out_specs=tuple(VM if isinstance(o, jax.ShapeDtypeStruct) else HB for o in outs),
        scratch_shapes=list(scratch),
        compiler_params=pltpu.CompilerParams(vmem_limit_bytes=mib * 1024 * 1024),
        cost_estimate=pl.CostEstimate(
            flops=us * 1000000000, bytes_accessed=1 << 20, transcendentals=0
        ),
    )(*ins)


def fetch(pairs, sems):
    moves = [pltpu.make_async_copy(a, b, sems.at[k]) for k, (a, b) in enumerate(pairs)]
    for m in moves:
        m.start()
    return moves


def place():
    return [lax.axis_index(a) for a in AXES]


def shift(value, axis, d):
    n = lax.axis_size(axis)
    return lax.ppermute(value, axis, [(i, (i + d) % n) for i in range(n)])


def exchange(value, axes):
    return lax.all_to_all(value, axes, 0, 0, tiled=True)


def silu(v):
    h = 0.5 * v
    return h + h * jnp.tanh(h)


def softplus(v):
    return jnp.maximum(v, 0.0) + jnp.log1p(jnp.exp(-jnp.abs(v)))


def dot(a, b, dims=((1,), (0,))):
    return lax.dot_general(a, b, (dims, ((), ())), preferred_element_type=f32)


def prepare(*refs):
    ins, w_out, held, sems = refs[:7], refs[7], refs[8:15], refs[15]
    moves = fetch(list(zip(ins, held)), sems)
    for m in moves:
        m.wait()
    xw, bw, cw, zw, dw, gain, ow = held
    z, yh, yl, _, _ = place()
    sp = z * 4 + yh * 2 + yl
    row = gain[pl.ds(lax.div(sp, 2), 1), :]
    first = lax.rem(sp, 2) == 0
    row = jnp.where(first, row[:, 0:64], row[:, 64:128])
    row = jnp.concatenate([row, row], axis=1)
    g = jnp.broadcast_to(row, (128, 128)).T[0:64]
    dt = dw[...].astype(f32)
    dt = jnp.concatenate([dt[0:1], dt[1:2]], axis=1) * row
    dt = jnp.broadcast_to(dt, (8, 128)).astype(bf16)
    ws = [(v[...].astype(f32) * g).astype(bf16) for v in (xw, bw, cw, zw)]
    o = ow[...]
    for j in range(4):
        w_out[0:64, 128 * j : 128 * j + 128] = ws[j]
    w_out[64:72, 0:128] = dt
    w_out[64:72, 128:512] = jnp.zeros((8, 384), bf16)
    for j in range(4):
        w_out[72:88, 128 * j : 128 * j + 128] = o[16 * j : 16 * j + 16]


def gather_y(p0, p1, p2, p3, out, o_out):
    _, yh, yl, _, _ = place()
    for d, p in enumerate((p0, p1, p2, p3)):
        at = lax.rem(2 * yh + yl - d + 4, 4)
        out[at] = p[0:72, :]
        for j in range(4):
            o_out[at, 16 * j : 16 * j + 16, :] = p[72:88, 128 * j : 128 * j + 128]


def order_in(p0, p1, p2, p3, w, steps):
    z = lax.axis_index("z")
    for d, p in enumerate((p0, p1, p2, p3)):
        first = lax.rem(z - d + 4, 4) * 256
        for k in range(4):
            w[pl.ds(pl.multiple_of(first + 64 * k, 64), 64), :] = p[k, 0:64, :]
        at = pl.ds(pl.multiple_of(first, 256), 256)
        rows = [p[k, 64:72, 0:128].astype(f32)[0:1] for k in range(4)]
        for h in range(2):
            row = jnp.concatenate([v[:, 64 * h : 64 * h + 64] for v in rows], axis=1)
            steps[16 * h : 16 * h + 16, at] = jnp.broadcast_to(row, (16, 256)).astype(bf16)


def slots():
    _, _, yl, x, c = place()
    return [
        (half * 4 + lax.rem(x - d + 4, 4)) * 2 + core
        for core in (c, 1 - c)
        for half, d in ((yl, 0), (yl, 1), (yl, 3), (1 - yl, 0), (1 - yl, 1), (1 - yl, 3), (yl, 2), (1 - yl, 2))
    ]


def project_all(*refs):
    here, there, (w, steps) = refs[:8], refs[8:16], refs[16:18]
    xb, cr, zr, dt_out, tail, x0 = refs[18:]
    places = slots()
    lane = lax.broadcasted_iota(jnp.int32, (128, 128), 1)
    for k in range(2):
        pieces = [v[...] for v in (here, there)[k]]
        rows = jnp.concatenate([p.reshape(SEQS * PIECE, 1024) for p in pieces], axis=0)
        wide = rows.astype(f32)
        r = lax.rsqrt(jnp.mean(wide * wide, axis=1, keepdims=True) + EPS)
        part = (dot(rows, w[...]) * r).astype(bf16).reshape(8, SEQS, PIECE, 512)
        d0, d1 = (
            jnp.sum(wide * jnp.concatenate([steps[16 * h : 16 * h + 16, :]] * 64, axis=0).astype(f32), axis=1, keepdims=True) * r
            for h in range(2)
        )
        for j in range(8):
            slot = places[8 * k + j]
            at = pl.ds(pl.multiple_of(slot * PIECE, PIECE), PIECE)
            for s in range(SEQS):
                for ref, lo, n in ((xb, 0, 256), (cr, 256, 128), (zr, 384, 128)):
                    ref[s, at, :] = part[j, s, :, lo : lo + n]
            one = slice(128 * j, 128 * j + 128)
            turned = jnp.where(lane < 64, d0[one], d1[one]).T
            both = jnp.concatenate([turned[0:1], turned[64:65]], axis=0)
            for s in range(SEQS):
                dt_out[s, slot] = both[:, 64 * s : 64 * s + 64]
    x0[...] = xb[:, 0:T, :]
    tail[:, :, 0:256] = xb[:, SPAN - HALO :, :]
    tail[:, :, 256:384] = cr[:, SPAN - HALO :, :]


def entering(halo, s, lane, end):
    z, yh, _, _, _ = place()
    v = halo[s, :, lane:end].astype(f32)
    return jnp.where(2 * z + yh == 0, jnp.zeros_like(v), v)


def convolve(rows, taps):
    part = (0.5 * taps[0:1, :]) * rows
    for k in range(1, 4):
        part = (0.5 * taps[k : k + 1, :]) * rows + pltpu.roll(part, 1, 0)
    half = part[HALO:]
    return half + half * jnp.tanh(half)


def halves(v):
    hi = v.astype(bf16)
    return [hi, (v - hi.astype(f32)).astype(bf16)]


def spread(rows, groups):
    count = max(groups) + 1
    source = lax.broadcasted_iota(jnp.int32, (8 * len(rows), 128 * count), 0)
    lane = lax.broadcasted_iota(jnp.int32, (8 * len(rows), 128 * count), 1)
    hit = None
    for k, g in enumerate(groups):
        want = lane // HEAD_P - 2 * g + 8 * k
        mine = jnp.logical_and(lane // 128 == g, source == want)
        hit = mine if hit is None else jnp.logical_or(hit, mine)
    return dot(jnp.concatenate(rows, axis=0), hit.astype(f32).astype(bf16), ((0,), (0,)))


def offsets(lines):
    total, ahead = jnp.zeros((8, 1), f32), []
    for k in range(SPAN // T):
        ahead.append(total)
        end = (k % 2) * T + T - 1
        total = total + lines[8 * (k // 2) : 8 * (k // 2) + 8, end : end + 1]
    return ahead, total


def absolute(lines, ahead):
    first = lax.broadcasted_iota(jnp.int32, (8, 128), 1) < T
    parts = []
    for b in range(SPAN // 128):
        parts.append(lines[8 * b : 8 * b + 8] + jnp.where(first, ahead[2 * b], ahead[2 * b + 1]))
    return jnp.concatenate(parts, axis=0)


def span_state(
    bias, rates, xb, raw, x_taps, b_taps, u_v, b_v, l_out, d_out, t_out, s_out, late_v, wide
):
    row = lax.rem(lax.broadcasted_iota(jnp.int32, (64, 1), 0), 8)
    dtb = jnp.where(row == 0, bias[0], jnp.where(row == 1, bias[1], 0.0))
    rate = jnp.where(row == 0, rates[0], jnp.where(row == 1, rates[1], 0.0))
    row = lax.broadcasted_iota(jnp.int32, (128, 128), 0)
    col = lax.broadcasted_iota(jnp.int32, (128, 128), 1)
    sums = jnp.logical_and(row <= col, row // T == col // T).astype(f32).astype(bf16)
    none = jnp.zeros((6, 128), f32)
    for s in range(SEQS):
        steps = []
        for b in range(SPAN // 128):
            steps += [jnp.concatenate([raw[s, 2 * b], raw[s, 2 * b + 1]], axis=1), none]
        dt = softplus(jnp.concatenate(steps, axis=0) + dtb)
        ld = -(dt * rate) / LENGTH
        both = dot(jnp.concatenate(halves(ld), axis=0), sums)
        lines = both[0:64] + both[64:128]
        l_out[s] = lines
        ahead, total = offsets(lines)
        total_all = jnp.concatenate([total] * 8, axis=0)
        late = dt * jnp.exp(total_all - absolute(lines, ahead))
        rows = halves(dt) + halves(late)
        for b in range(SPAN // 128):
            block = [v[8 * b : 8 * b + 8] for v in rows]
            wide[128 * b : 128 * b + 128, :] = spread(block, (0, 0, 1, 1))
        d_out[s] = wide[0:T]
        head = lax.broadcasted_iota(jnp.int32, (1, 128), 1) < HEAD_P
        t_out[s] = jnp.broadcast_to(jnp.where(head, total[0:1], total[1:2]), (8, 128))
        for first in range(T, SPAN, 128):
            last = min(first + 128, SPAN)
            rows = xb[s, first - HALO : last, :].astype(f32)
            x = convolve(rows[:, 0:128], x_taps)
            u_v[s, first:last, :] = (x * wide[first:last, 0:128]).astype(bf16)
            late_v[first:last, :] = (x * wide[first:last, 128:256]).astype(bf16)
            b_v[s, first:last, :] = convolve(rows[:, 128:256], b_taps).astype(bf16)
        s_out[s] = dot(b_v[s, T:, :], late_v[T:, :], ((0,), (0,)))


def two_parts(row):
    high = row.astype(bf16).astype(f32)
    which = lax.broadcasted_iota(jnp.int32, (16, 128), 0)
    return jnp.where(which == 0, high, jnp.where(which == 1, row - high, 0.0)).astype(bf16)


def log_of(pack, s):
    return pack[s, 128:129, :].astype(f32) + pack[s, 129:130, :].astype(f32)


def span_first(x0, halo, x_taps, b_taps, dt, totals, part, u_out, b_out, pack):
    for s in range(SEQS):
        rows = jnp.concatenate([entering(halo, s, 0, 256), x0[s].astype(f32)], axis=0)
        total = totals[s, 0:1, :]
        x = convolve(rows[:, 0:128], x_taps)
        b = convolve(rows[:, 128:256], b_taps).astype(bf16)
        u_out[s] = (x * dt[s, :, 0:128]).astype(bf16)
        b_out[s] = b
        late = (x * dt[s, :, 128:256]).astype(bf16)
        state = (part[s] + dot(b, late, ((0,), (0,)))).astype(bf16)
        pack[s, 0:128, :] = state
        pack[s, 128:144, :] = two_parts(total)


def span_own(s, u, b, u0, b0, l, cr, zr, halo, taps, y_out, c_out, e_out, mv, sv, wide):
    row = lax.broadcasted_iota(jnp.int32, (T, 128), 0)
    col = lax.rem(lax.broadcasted_iota(jnp.int32, (T, 128), 1), T)
    seen = col <= row
    left = lax.broadcasted_iota(jnp.int32, (T, 128), 1) < T
    first = lax.broadcasted_iota(jnp.int32, (8, 128), 1) < T
    lines = l[s]
    ahead, _ = offsets(lines)
    past = absolute(lines, ahead)
    for k in range(SPAN // 128):
        v = lines[8 * k : 8 * k + 8]
        rest = jnp.where(first, v[:, T - 1 : T], v[:, 2 * T - 1 : 2 * T]) - v
        rows = halves(v)
        rows += [jnp.exp(r).astype(bf16) for r in (v, rest, past[8 * k : 8 * k + 8])]
        wide[128 * k : 128 * k + 128, :] = spread(rows, (0, 0, 1, 2, 3))
    for k in range(0, SPAN, 128):
        if k == 0:
            rows = jnp.concatenate([entering(halo, s, 256, 384), cr[s, 0:128, :].astype(f32)], axis=0)
        else:
            rows = cr[s, k - HALO : k + 128, :].astype(f32)
        c_out[k : k + 128, :] = convolve(rows, taps).astype(bf16)
    chunks = [(k, slice(k * T, k * T + T)) for k in range(SPAN // T)]

    def rows_of(start, later, k, at):
        return start[s] if k == 0 else later[s, at, :]

    for k, at in chunks:
        bc = rows_of(b0, b, k, at)
        half = slice((k % 2) * T, (k % 2) * T + T)
        at_8 = 8 * (k // 2)
        l_row = jnp.concatenate([l[s, at_8 : at_8 + 1, half], l[s, at_8 + 1 : at_8 + 2, half]], axis=1)
        pairs = dot(c_out[at, :], jnp.concatenate([bc, bc], axis=0), ((1,), (1,)))
        gap = jnp.exp(jnp.where(seen, wide[at, 0:128] - l_row, -jnp.inf))
        mv[at, :] = (pairs * gap).astype(bf16)
    state = jnp.zeros((128, 128), f32)
    for k, at in chunks[:-1]:
        late = (rows_of(u0, u, k, at).astype(f32) * wide[at, 256:384]).astype(bf16)
        fresh = dot(rows_of(b0, b, k, at), late, ((0,), (0,)))
        state = state * wide[k * T + T - 1 : k * T + T, 128:256] + fresh
        sv[k + 1] = state.astype(bf16)
    for k, at in chunks:
        uc = rows_of(u0, u, k, at)
        zero = jnp.zeros_like(uc)
        blocks = jnp.concatenate([jnp.where(left, uc, zero), jnp.where(left, zero, uc)], axis=0)
        y = dot(mv[at, :], blocks)
        if k > 0:
            y = y + dot(c_out[at, :], sv[k]) * wide[at, 128:256]
        gate = silu(zr[s, at, :].astype(f32))
        e_out[at, :] = (gate * wide[at, 384:512]).astype(bf16)
        y_out[at, :] = (y * gate).astype(bf16)


def span_own_0(*refs):
    span_own(0, *refs)


def span_own_1(*refs):
    span_own(1, *refs)


def combine_y(mine, other, total, before, l_before):
    late = lax.axis_index("yh") == 1
    for s in range(SEQS):
        log_0, log_1 = log_of(mine, s), log_of(other, s)
        state_0, state_1 = mine[s, 0:128, :].astype(f32), other[s, 0:128, :].astype(f32)
        ahead = state_0 * jnp.exp(log_1) + state_1
        behind = state_1 * jnp.exp(log_0) + state_0
        total[s, 0:128, :] = jnp.where(late, behind, ahead).astype(bf16)
        total[s, 128:144, :] = two_parts(log_0 + log_1)
        before[s] = jnp.where(late, state_1, jnp.zeros_like(state_1))
        l_before[s] = jnp.broadcast_to(jnp.where(late, log_1, jnp.zeros_like(log_1)), (8, 128))


def finish(*refs):
    packs, (before, l_before), own, (gain, out) = refs[:3], refs[3:5], refs[5:11], refs[11:]
    z = lax.axis_index("z")
    for s in range(SEQS):
        y_own, cc, decay = own[3 * s : 3 * s + 3]
        log = l_before[s, 0:1, :]
        state = before[s]
        for d in range(1, 4):
            past = packs[d - 1][s, 0:128, :].astype(f32)
            state = state + jnp.where(d <= z, past * jnp.exp(log), jnp.zeros_like(past))
            log = log + log_of(packs[d - 1], s)
        g = y_own[...].astype(f32) + dot(cc[...], state.astype(bf16)) * decay[...].astype(f32)
        g = g * lax.rsqrt(jnp.mean(g * g, axis=1, keepdims=True) + EPS) * gain[...]
        g = g.astype(bf16)
        for k in range(PIECES):
            out[k, s] = g[k * PIECE : k * PIECE + PIECE, :]


def order_o(p0, p1, p2, p3, _, out):
    z = lax.axis_index("z")
    for d, p in enumerate((p0, p1, p2, p3)):
        at = pl.multiple_of(lax.rem(z - d + 4, 4) * 256, 256)
        out[pl.ds(at, 256), :] = p[...].reshape(256, 128)


def order_out(*refs):
    ins, out, held, sems = refs[:8], refs[8], refs[9], refs[10]
    moves = fetch([(r, held.at[k]) for k, r in enumerate(ins)], sems)
    _, _, _, x, c = place()
    for core in range(2):
        half = lax.rem(c + core, 2)
        for d in range(4):
            at = pl.multiple_of((2 * lax.rem(x - d + 4, 4) + half) * 128, 128)
            moves[4 * core + d].wait()
            out[pl.ds(at, 128), :] = held[4 * core + d].astype(f32).T.astype(bf16)


def project_out(g, w, out):
    for k in range(2):
        rows = jnp.concatenate([g[8 * k + j].reshape(SEQS * PIECE, 128) for j in range(8)], axis=1)
        out[128 * k : 128 * k + 128, :] = dot(rows, w[...]).astype(bf16)


def struct(shape, kind=bf16):
    return jax.ShapeDtypeStruct(shape, kind)


def local(
    tokens,
    norm_gain,
    x_weight,
    z_weight,
    b_weight,
    c_weight,
    dt_weight,
    x_conv,
    b_conv,
    c_conv,
    dt_bias,
    decay_rate,
    out_gain,
    out_weight,
):
    even = lax.axis_index("yl") == 0
    keep = jnp.where(even, tokens[0:2], tokens[2:4])
    give = jnp.where(even, tokens[2:4], tokens[0:2])
    got = shift(give, "yl", 1)
    left_a = shift(keep, "x", 1)
    right_a = shift(keep, "x", -1)
    left_b = shift(got, "x", 1)
    right_b = shift(got, "x", -1)
    far_a = shift(left_a, "x", 1)
    far_b = shift(right_b, "x", -1)
    here = (keep, left_a, right_a, got, left_b, right_b, far_a, far_b)
    there = tuple(shift(v, "c", 1) for v in here)

    weights = [x_weight, b_weight, c_weight, z_weight]
    weights = weights + [dt_weight.T, norm_gain.reshape(8, 128), out_weight.T]
    (w_own,) = call(
        prepare,
        (struct((88, 512)),),
        weights,
        [pltpu.VMEM(w.shape, w.dtype) for w in weights] + [DMA((7,))],
        hbm=range(7),
    )
    y_parts = [w_own] + [shift(w_own, ("yh", "yl"), d) for d in (1, 2, 3)]
    w_line, o_line = call(gather_y, (struct((4, 72, 512)), struct((4, 64, 128))), y_parts)
    z_parts = [w_line] + [shift(w_line, "z", d) for d in (1, 2, 3)]
    w_in, steps = call(order_in, (struct((1024, 512)), struct((32, 1024))), z_parts)
    o_parts = [o_line] + [shift(o_line, "z", d) for d in (1, 2, 3)]

    half = struct((SEQS, SPAN, 128))
    first = struct((SEQS, T, 128))
    state = struct((SEQS, 128, 128), f32)
    far_s = pltpu.HBM(half.shape, bf16)
    lines = struct((SEQS, 64, 128), f32)
    totals_s = struct((SEQS, 8, 128), f32)
    first_s = struct((SEQS, T, 256), f32)
    xb, cr, zr, raw, tail, x0 = call(
        project_all,
        (
            struct((SEQS, SPAN, 256)),
            half,
            half,
            struct((SEQS, PIECES, 2, PIECE), f32),
            struct((SEQS, HALO, 384)),
            struct((SEQS, T, 256)),
        ),
        [*here, *there, w_in, steps],
        us=5,
    )
    (o_here,) = call(order_o, (struct((1024, 128)),), [*o_parts, tail])
    outs = [o_here] + [shift(o_here, "x", d) for d in (1, 2, 3)]
    outs = outs + [shift(v, "c", 1) for v in outs]
    (w_out,) = call(
        order_out,
        (struct((1024, 1024)),),
        outs,
        [pltpu.VMEM((8, 1024, 128), bf16), DMA((8,))],
        hbm=range(8),
    )
    halo = shift(tail, LINE, 1)
    u, b, l, dt0, totals, part = call(
        span_state,
        (half, half, lines, first_s, totals_s, state),
        [dt_bias, decay_rate, xb, raw, x_conv, b_conv],
        [pltpu.VMEM((SPAN, 128), bf16), pltpu.VMEM((SPAN, 256), f32)],
        us=4,
        scalars=2,
    )
    u0, b0, pack = call(
        span_first,
        (first, first, struct((SEQS, 144, 128))),
        [x0, halo, x_conv, b_conv, dt0, totals, part],
    )
    near_pack = shift(pack, "yh", 1)
    one = struct((SPAN, 128))
    own = []
    for k in range(SEQS):
        own.append(
            call(
                (span_own_0, span_own_1)[k],
                (one, one, one),
                [u, b, u0, b0, l, cr, zr, halo, c_conv],
                [
                    pltpu.VMEM((SPAN, 128), bf16),
                    pltpu.VMEM((PIECES, 128, 128), bf16),
                    pltpu.VMEM((SPAN, 512), f32),
                ],
                us=2,
            )
        )
    total, before, l_before = call(
        combine_y,
        (struct((SEQS, 144, 128)), state, struct((SEQS, 8, 128), f32)),
        [pack, near_pack],
    )
    packs = [shift(total, "z", d) for d in (1, 2, 3)]
    (gated,) = call(
        finish,
        (struct((PIECES, SEQS, PIECE, 128)),),
        [*packs, before, l_before, *own[0], *own[1], out_gain[None]],
    )
    back = exchange(gated, GROUP)
    (out,) = call(project_out, (struct((256, 1024)),), [back, w_out])
    return out.reshape(2 * SEQS, PIECE, 1024)


def solution(mesh):
    torus = Mesh(mesh.devices.reshape(4, 2, 2, 4, 2), AXES)
    return jax.shard_map(
        local,
        mesh=torus,
        in_specs=(
            P(None, AXES, None),
            P(),
            P(SP, TP),
            P(SP, TP),
            P(SP, TP),
            P(SP, TP),
            P(SP, TP),
            P(None, TP),
            P(None, TP),
            P(None, TP),
            P(TP),
            P(TP),
            P(TP),
            P(TP, SP),
        ),
        out_specs=P(None, AXES, None),
        check_vma=False,
    )
```

```python
import jax
import jax.numpy as jnp
from jax import lax
from jax.experimental import pallas as pl
from jax.experimental.pallas import tpu as pltpu
from jax.sharding import Mesh
from jax.sharding import PartitionSpec as P


LENGTH = 8192
HEAD_P = 64
SEQS = 2
SPAN = 1024
PIECE = 64
PIECES = 16
T = 64
HALO = 16
EPS = 1e-05
AXES = ("z", "yh", "yl", "x", "c")
SP = ("z", "yh", "yl")
TP = ("x", "c")
LINE = ("z", "yh")
GROUP = ("yl", "x", "c")
bf16 = jnp.bfloat16
f32 = jnp.float32
VM = pl.BlockSpec(memory_space=pltpu.VMEM)
SM = pl.BlockSpec(memory_space=pltpu.SMEM)


HB = pl.BlockSpec(memory_space=pltpu.HBM)
DMA = pltpu.SemaphoreType.DMA


def call(body, outs, ins, scratch=(), mib=16, us=2, scalars=0, hbm=()):
    ins = [pltpu.with_memory_space_constraint(v, pltpu.HBM) if k in hbm else v for k, v in enumerate(ins)]
    return pl.pallas_call(
        body,
        out_shape=outs,
        in_specs=[SM if k < scalars else HB if k in hbm else VM for k in range(len(ins))],
        out_specs=tuple(VM if isinstance(o, jax.ShapeDtypeStruct) else HB for o in outs),
        scratch_shapes=list(scratch),
        compiler_params=pltpu.CompilerParams(vmem_limit_bytes=mib * 1024 * 1024),
        cost_estimate=pl.CostEstimate(
            flops=us * 1000000000, bytes_accessed=1 << 20, transcendentals=0
        ),
    )(*ins)


def fetch(pairs, sems):
    moves = [pltpu.make_async_copy(a, b, sems.at[k]) for k, (a, b) in enumerate(pairs)]
    for m in moves:
        m.start()
    return moves


def place():
    return [lax.axis_index(a) for a in AXES]


def shift(value, axis, d):
    n = lax.axis_size(axis)
    return lax.ppermute(value, axis, [(i, (i + d) % n) for i in range(n)])


def exchange(value, axes):
    return lax.all_to_all(value, axes, 0, 0, tiled=True)


def silu(v):
    h = 0.5 * v
    return h + h * jnp.tanh(h)


def softplus(v):
    return jnp.maximum(v, 0.0) + jnp.log1p(jnp.exp(-jnp.abs(v)))


def dot(a, b, dims=((1,), (0,))):
    return lax.dot_general(a, b, (dims, ((), ())), preferred_element_type=f32)


def prepare(*refs):
    ins, w_out, held, sems = refs[:7], refs[7], refs[8:15], refs[15]
    moves = fetch(list(zip(ins, held)), sems)
    for m in moves:
        m.wait()
    xw, bw, cw, zw, dw, gain, ow = held
    z, yh, yl, _, _ = place()
    sp = z * 4 + yh * 2 + yl
    row = gain[pl.ds(lax.div(sp, 2), 1), :]
    first = lax.rem(sp, 2) == 0
    row = jnp.where(first, row[:, 0:64], row[:, 64:128])
    row = jnp.concatenate([row, row], axis=1)
    g = jnp.broadcast_to(row, (128, 128)).T[0:64]
    dt = dw[...].astype(f32)
    dt = jnp.concatenate([dt[0:1], dt[1:2]], axis=1) * row
    dt = jnp.broadcast_to(dt, (8, 128)).astype(bf16)
    ws = [(v[...].astype(f32) * g).astype(bf16) for v in (xw, bw, cw, zw)]
    o = ow[...]
    for j in range(4):
        w_out[0:64, 128 * j : 128 * j + 128] = ws[j]
    w_out[64:72, 0:128] = dt
    w_out[64:72, 128:512] = jnp.zeros((8, 384), bf16)
    for j in range(4):
        w_out[72:88, 128 * j : 128 * j + 128] = o[16 * j : 16 * j + 16]


def gather_y(p0, p1, p2, p3, out):
    _, yh, yl, _, _ = place()
    for d, p in enumerate((p0, p1, p2, p3)):
        out[lax.rem(2 * yh + yl - d + 4, 4)] = p[...]


def order_in(p0, p1, p3, p2a, p2b, w, steps, o_out):
    z = lax.axis_index("z")
    for d in range(4):
        parts = [(p0, k) for k in range(4)]
        if d > 0:
            whole = {1: p1, 3: p3}.get(d)
            parts = [(whole, k) for k in range(4)] if whole is not None else [(p2a, 0), (p2a, 1), (p2b, 0), (p2b, 1)]
        first = lax.rem(z - d + 4, 4) * 256
        for k, (p, j) in enumerate(parts):
            at = pl.multiple_of(first + 64 * k, 64)
            w[pl.ds(at, 64), :] = p[j, 0:64, :]
            for n in range(4):
                o_out[pl.ds(at + 16 * n, 16), :] = p[j, 72:88, 128 * n : 128 * n + 128]
        at = pl.ds(pl.multiple_of(first, 256), 256)
        rows = [p[j, 64:72, 0:128].astype(f32)[0:1] for p, j in parts]
        for h in range(2):
            row = jnp.concatenate([v[:, 64 * h : 64 * h + 64] for v in rows], axis=1)
            steps[16 * h : 16 * h + 16, at] = jnp.broadcast_to(row, (16, 256)).astype(bf16)


def slots():
    _, _, yl, x, c = place()
    return [
        (half * 4 + lax.rem(x - d + 4, 4)) * 2 + core
        for core in (c, 1 - c)
        for half, d in ((yl, 0), (yl, 1), (yl, 3), (1 - yl, 0), (1 - yl, 1), (1 - yl, 3), (yl, 2), (1 - yl, 2))
    ]


def project_all(*refs):
    here, there, (w, steps) = refs[:8], refs[8:16], refs[16:18]
    xb, cr, zr, dt_out, tail, x0 = refs[18:]
    places = slots()
    lane = lax.broadcasted_iota(jnp.int32, (128, 128), 1)
    for k in range(2):
        pieces = [v[...] for v in (here, there)[k]]
        rows = jnp.concatenate([p.reshape(SEQS * PIECE, 1024) for p in pieces], axis=0)
        wide = rows.astype(f32)
        r = lax.rsqrt(jnp.mean(wide * wide, axis=1, keepdims=True) + EPS)
        part = (dot(rows, w[...]) * r).astype(bf16).reshape(8, SEQS, PIECE, 512)
        d0, d1 = (
            jnp.sum(wide * jnp.concatenate([steps[16 * h : 16 * h + 16, :]] * 64, axis=0).astype(f32), axis=1, keepdims=True) * r
            for h in range(2)
        )
        for j in range(8):
            slot = places[8 * k + j]
            at = pl.ds(pl.multiple_of(slot * PIECE, PIECE), PIECE)
            for s in range(SEQS):
                for ref, lo, n in ((xb, 0, 256), (cr, 256, 128), (zr, 384, 128)):
                    ref[s, at, :] = part[j, s, :, lo : lo + n]
            one = slice(128 * j, 128 * j + 128)
            turned = jnp.where(lane < 64, d0[one], d1[one]).T
            both = jnp.concatenate([turned[0:1], turned[64:65]], axis=0)
            for s in range(SEQS):
                dt_out[s, slot] = both[:, 64 * s : 64 * s + 64]
    x0[...] = xb[:, 0:T, :]
    tail[:, :, 0:256] = xb[:, SPAN - HALO :, :]
    tail[:, :, 256:384] = cr[:, SPAN - HALO :, :]


def entering(halo, s, lane, end):
    z, yh, _, _, _ = place()
    v = halo[s, :, lane:end].astype(f32)
    return jnp.where(2 * z + yh == 0, jnp.zeros_like(v), v)


def convolve(rows, taps):
    part = (0.5 * taps[0:1, :]) * rows
    for k in range(1, 4):
        part = (0.5 * taps[k : k + 1, :]) * rows + pltpu.roll(part, 1, 0)
    half = part[HALO:]
    return half + half * jnp.tanh(half)


def halves(v):
    hi = v.astype(bf16)
    return [hi, (v - hi.astype(f32)).astype(bf16)]


def spread(rows, groups):
    count = max(groups) + 1
    source = lax.broadcasted_iota(jnp.int32, (8 * len(rows), 128 * count), 0)
    lane = lax.broadcasted_iota(jnp.int32, (8 * len(rows), 128 * count), 1)
    hit = None
    for k, g in enumerate(groups):
        want = lane // HEAD_P - 2 * g + 8 * k
        mine = jnp.logical_and(lane // 128 == g, source == want)
        hit = mine if hit is None else jnp.logical_or(hit, mine)
    return dot(jnp.concatenate(rows, axis=0), hit.astype(f32).astype(bf16), ((0,), (0,)))


def offsets(lines):
    total, ahead = jnp.zeros((8, 1), f32), []
    for k in range(SPAN // T):
        ahead.append(total)
        end = (k % 2) * T + T - 1
        total = total + lines[8 * (k // 2) : 8 * (k // 2) + 8, end : end + 1]
    return ahead, total


def absolute(lines, ahead):
    first = lax.broadcasted_iota(jnp.int32, (8, 128), 1) < T
    parts = []
    for b in range(SPAN // 128):
        parts.append(lines[8 * b : 8 * b + 8] + jnp.where(first, ahead[2 * b], ahead[2 * b + 1]))
    return jnp.concatenate(parts, axis=0)


def span_state(
    bias, rates, xb, raw, x_taps, b_taps, u_v, b_v, l_out, d_out, t_out, s_out, late_v, wide
):
    row = lax.rem(lax.broadcasted_iota(jnp.int32, (64, 1), 0), 8)
    dtb = jnp.where(row == 0, bias[0], jnp.where(row == 1, bias[1], 0.0))
    rate = jnp.where(row == 0, rates[0], jnp.where(row == 1, rates[1], 0.0))
    row = lax.broadcasted_iota(jnp.int32, (128, 128), 0)
    col = lax.broadcasted_iota(jnp.int32, (128, 128), 1)
    sums = jnp.logical_and(row <= col, row // T == col // T).astype(f32).astype(bf16)
    none = jnp.zeros((6, 128), f32)
    for s in range(SEQS):
        steps = []
        for b in range(SPAN // 128):
            steps += [jnp.concatenate([raw[s, 2 * b], raw[s, 2 * b + 1]], axis=1), none]
        dt = softplus(jnp.concatenate(steps, axis=0) + dtb)
        ld = -(dt * rate) / LENGTH
        both = dot(jnp.concatenate(halves(ld), axis=0), sums)
        lines = both[0:64] + both[64:128]
        l_out[s] = lines
        ahead, total = offsets(lines)
        total_all = jnp.concatenate([total] * 8, axis=0)
        late = dt * jnp.exp(total_all - absolute(lines, ahead))
        rows = halves(dt) + halves(late)
        for b in range(SPAN // 128):
            block = [v[8 * b : 8 * b + 8] for v in rows]
            wide[128 * b : 128 * b + 128, :] = spread(block, (0, 0, 1, 1))
        d_out[s] = wide[0:T]
        head = lax.broadcasted_iota(jnp.int32, (1, 128), 1) < HEAD_P
        t_out[s] = jnp.broadcast_to(jnp.where(head, total[0:1], total[1:2]), (8, 128))
        for first in range(T, SPAN, 128):
            last = min(first + 128, SPAN)
            rows = xb[s, first - HALO : last, :].astype(f32)
            x = convolve(rows[:, 0:128], x_taps)
            u_v[s, first:last, :] = (x * wide[first:last, 0:128]).astype(bf16)
            late_v[first:last, :] = (x * wide[first:last, 128:256]).astype(bf16)
            b_v[s, first:last, :] = convolve(rows[:, 128:256], b_taps).astype(bf16)
        s_out[s] = dot(b_v[s, T:, :], late_v[T:, :], ((0,), (0,)))


def two_parts(row):
    high = row.astype(bf16).astype(f32)
    which = lax.broadcasted_iota(jnp.int32, (16, 128), 0)
    return jnp.where(which == 0, high, jnp.where(which == 1, row - high, 0.0)).astype(bf16)


def log_of(pack, s):
    return pack[s, 128:129, :].astype(f32) + pack[s, 129:130, :].astype(f32)


def span_first(x0, halo, x_taps, b_taps, dt, totals, part, u_out, b_out, pack):
    for s in range(SEQS):
        rows = jnp.concatenate([entering(halo, s, 0, 256), x0[s].astype(f32)], axis=0)
        total = totals[s, 0:1, :]
        x = convolve(rows[:, 0:128], x_taps)
        b = convolve(rows[:, 128:256], b_taps).astype(bf16)
        u_out[s] = (x * dt[s, :, 0:128]).astype(bf16)
        b_out[s] = b
        late = (x * dt[s, :, 128:256]).astype(bf16)
        state = (part[s] + dot(b, late, ((0,), (0,)))).astype(bf16)
        pack[s, 0:128, :] = state
        pack[s, 128:144, :] = two_parts(total)


def span_own(s, u, b, u0, b0, l, cr, zr, halo, taps, y_out, c_out, e_out, mv, sv, wide):
    row = lax.broadcasted_iota(jnp.int32, (T, 128), 0)
    col = lax.rem(lax.broadcasted_iota(jnp.int32, (T, 128), 1), T)
    seen = col <= row
    left = lax.broadcasted_iota(jnp.int32, (T, 128), 1) < T
    first = lax.broadcasted_iota(jnp.int32, (8, 128), 1) < T
    lines = l[s]
    ahead, _ = offsets(lines)
    past = absolute(lines, ahead)
    for k in range(SPAN // 128):
        v = lines[8 * k : 8 * k + 8]
        rest = jnp.where(first, v[:, T - 1 : T], v[:, 2 * T - 1 : 2 * T]) - v
        rows = halves(v)
        rows += [jnp.exp(r).astype(bf16) for r in (v, rest, past[8 * k : 8 * k + 8])]
        wide[128 * k : 128 * k + 128, :] = spread(rows, (0, 0, 1, 2, 3))
    for k in range(0, SPAN, 128):
        if k == 0:
            rows = jnp.concatenate([entering(halo, s, 256, 384), cr[s, 0:128, :].astype(f32)], axis=0)
        else:
            rows = cr[s, k - HALO : k + 128, :].astype(f32)
        c_out[k : k + 128, :] = convolve(rows, taps).astype(bf16)
    chunks = [(k, slice(k * T, k * T + T)) for k in range(SPAN // T)]

    def rows_of(start, later, k, at):
        return start[s] if k == 0 else later[s, at, :]

    for k, at in chunks:
        bc = rows_of(b0, b, k, at)
        half = slice((k % 2) * T, (k % 2) * T + T)
        at_8 = 8 * (k // 2)
        l_row = jnp.concatenate([l[s, at_8 : at_8 + 1, half], l[s, at_8 + 1 : at_8 + 2, half]], axis=1)
        pairs = dot(c_out[at, :], jnp.concatenate([bc, bc], axis=0), ((1,), (1,)))
        gap = jnp.exp(jnp.where(seen, wide[at, 0:128] - l_row, -jnp.inf))
        mv[at, :] = (pairs * gap).astype(bf16)
    state = jnp.zeros((128, 128), f32)
    for k, at in chunks[:-1]:
        late = (rows_of(u0, u, k, at).astype(f32) * wide[at, 256:384]).astype(bf16)
        fresh = dot(rows_of(b0, b, k, at), late, ((0,), (0,)))
        state = state * wide[k * T + T - 1 : k * T + T, 128:256] + fresh
        sv[k + 1] = state.astype(bf16)
    for k, at in chunks:
        uc = rows_of(u0, u, k, at)
        zero = jnp.zeros_like(uc)
        blocks = jnp.concatenate([jnp.where(left, uc, zero), jnp.where(left, zero, uc)], axis=0)
        y = dot(mv[at, :], blocks)
        if k > 0:
            y = y + dot(c_out[at, :], sv[k]) * wide[at, 128:256]
        gate = silu(zr[s, at, :].astype(f32))
        e_out[at, :] = (gate * wide[at, 384:512]).astype(bf16)
        y_out[at, :] = (y * gate).astype(bf16)


def span_own_0(*refs):
    span_own(0, *refs)


def span_own_1(*refs):
    span_own(1, *refs)


def combine_y(mine, other, total, before, l_before):
    late = lax.axis_index("yh") == 1
    for s in range(SEQS):
        log_0, log_1 = log_of(mine, s), log_of(other, s)
        state_0, state_1 = mine[s, 0:128, :].astype(f32), other[s, 0:128, :].astype(f32)
        ahead = state_0 * jnp.exp(log_1) + state_1
        behind = state_1 * jnp.exp(log_0) + state_0
        total[s, 0:128, :] = jnp.where(late, behind, ahead).astype(bf16)
        total[s, 128:144, :] = two_parts(log_0 + log_1)
        before[s] = jnp.where(late, state_1, jnp.zeros_like(state_1))
        l_before[s] = jnp.broadcast_to(jnp.where(late, log_1, jnp.zeros_like(log_1)), (8, 128))


def finish(*refs):
    packs, (before, l_before), own, (gain, out) = refs[:3], refs[3:5], refs[5:11], refs[11:]
    z = lax.axis_index("z")
    for s in range(SEQS):
        y_own, cc, decay = own[3 * s : 3 * s + 3]
        log = l_before[s, 0:1, :]
        state = before[s]
        for d in range(1, 4):
            past = packs[d - 1][s, 0:128, :].astype(f32)
            state = state + jnp.where(d <= z, past * jnp.exp(log), jnp.zeros_like(past))
            log = log + log_of(packs[d - 1], s)
        g = y_own[...].astype(f32) + dot(cc[...], state.astype(bf16)) * decay[...].astype(f32)
        g = g * lax.rsqrt(jnp.mean(g * g, axis=1, keepdims=True) + EPS) * gain[...]
        g = g.astype(bf16)
        for k in range(PIECES):
            out[k, s] = g[k * PIECE : k * PIECE + PIECE, :]


def order_out(*refs):
    ins, out, held, sems = refs[:8], refs[8], refs[9], refs[10]
    moves = fetch([(r, held.at[k]) for k, r in enumerate(ins)], sems)
    _, _, _, x, c = place()
    for core in range(2):
        half = lax.rem(c + core, 2)
        for d in range(4):
            at = pl.multiple_of((2 * lax.rem(x - d + 4, 4) + half) * 128, 128)
            moves[4 * core + d].wait()
            out[pl.ds(at, 128), :] = held[4 * core + d].astype(f32).T.astype(bf16)


def project_out(g, w, out):
    for k in range(2):
        rows = jnp.concatenate([g[8 * k + j].reshape(SEQS * PIECE, 128) for j in range(8)], axis=1)
        out[128 * k : 128 * k + 128, :] = dot(rows, w[...]).astype(bf16)


def struct(shape, kind=bf16):
    return jax.ShapeDtypeStruct(shape, kind)


def local(
    tokens,
    norm_gain,
    x_weight,
    z_weight,
    b_weight,
    c_weight,
    dt_weight,
    x_conv,
    b_conv,
    c_conv,
    dt_bias,
    decay_rate,
    out_gain,
    out_weight,
):
    even = lax.axis_index("yl") == 0
    keep = jnp.where(even, tokens[0:2], tokens[2:4])
    give = jnp.where(even, tokens[2:4], tokens[0:2])
    got = shift(give, "yl", 1)
    left_a = shift(keep, "x", 1)
    right_a = shift(keep, "x", -1)
    left_b = shift(got, "x", 1)
    right_b = shift(got, "x", -1)
    far_a = shift(left_a, "x", 1)
    far_b = shift(right_b, "x", -1)
    here = (keep, left_a, right_a, got, left_b, right_b, far_a, far_b)
    there = tuple(shift(v, "c", 1) for v in here)

    weights = [x_weight, b_weight, c_weight, z_weight]
    weights = weights + [dt_weight.T, norm_gain.reshape(8, 128), out_weight.T]
    (w_own,) = call(
        prepare,
        (struct((88, 512)),),
        weights,
        [pltpu.VMEM(w.shape, w.dtype) for w in weights] + [DMA((7,))],
        hbm=range(7),
    )
    y_parts = [w_own] + [shift(w_own, ("yh", "yl"), d) for d in (1, 2, 3)]
    (w_line,) = call(gather_y, (struct((4, 88, 512)),), y_parts)
    w_back = shift(w_line, "z", 1)
    w_front = shift(w_line, "z", -1)
    w_far_a = shift(w_back[0:2], "z", 1)
    w_far_b = shift(w_front[2:4], "z", -1)
    w_in, steps, o_here = call(
        order_in,
        (struct((1024, 512)), struct((32, 1024)), struct((1024, 128))),
        [w_line, w_back, w_front, w_far_a, w_far_b],
    )

    half = struct((SEQS, SPAN, 128))
    first = struct((SEQS, T, 128))
    state = struct((SEQS, 128, 128), f32)
    far_s = pltpu.HBM(half.shape, bf16)
    lines = struct((SEQS, 64, 128), f32)
    totals_s = struct((SEQS, 8, 128), f32)
    first_s = struct((SEQS, T, 256), f32)
    xb, cr, zr, raw, tail, x0 = call(
        project_all,
        (
            struct((SEQS, SPAN, 256)),
            half,
            half,
            struct((SEQS, PIECES, 2, PIECE), f32),
            struct((SEQS, HALO, 384)),
            struct((SEQS, T, 256)),
        ),
        [*here, *there, w_in, steps],
        us=5,
    )
    outs = [o_here] + [shift(o_here, "x", d) for d in (1, 2, 3)]
    outs = outs + [shift(v, "c", 1) for v in outs]
    (w_out,) = call(
        order_out,
        (struct((1024, 1024)),),
        outs,
        [pltpu.VMEM((8, 1024, 128), bf16), DMA((8,))],
        hbm=range(8),
    )
    halo = shift(tail, LINE, 1)
    u, b, l, dt0, totals, part = call(
        span_state,
        (half, half, lines, first_s, totals_s, state),
        [dt_bias, decay_rate, xb, raw, x_conv, b_conv],
        [pltpu.VMEM((SPAN, 128), bf16), pltpu.VMEM((SPAN, 256), f32)],
        us=4,
        scalars=2,
    )
    u0, b0, pack = call(
        span_first,
        (first, first, struct((SEQS, 144, 128))),
        [x0, halo, x_conv, b_conv, dt0, totals, part],
    )
    near_pack = shift(pack, "yh", 1)
    one = struct((SPAN, 128))
    own = []
    for k in range(SEQS):
        own.append(
            call(
                (span_own_0, span_own_1)[k],
                (one, one, one),
                [u, b, u0, b0, l, cr, zr, halo, c_conv],
                [
                    pltpu.VMEM((SPAN, 128), bf16),
                    pltpu.VMEM((PIECES, 128, 128), bf16),
                    pltpu.VMEM((SPAN, 512), f32),
                ],
                us=2,
            )
        )
    total, before, l_before = call(
        combine_y,
        (struct((SEQS, 144, 128)), state, struct((SEQS, 8, 128), f32)),
        [pack, near_pack],
    )
    packs = [shift(total, "z", d) for d in (1, 2, 3)]
    (gated,) = call(
        finish,
        (struct((PIECES, SEQS, PIECE, 128)),),
        [*packs, before, l_before, *own[0], *own[1], out_gain[None]],
    )
    back = exchange(gated, GROUP)
    (out,) = call(project_out, (struct((256, 1024)),), [back, w_out])
    return out.reshape(2 * SEQS, PIECE, 1024)


def solution(mesh):
    torus = Mesh(mesh.devices.reshape(4, 2, 2, 4, 2), AXES)
    return jax.shard_map(
        local,
        mesh=torus,
        in_specs=(
            P(None, AXES, None),
            P(),
            P(SP, TP),
            P(SP, TP),
            P(SP, TP),
            P(SP, TP),
            P(SP, TP),
            P(None, TP),
            P(None, TP),
            P(None, TP),
            P(TP),
            P(TP),
            P(TP),
            P(TP, SP),
        ),
        out_specs=P(None, AXES, None),
        check_vma=False,
    )
```

```python
import jax
import jax.numpy as jnp
from jax import lax
from jax.experimental import pallas as pl
from jax.experimental.pallas import tpu as pltpu
from jax.sharding import Mesh
from jax.sharding import PartitionSpec as P


LENGTH = 8192
HEAD_P = 64
SEQS = 2
SPAN = 1024
PIECE = 64
PIECES = 16
T = 64
HALO = 16
EPS = 1e-05
AXES = ("z", "yh", "yl", "x", "c")
SP = ("z", "yh", "yl")
TP = ("x", "c")
LINE = ("z", "yh")
GROUP = ("yl", "x", "c")
bf16 = jnp.bfloat16
f32 = jnp.float32
VM = pl.BlockSpec(memory_space=pltpu.VMEM)
SM = pl.BlockSpec(memory_space=pltpu.SMEM)


HB = pl.BlockSpec(memory_space=pltpu.HBM)
DMA = pltpu.SemaphoreType.DMA


def call(body, outs, ins, scratch=(), mib=16, us=2, scalars=0, hbm=()):
    ins = [pltpu.with_memory_space_constraint(v, pltpu.HBM) if k in hbm else v for k, v in enumerate(ins)]
    return pl.pallas_call(
        body,
        out_shape=outs,
        in_specs=[SM if k < scalars else HB if k in hbm else VM for k in range(len(ins))],
        out_specs=tuple(VM if isinstance(o, jax.ShapeDtypeStruct) else HB for o in outs),
        scratch_shapes=list(scratch),
        compiler_params=pltpu.CompilerParams(vmem_limit_bytes=mib * 1024 * 1024),
        cost_estimate=pl.CostEstimate(
            flops=us * 1000000000, bytes_accessed=1 << 20, transcendentals=0
        ),
    )(*ins)


def fetch(pairs, sems):
    moves = [pltpu.make_async_copy(a, b, sems.at[k]) for k, (a, b) in enumerate(pairs)]
    for m in moves:
        m.start()
    return moves


def place():
    return [lax.axis_index(a) for a in AXES]


def shift(value, axis, d):
    n = lax.axis_size(axis)
    return lax.ppermute(value, axis, [(i, (i + d) % n) for i in range(n)])


def exchange(value, axes):
    return lax.all_to_all(value, axes, 0, 0, tiled=True)


def silu(v):
    h = 0.5 * v
    return h + h * jnp.tanh(h)


def softplus(v):
    return jnp.maximum(v, 0.0) + jnp.log1p(jnp.exp(-jnp.abs(v)))


def dot(a, b, dims=((1,), (0,))):
    return lax.dot_general(a, b, (dims, ((), ())), preferred_element_type=f32)


def prepare(*refs):
    ins, w_out, held, sems = refs[:7], refs[7], refs[8:15], refs[15]
    moves = fetch(list(zip(ins, held)), sems)
    for m in moves:
        m.wait()
    xw, bw, cw, zw, dw, gain, ow = held
    z, yh, yl, _, _ = place()
    sp = z * 4 + yh * 2 + yl
    row = gain[pl.ds(lax.div(sp, 2), 1), :]
    first = lax.rem(sp, 2) == 0
    row = jnp.where(first, row[:, 0:64], row[:, 64:128])
    row = jnp.concatenate([row, row], axis=1)
    g = jnp.broadcast_to(row, (128, 128)).T[0:64]
    dt = dw[...].astype(f32)
    dt = jnp.concatenate([dt[0:1], dt[1:2]], axis=1) * row
    dt = jnp.broadcast_to(dt, (8, 128)).astype(bf16)
    ws = [(v[...].astype(f32) * g).astype(bf16) for v in (xw, bw, cw, zw)]
    o = ow[...]
    for k in range(4):
        for j in range(4):
            w_out[k, 0:64, 128 * j : 128 * j + 128] = ws[j]
            w_out[k, 72:88, 128 * j : 128 * j + 128] = o[16 * j : 16 * j + 16]
        w_out[k, 64:72, 0:128] = dt
        w_out[k, 64:72, 128:512] = jnp.zeros((8, 384), bf16)


def order_in(p0, p1, p3, p2a, p2b, w, steps, o_out):
    z = lax.axis_index("z")
    for d in range(4):
        parts = [(p0, k) for k in range(4)]
        if d > 0:
            whole = {1: p1, 3: p3}.get(d)
            parts = [(whole, k) for k in range(4)] if whole is not None else [(p2a, 0), (p2a, 1), (p2b, 0), (p2b, 1)]
        first = lax.rem(z - d + 4, 4) * 256
        for k, (p, j) in enumerate(parts):
            at = pl.multiple_of(first + 64 * k, 64)
            w[pl.ds(at, 64), :] = p[j, 0:64, :]
            for n in range(4):
                o_out[pl.ds(at + 16 * n, 16), :] = p[j, 72:88, 128 * n : 128 * n + 128]
        at = pl.ds(pl.multiple_of(first, 256), 256)
        rows = [p[j, 64:72, 0:128].astype(f32)[0:1] for p, j in parts]
        for h in range(2):
            row = jnp.concatenate([v[:, 64 * h : 64 * h + 64] for v in rows], axis=1)
            steps[16 * h : 16 * h + 16, at] = jnp.broadcast_to(row, (16, 256)).astype(bf16)


def slots():
    _, _, yl, x, c = place()
    return [
        (half * 4 + lax.rem(x - d + 4, 4)) * 2 + core
        for core in (c, 1 - c)
        for half, d in ((yl, 0), (yl, 1), (yl, 3), (1 - yl, 0), (1 - yl, 1), (1 - yl, 3), (yl, 2), (1 - yl, 2))
    ]


def project_tail(*refs):
    pieces, w, tail, rows = refs[:16], refs[16], refs[17], refs[18]
    for slot, piece in zip(slots(), pieces):

        @pl.when(slot == PIECES - 1)
        def _(piece=piece):
            rows[...] = piece[:, PIECE - HALO :, :]

    v = rows[...].reshape(SEQS * HALO, 1024)
    wide = v.astype(f32)
    r = lax.rsqrt(jnp.mean(wide * wide, axis=1, keepdims=True) + EPS)
    tail[...] = (dot(v, w[:, 0:384]) * r).astype(bf16).reshape(SEQS, HALO, 384)


def project_all(*refs):
    here, there, (w, steps) = refs[:8], refs[8:16], refs[16:18]
    xb, cr, zr, dt_out, x0 = refs[18:]
    places = slots()
    lane = lax.broadcasted_iota(jnp.int32, (128, 128), 1)
    for k in range(2):
        pieces = [v[...] for v in (here, there)[k]]
        rows = jnp.concatenate([p.reshape(SEQS * PIECE, 1024) for p in pieces], axis=0)
        wide = rows.astype(f32)
        r = lax.rsqrt(jnp.mean(wide * wide, axis=1, keepdims=True) + EPS)
        part = (dot(rows, w[...]) * r).astype(bf16).reshape(8, SEQS, PIECE, 512)
        d0, d1 = (
            jnp.sum(wide * jnp.concatenate([steps[16 * h : 16 * h + 16, :]] * 64, axis=0).astype(f32), axis=1, keepdims=True) * r
            for h in range(2)
        )
        for j in range(8):
            slot = places[8 * k + j]
            at = pl.ds(pl.multiple_of(slot * PIECE, PIECE), PIECE)
            for s in range(SEQS):
                for ref, lo, n in ((xb, 0, 256), (cr, 256, 128), (zr, 384, 128)):
                    ref[s, at, :] = part[j, s, :, lo : lo + n]
            one = slice(128 * j, 128 * j + 128)
            turned = jnp.where(lane < 64, d0[one], d1[one]).T
            both = jnp.concatenate([turned[0:1], turned[64:65]], axis=0)
            for s in range(SEQS):
                dt_out[s, slot] = both[:, 64 * s : 64 * s + 64]
    x0[...] = xb[:, 0:T, :]


def entering(halo, s, lane, end):
    z, yh, _, _, _ = place()
    v = halo[s, :, lane:end].astype(f32)
    return jnp.where(2 * z + yh == 0, jnp.zeros_like(v), v)


def convolve(rows, taps):
    part = (0.5 * taps[0:1, :]) * rows
    for k in range(1, 4):
        part = (0.5 * taps[k : k + 1, :]) * rows + pltpu.roll(part, 1, 0)
    half = part[HALO:]
    return half + half * jnp.tanh(half)


def halves(v):
    hi = v.astype(bf16)
    return [hi, (v - hi.astype(f32)).astype(bf16)]


def spread(rows, groups):
    count = max(groups) + 1
    source = lax.broadcasted_iota(jnp.int32, (8 * len(rows), 128 * count), 0)
    lane = lax.broadcasted_iota(jnp.int32, (8 * len(rows), 128 * count), 1)
    hit = None
    for k, g in enumerate(groups):
        want = lane // HEAD_P - 2 * g + 8 * k
        mine = jnp.logical_and(lane // 128 == g, source == want)
        hit = mine if hit is None else jnp.logical_or(hit, mine)
    return dot(jnp.concatenate(rows, axis=0), hit.astype(f32).astype(bf16), ((0,), (0,)))


def offsets(lines):
    total, ahead = jnp.zeros((8, 1), f32), []
    for k in range(SPAN // T):
        ahead.append(total)
        end = (k % 2) * T + T - 1
        total = total + lines[8 * (k // 2) : 8 * (k // 2) + 8, end : end + 1]
    return ahead, total


def absolute(lines, ahead):
    first = lax.broadcasted_iota(jnp.int32, (8, 128), 1) < T
    parts = []
    for b in range(SPAN // 128):
        parts.append(lines[8 * b : 8 * b + 8] + jnp.where(first, ahead[2 * b], ahead[2 * b + 1]))
    return jnp.concatenate(parts, axis=0)


def span_state(
    bias, rates, xb, raw, x_taps, b_taps, u_v, b_v, l_out, d_out, t_out, s_out, late_v, wide
):
    row = lax.rem(lax.broadcasted_iota(jnp.int32, (64, 1), 0), 8)
    dtb = jnp.where(row == 0, bias[0], jnp.where(row == 1, bias[1], 0.0))
    rate = jnp.where(row == 0, rates[0], jnp.where(row == 1, rates[1], 0.0))
    row = lax.broadcasted_iota(jnp.int32, (128, 128), 0)
    col = lax.broadcasted_iota(jnp.int32, (128, 128), 1)
    sums = jnp.logical_and(row <= col, row // T == col // T).astype(f32).astype(bf16)
    none = jnp.zeros((6, 128), f32)
    for s in range(SEQS):
        steps = []
        for b in range(SPAN // 128):
            steps += [jnp.concatenate([raw[s, 2 * b], raw[s, 2 * b + 1]], axis=1), none]
        dt = softplus(jnp.concatenate(steps, axis=0) + dtb)
        ld = -(dt * rate) / LENGTH
        both = dot(jnp.concatenate(halves(ld), axis=0), sums)
        lines = both[0:64] + both[64:128]
        l_out[s] = lines
        ahead, total = offsets(lines)
        total_all = jnp.concatenate([total] * 8, axis=0)
        late = dt * jnp.exp(total_all - absolute(lines, ahead))
        rows = halves(dt) + halves(late)
        for b in range(SPAN // 128):
            block = [v[8 * b : 8 * b + 8] for v in rows]
            wide[128 * b : 128 * b + 128, :] = spread(block, (0, 0, 1, 1))
        d_out[s] = wide[0:T]
        head = lax.broadcasted_iota(jnp.int32, (1, 128), 1) < HEAD_P
        t_out[s] = jnp.broadcast_to(jnp.where(head, total[0:1], total[1:2]), (8, 128))
        for first in range(T, SPAN, 128):
            last = min(first + 128, SPAN)
            rows = xb[s, first - HALO : last, :].astype(f32)
            x = convolve(rows[:, 0:128], x_taps)
            u_v[s, first:last, :] = (x * wide[first:last, 0:128]).astype(bf16)
            late_v[first:last, :] = (x * wide[first:last, 128:256]).astype(bf16)
            b_v[s, first:last, :] = convolve(rows[:, 128:256], b_taps).astype(bf16)
        s_out[s] = dot(b_v[s, T:, :], late_v[T:, :], ((0,), (0,)))


def two_parts(row):
    high = row.astype(bf16).astype(f32)
    which = lax.broadcasted_iota(jnp.int32, (16, 128), 0)
    return jnp.where(which == 0, high, jnp.where(which == 1, row - high, 0.0)).astype(bf16)


def log_of(pack, s):
    return pack[s, 128:129, :].astype(f32) + pack[s, 129:130, :].astype(f32)


def span_first(x0, halo, x_taps, b_taps, dt, totals, part, u_out, b_out, pack):
    for s in range(SEQS):
        rows = jnp.concatenate([entering(halo, s, 0, 256), x0[s].astype(f32)], axis=0)
        total = totals[s, 0:1, :]
        x = convolve(rows[:, 0:128], x_taps)
        b = convolve(rows[:, 128:256], b_taps).astype(bf16)
        u_out[s] = (x * dt[s, :, 0:128]).astype(bf16)
        b_out[s] = b
        late = (x * dt[s, :, 128:256]).astype(bf16)
        state = (part[s] + dot(b, late, ((0,), (0,)))).astype(bf16)
        pack[s, 0:128, :] = state
        pack[s, 128:144, :] = two_parts(total)


def span_own(s, u, b, u0, b0, l, cr, zr, halo, taps, y_out, c_out, e_out, mv, sv, wide):
    row = lax.broadcasted_iota(jnp.int32, (T, 128), 0)
    col = lax.rem(lax.broadcasted_iota(jnp.int32, (T, 128), 1), T)
    seen = col <= row
    left = lax.broadcasted_iota(jnp.int32, (T, 128), 1) < T
    first = lax.broadcasted_iota(jnp.int32, (8, 128), 1) < T
    lines = l[s]
    ahead, _ = offsets(lines)
    past = absolute(lines, ahead)
    for k in range(SPAN // 128):
        v = lines[8 * k : 8 * k + 8]
        rest = jnp.where(first, v[:, T - 1 : T], v[:, 2 * T - 1 : 2 * T]) - v
        rows = halves(v)
        rows += [jnp.exp(r).astype(bf16) for r in (v, rest, past[8 * k : 8 * k + 8])]
        wide[128 * k : 128 * k + 128, :] = spread(rows, (0, 0, 1, 2, 3))
    for k in range(0, SPAN, 128):
        if k == 0:
            rows = jnp.concatenate([entering(halo, s, 256, 384), cr[s, 0:128, :].astype(f32)], axis=0)
        else:
            rows = cr[s, k - HALO : k + 128, :].astype(f32)
        c_out[k : k + 128, :] = convolve(rows, taps).astype(bf16)
    chunks = [(k, slice(k * T, k * T + T)) for k in range(SPAN // T)]

    def rows_of(start, later, k, at):
        return start[s] if k == 0 else later[s, at, :]

    for k, at in chunks:
        bc = rows_of(b0, b, k, at)
        half = slice((k % 2) * T, (k % 2) * T + T)
        at_8 = 8 * (k // 2)
        l_row = jnp.concatenate([l[s, at_8 : at_8 + 1, half], l[s, at_8 + 1 : at_8 + 2, half]], axis=1)
        pairs = dot(c_out[at, :], jnp.concatenate([bc, bc], axis=0), ((1,), (1,)))
        gap = jnp.exp(jnp.where(seen, wide[at, 0:128] - l_row, -jnp.inf))
        mv[at, :] = (pairs * gap).astype(bf16)
    state = jnp.zeros((128, 128), f32)
    for k, at in chunks[:-1]:
        late = (rows_of(u0, u, k, at).astype(f32) * wide[at, 256:384]).astype(bf16)
        fresh = dot(rows_of(b0, b, k, at), late, ((0,), (0,)))
        state = state * wide[k * T + T - 1 : k * T + T, 128:256] + fresh
        sv[k + 1] = state.astype(bf16)
    for k, at in chunks:
        uc = rows_of(u0, u, k, at)
        zero = jnp.zeros_like(uc)
        blocks = jnp.concatenate([jnp.where(left, uc, zero), jnp.where(left, zero, uc)], axis=0)
        y = dot(mv[at, :], blocks)
        if k > 0:
            y = y + dot(c_out[at, :], sv[k]) * wide[at, 128:256]
        gate = silu(zr[s, at, :].astype(f32))
        e_out[at, :] = (gate * wide[at, 384:512]).astype(bf16)
        y_out[at, :] = (y * gate).astype(bf16)


def span_own_0(*refs):
    span_own(0, *refs)


def span_own_1(*refs):
    span_own(1, *refs)


def combine_y(mine, other, total, before, l_before):
    late = lax.axis_index("yh") == 1
    for s in range(SEQS):
        log_0, log_1 = log_of(mine, s), log_of(other, s)
        state_0, state_1 = mine[s, 0:128, :].astype(f32), other[s, 0:128, :].astype(f32)
        ahead = state_0 * jnp.exp(log_1) + state_1
        behind = state_1 * jnp.exp(log_0) + state_0
        total[s, 0:128, :] = jnp.where(late, behind, ahead).astype(bf16)
        total[s, 128:144, :] = two_parts(log_0 + log_1)
        before[s] = jnp.where(late, state_1, jnp.zeros_like(state_1))
        l_before[s] = jnp.broadcast_to(jnp.where(late, log_1, jnp.zeros_like(log_1)), (8, 128))


def finish(*refs):
    packs, (before, l_before), own, (gain, out) = refs[:3], refs[3:5], refs[5:11], refs[11:]
    z = lax.axis_index("z")
    for s in range(SEQS):
        y_own, cc, decay = own[3 * s : 3 * s + 3]
        log = l_before[s, 0:1, :]
        state = before[s]
        for d in range(1, 4):
            past = packs[d - 1][s, 0:128, :].astype(f32)
            state = state + jnp.where(d <= z, past * jnp.exp(log), jnp.zeros_like(past))
            log = log + log_of(packs[d - 1], s)
        g = y_own[...].astype(f32) + dot(cc[...], state.astype(bf16)) * decay[...].astype(f32)
        g = g * lax.rsqrt(jnp.mean(g * g, axis=1, keepdims=True) + EPS) * gain[...]
        g = g.astype(bf16)
        for k in range(PIECES):
            out[k, s] = g[k * PIECE : k * PIECE + PIECE, :]


def order_out(*refs):
    ins, out, held, sems = refs[:8], refs[8], refs[9], refs[10]
    moves = fetch([(r, held.at[k]) for k, r in enumerate(ins)], sems)
    _, _, _, x, c = place()
    for core in range(2):
        half = lax.rem(c + core, 2)
        for d in range(4):
            at = pl.multiple_of((2 * lax.rem(x - d + 4, 4) + half) * 128, 128)
            moves[4 * core + d].wait()
            out[pl.ds(at, 128), :] = held[4 * core + d].astype(f32).T.astype(bf16)


def project_out(g, w, out):
    for k in range(2):
        rows = jnp.concatenate([g[8 * k + j].reshape(SEQS * PIECE, 128) for j in range(8)], axis=1)
        out[128 * k : 128 * k + 128, :] = dot(rows, w[...]).astype(bf16)


def struct(shape, kind=bf16):
    return jax.ShapeDtypeStruct(shape, kind)


def local(
    tokens,
    norm_gain,
    x_weight,
    z_weight,
    b_weight,
    c_weight,
    dt_weight,
    x_conv,
    b_conv,
    c_conv,
    dt_bias,
    decay_rate,
    out_gain,
    out_weight,
):
    even = lax.axis_index("yl") == 0
    keep = jnp.where(even, tokens[0:2], tokens[2:4])
    give = jnp.where(even, tokens[2:4], tokens[0:2])
    got = shift(give, "yl", 1)
    left_a = shift(keep, "x", 1)
    right_a = shift(keep, "x", -1)
    left_b = shift(got, "x", 1)
    right_b = shift(got, "x", -1)
    far_a = shift(left_a, "x", 1)
    far_b = shift(right_b, "x", -1)
    here = (keep, left_a, right_a, got, left_b, right_b, far_a, far_b)
    there = tuple(shift(v, "c", 1) for v in here)

    weights = [x_weight, b_weight, c_weight, z_weight]
    weights = weights + [dt_weight.T, norm_gain.reshape(8, 128), out_weight.T]
    (w_own,) = call(
        prepare,
        (struct((4, 88, 512)),),
        weights,
        [pltpu.VMEM(w.shape, w.dtype) for w in weights] + [DMA((7,))],
        hbm=range(7),
    )
    w_line = exchange(w_own, ("yh", "yl"))
    w_back = shift(w_line, "z", 1)
    w_front = shift(w_line, "z", -1)
    w_far_a = shift(w_back[0:2], "z", 1)
    w_far_b = shift(w_front[2:4], "z", -1)
    w_in, steps, o_here = call(
        order_in,
        (struct((1024, 512)), struct((32, 1024)), struct((1024, 128))),
        [w_line, w_back, w_front, w_far_a, w_far_b],
    )

    half = struct((SEQS, SPAN, 128))
    first = struct((SEQS, T, 128))
    state = struct((SEQS, 128, 128), f32)
    far_s = pltpu.HBM(half.shape, bf16)
    lines = struct((SEQS, 64, 128), f32)
    totals_s = struct((SEQS, 8, 128), f32)
    first_s = struct((SEQS, T, 256), f32)
    (tail,) = call(
        project_tail,
        (struct((SEQS, HALO, 384)),),
        [*here, *there, w_in],
        [pltpu.VMEM((SEQS, HALO, 1024), bf16)],
        us=1,
    )
    halo = shift(tail, LINE, 1)
    xb, cr, zr, raw, x0 = call(
        project_all,
        (
            struct((SEQS, SPAN, 256)),
            half,
            half,
            struct((SEQS, PIECES, 2, PIECE), f32),
            struct((SEQS, T, 256)),
        ),
        [*here, *there, w_in, steps],
        us=5,
    )
    outs = [o_here] + [shift(o_here, "x", d) for d in (1, 2, 3)]
    outs = outs + [shift(v, "c", 1) for v in outs]
    (w_out,) = call(
        order_out,
        (struct((1024, 1024)),),
        outs,
        [pltpu.VMEM((8, 1024, 128), bf16), DMA((8,))],
        hbm=range(8),
    )
    u, b, l, dt0, totals, part = call(
        span_state,
        (half, half, lines, first_s, totals_s, state),
        [dt_bias, decay_rate, xb, raw, x_conv, b_conv],
        [pltpu.VMEM((SPAN, 128), bf16), pltpu.VMEM((SPAN, 256), f32)],
        us=4,
        scalars=2,
    )
    u0, b0, pack = call(
        span_first,
        (first, first, struct((SEQS, 144, 128))),
        [x0, halo, x_conv, b_conv, dt0, totals, part],
    )
    near_pack = shift(pack, "yh", 1)
    one = struct((SPAN, 128))
    own = []
    for k in range(SEQS):
        own.append(
            call(
                (span_own_0, span_own_1)[k],
                (one, one, one),
                [u, b, u0, b0, l, cr, zr, halo, c_conv],
                [
                    pltpu.VMEM((SPAN, 128), bf16),
                    pltpu.VMEM((PIECES, 128, 128), bf16),
                    pltpu.VMEM((SPAN, 512), f32),
                ],
                us=2,
            )
        )
    total, before, l_before = call(
        combine_y,
        (struct((SEQS, 144, 128)), state, struct((SEQS, 8, 128), f32)),
        [pack, near_pack],
    )
    packs = [shift(total, "z", d) for d in (1, 2, 3)]
    (gated,) = call(
        finish,
        (struct((PIECES, SEQS, PIECE, 128)),),
        [*packs, before, l_before, *own[0], *own[1], out_gain[None]],
    )
    back = exchange(gated, GROUP)
    (out,) = call(project_out, (struct((256, 1024)),), [back, w_out])
    return out.reshape(2 * SEQS, PIECE, 1024)


def solution(mesh):
    torus = Mesh(mesh.devices.reshape(4, 2, 2, 4, 2), AXES)
    return jax.shard_map(
        local,
        mesh=torus,
        in_specs=(
            P(None, AXES, None),
            P(),
            P(SP, TP),
            P(SP, TP),
            P(SP, TP),
            P(SP, TP),
            P(SP, TP),
            P(None, TP),
            P(None, TP),
            P(None, TP),
            P(TP),
            P(TP),
            P(TP),
            P(TP, SP),
        ),
        out_specs=P(None, AXES, None),
        check_vma=False,
    )
```

```python
import jax
import jax.numpy as jnp
from jax import lax
from jax.experimental import pallas as pl
from jax.experimental.pallas import tpu as pltpu
from jax.sharding import Mesh
from jax.sharding import PartitionSpec as P


LENGTH = 8192
HEAD_P = 64
SEQS = 2
SPAN = 1024
PIECE = 64
PIECES = 16
T = 64
HALO = 16
EPS = 1e-05
AXES = ("z", "yh", "yl", "x", "c")
SP = ("z", "yh", "yl")
TP = ("x", "c")
LINE = ("z", "yh")
GROUP = ("yl", "x", "c")
bf16 = jnp.bfloat16
f32 = jnp.float32
VM = pl.BlockSpec(memory_space=pltpu.VMEM)
SM = pl.BlockSpec(memory_space=pltpu.SMEM)


HB = pl.BlockSpec(memory_space=pltpu.HBM)
DMA = pltpu.SemaphoreType.DMA


def call(body, outs, ins, scratch=(), mib=16, us=2, scalars=0, hbm=()):
    ins = [pltpu.with_memory_space_constraint(v, pltpu.HBM) if k in hbm else v for k, v in enumerate(ins)]
    return pl.pallas_call(
        body,
        out_shape=outs,
        in_specs=[SM if k < scalars else HB if k in hbm else VM for k in range(len(ins))],
        out_specs=tuple(VM if isinstance(o, jax.ShapeDtypeStruct) else HB for o in outs),
        scratch_shapes=list(scratch),
        compiler_params=pltpu.CompilerParams(vmem_limit_bytes=mib * 1024 * 1024),
        cost_estimate=pl.CostEstimate(
            flops=us * 1000000000, bytes_accessed=1 << 20, transcendentals=0
        ),
    )(*ins)


def fetch(pairs, sems):
    moves = [pltpu.make_async_copy(a, b, sems.at[k]) for k, (a, b) in enumerate(pairs)]
    for m in moves:
        m.start()
    return moves


def place():
    return [lax.axis_index(a) for a in AXES]


def shift(value, axis, d):
    n = lax.axis_size(axis)
    return lax.ppermute(value, axis, [(i, (i + d) % n) for i in range(n)])


def exchange(value, axes):
    return lax.all_to_all(value, axes, 0, 0, tiled=True)


def silu(v):
    h = 0.5 * v
    return h + h * jnp.tanh(h)


def softplus(v):
    return jnp.maximum(v, 0.0) + jnp.log1p(jnp.exp(-jnp.abs(v)))


def dot(a, b, dims=((1,), (0,))):
    return lax.dot_general(a, b, (dims, ((), ())), preferred_element_type=f32)


def prepare(*refs):
    ins, w_out, held, sems = refs[:7], refs[7], refs[8:15], refs[15]
    moves = fetch(list(zip(ins, held)), sems)
    for m in moves:
        m.wait()
    xw, bw, cw, zw, dw, gain, ow = held
    z, yh, yl, _, _ = place()
    sp = z * 4 + yh * 2 + yl
    row = gain[pl.ds(lax.div(sp, 2), 1), :]
    first = lax.rem(sp, 2) == 0
    row = jnp.where(first, row[:, 0:64], row[:, 64:128])
    row = jnp.concatenate([row, row], axis=1)
    g = jnp.broadcast_to(row, (128, 128)).T[0:64]
    dt = dw[...].astype(f32)
    dt = jnp.concatenate([dt[0:1], dt[1:2]], axis=1) * row
    dt = jnp.broadcast_to(dt, (8, 128)).astype(bf16)
    ws = [(v[...].astype(f32) * g).astype(bf16) for v in (xw, bw, cw, zw)]
    o = ow[...]
    for j in range(4):
        w_out[0:64, 128 * j : 128 * j + 128] = ws[j]
    w_out[64:72, 0:128] = dt
    w_out[64:72, 128:512] = jnp.zeros((8, 384), bf16)
    for j in range(4):
        w_out[72:88, 128 * j : 128 * j + 128] = o[16 * j : 16 * j + 16]


def gather_y(p0, p1, p2, p3, out):
    _, yh, yl, _, _ = place()
    for d, p in enumerate((p0, p1, p2, p3)):
        out[lax.rem(2 * yh + yl - d + 4, 4)] = p[...]


def order_in(p0, p1, p3, p2a, p2b, w, steps, o_out):
    z = lax.axis_index("z")
    for d in range(4):
        parts = [(p0, k) for k in range(4)]
        if d > 0:
            whole = {1: p1, 3: p3}.get(d)
            parts = [(whole, k) for k in range(4)] if whole is not None else [(p2a, 0), (p2a, 1), (p2b, 0), (p2b, 1)]
        first = lax.rem(z - d + 4, 4) * 256
        for k, (p, j) in enumerate(parts):
            at = pl.multiple_of(first + 64 * k, 64)
            w[pl.ds(at, 64), :] = p[j, 0:64, :]
            for n in range(4):
                o_out[pl.ds(at + 16 * n, 16), :] = p[j, 72:88, 128 * n : 128 * n + 128]
        at = pl.ds(pl.multiple_of(first, 256), 256)
        rows = [p[j, 64:72, 0:128].astype(f32)[0:1] for p, j in parts]
        for h in range(2):
            row = jnp.concatenate([v[:, 64 * h : 64 * h + 64] for v in rows], axis=1)
            steps[16 * h : 16 * h + 16, at] = jnp.broadcast_to(row, (16, 256)).astype(bf16)


def slots():
    _, _, yl, x, c = place()
    return [
        (half * 4 + lax.rem(x - d + 4, 4)) * 2 + core
        for core in (c, 1 - c)
        for half, d in ((yl, 0), (yl, 1), (yl, 3), (1 - yl, 0), (1 - yl, 1), (1 - yl, 3), (yl, 2), (1 - yl, 2))
    ]


def project_tail(*refs):
    pieces, w, tail, rows = refs[:16], refs[16], refs[17], refs[18]
    for slot, piece in zip(slots(), pieces):

        @pl.when(slot == PIECES - 1)
        def _(piece=piece):
            rows[...] = piece[:, PIECE - HALO :, :]

    v = rows[...].reshape(SEQS * HALO, 1024)
    wide = v.astype(f32)
    r = lax.rsqrt(jnp.mean(wide * wide, axis=1, keepdims=True) + EPS)
    tail[...] = (dot(v, w[:, 0:384]) * r).astype(bf16).reshape(SEQS, HALO, 384)


def project_all(*refs):
    here, there, (w, steps) = refs[:8], refs[8:16], refs[16:18]
    xb, cr, zr, dt_out, x0 = refs[18:]
    places = slots()
    lane = lax.broadcasted_iota(jnp.int32, (128, 128), 1)
    for k in range(2):
        pieces = [v[...] for v in (here, there)[k]]
        rows = jnp.concatenate([p.reshape(SEQS * PIECE, 1024) for p in pieces], axis=0)
        wide = rows.astype(f32)
        r = lax.rsqrt(jnp.mean(wide * wide, axis=1, keepdims=True) + EPS)
        part = (dot(rows, w[...]) * r).astype(bf16).reshape(8, SEQS, PIECE, 512)
        d0, d1 = (
            jnp.sum(wide * jnp.concatenate([steps[16 * h : 16 * h + 16, :]] * 64, axis=0).astype(f32), axis=1, keepdims=True) * r
            for h in range(2)
        )
        for j in range(8):
            slot = places[8 * k + j]
            at = pl.ds(pl.multiple_of(slot * PIECE, PIECE), PIECE)
            for s in range(SEQS):
                for ref, lo, n in ((xb, 0, 256), (cr, 256, 128), (zr, 384, 128)):
                    ref[s, at, :] = part[j, s, :, lo : lo + n]
            one = slice(128 * j, 128 * j + 128)
            turned = jnp.where(lane < 64, d0[one], d1[one]).T
            both = jnp.concatenate([turned[0:1], turned[64:65]], axis=0)
            for s in range(SEQS):
                dt_out[s, slot] = both[:, 64 * s : 64 * s + 64]
    x0[...] = xb[:, 0:T, :]


def entering(halo, s, lane, end):
    z, yh, _, _, _ = place()
    v = halo[s, :, lane:end].astype(f32)
    return jnp.where(2 * z + yh == 0, jnp.zeros_like(v), v)


def convolve(rows, taps):
    part = (0.5 * taps[0:1, :]) * rows
    for k in range(1, 4):
        part = (0.5 * taps[k : k + 1, :]) * rows + pltpu.roll(part, 1, 0)
    half = part[HALO:]
    return half + half * jnp.tanh(half)


def halves(v):
    hi = v.astype(bf16)
    return [hi, (v - hi.astype(f32)).astype(bf16)]


def spread(rows, groups):
    count = max(groups) + 1
    source = lax.broadcasted_iota(jnp.int32, (8 * len(rows), 128 * count), 0)
    lane = lax.broadcasted_iota(jnp.int32, (8 * len(rows), 128 * count), 1)
    hit = None
    for k, g in enumerate(groups):
        want = lane // HEAD_P - 2 * g + 8 * k
        mine = jnp.logical_and(lane // 128 == g, source == want)
        hit = mine if hit is None else jnp.logical_or(hit, mine)
    return dot(jnp.concatenate(rows, axis=0), hit.astype(f32).astype(bf16), ((0,), (0,)))


def offsets(lines):
    total, ahead = jnp.zeros((8, 1), f32), []
    for k in range(SPAN // T):
        ahead.append(total)
        end = (k % 2) * T + T - 1
        total = total + lines[8 * (k // 2) : 8 * (k // 2) + 8, end : end + 1]
    return ahead, total


def absolute(lines, ahead):
    first = lax.broadcasted_iota(jnp.int32, (8, 128), 1) < T
    parts = []
    for b in range(SPAN // 128):
        parts.append(lines[8 * b : 8 * b + 8] + jnp.where(first, ahead[2 * b], ahead[2 * b + 1]))
    return jnp.concatenate(parts, axis=0)


def span_state(
    bias, rates, xb, raw, x_taps, b_taps, u_v, b_v, l_out, d_out, t_out, s_out, late_v, wide
):
    row = lax.rem(lax.broadcasted_iota(jnp.int32, (64, 1), 0), 8)
    dtb = jnp.where(row == 0, bias[0], jnp.where(row == 1, bias[1], 0.0))
    rate = jnp.where(row == 0, rates[0], jnp.where(row == 1, rates[1], 0.0))
    row = lax.broadcasted_iota(jnp.int32, (128, 128), 0)
    col = lax.broadcasted_iota(jnp.int32, (128, 128), 1)
    sums = jnp.logical_and(row <= col, row // T == col // T).astype(f32).astype(bf16)
    none = jnp.zeros((6, 128), f32)
    for s in range(SEQS):
        steps = []
        for b in range(SPAN // 128):
            steps += [jnp.concatenate([raw[s, 2 * b], raw[s, 2 * b + 1]], axis=1), none]
        dt = softplus(jnp.concatenate(steps, axis=0) + dtb)
        ld = -(dt * rate) / LENGTH
        both = dot(jnp.concatenate(halves(ld), axis=0), sums)
        lines = both[0:64] + both[64:128]
        l_out[s] = lines
        ahead, total = offsets(lines)
        total_all = jnp.concatenate([total] * 8, axis=0)
        late = dt * jnp.exp(total_all - absolute(lines, ahead))
        rows = halves(dt) + halves(late)
        for b in range(SPAN // 128):
            block = [v[8 * b : 8 * b + 8] for v in rows]
            wide[128 * b : 128 * b + 128, :] = spread(block, (0, 0, 1, 1))
        d_out[s] = wide[0:T]
        head = lax.broadcasted_iota(jnp.int32, (1, 128), 1) < HEAD_P
        t_out[s] = jnp.broadcast_to(jnp.where(head, total[0:1], total[1:2]), (8, 128))
        for first in range(T, SPAN, 128):
            last = min(first + 128, SPAN)
            rows = xb[s, first - HALO : last, :].astype(f32)
            x = convolve(rows[:, 0:128], x_taps)
            u_v[s, first:last, :] = (x * wide[first:last, 0:128]).astype(bf16)
            late_v[first:last, :] = (x * wide[first:last, 128:256]).astype(bf16)
            b_v[s, first:last, :] = convolve(rows[:, 128:256], b_taps).astype(bf16)
        s_out[s] = dot(b_v[s, T:, :], late_v[T:, :], ((0,), (0,)))


def two_parts(row):
    high = row.astype(bf16).astype(f32)
    which = lax.broadcasted_iota(jnp.int32, (16, 128), 0)
    return jnp.where(which == 0, high, jnp.where(which == 1, row - high, 0.0)).astype(bf16)


def log_of(pack, s):
    return pack[s, 128:129, :].astype(f32) + pack[s, 129:130, :].astype(f32)


def span_first(x0, halo, x_taps, b_taps, dt, totals, part, u_out, b_out, pack):
    for s in range(SEQS):
        rows = jnp.concatenate([entering(halo, s, 0, 256), x0[s].astype(f32)], axis=0)
        total = totals[s, 0:1, :]
        x = convolve(rows[:, 0:128], x_taps)
        b = convolve(rows[:, 128:256], b_taps).astype(bf16)
        u_out[s] = (x * dt[s, :, 0:128]).astype(bf16)
        b_out[s] = b
        late = (x * dt[s, :, 128:256]).astype(bf16)
        state = (part[s] + dot(b, late, ((0,), (0,)))).astype(bf16)
        pack[s, 0:128, :] = state
        pack[s, 128:144, :] = two_parts(total)


def span_own(s, u, b, u0, b0, l, cr, zr, halo, taps, y_out, c_out, e_out, mv, sv, wide):
    row = lax.broadcasted_iota(jnp.int32, (T, 128), 0)
    col = lax.rem(lax.broadcasted_iota(jnp.int32, (T, 128), 1), T)
    seen = col <= row
    left = lax.broadcasted_iota(jnp.int32, (T, 128), 1) < T
    first = lax.broadcasted_iota(jnp.int32, (8, 128), 1) < T
    lines = l[s]
    ahead, _ = offsets(lines)
    past = absolute(lines, ahead)
    for k in range(SPAN // 128):
        v = lines[8 * k : 8 * k + 8]
        rest = jnp.where(first, v[:, T - 1 : T], v[:, 2 * T - 1 : 2 * T]) - v
        rows = halves(v)
        rows += [jnp.exp(r).astype(bf16) for r in (v, rest, past[8 * k : 8 * k + 8])]
        wide[128 * k : 128 * k + 128, :] = spread(rows, (0, 0, 1, 2, 3))
    for k in range(0, SPAN, 128):
        if k == 0:
            rows = jnp.concatenate([entering(halo, s, 256, 384), cr[s, 0:128, :].astype(f32)], axis=0)
        else:
            rows = cr[s, k - HALO : k + 128, :].astype(f32)
        c_out[k : k + 128, :] = convolve(rows, taps).astype(bf16)
    chunks = [(k, slice(k * T, k * T + T)) for k in range(SPAN // T)]

    def rows_of(start, later, k, at):
        return start[s] if k == 0 else later[s, at, :]

    for k, at in chunks:
        bc = rows_of(b0, b, k, at)
        half = slice((k % 2) * T, (k % 2) * T + T)
        at_8 = 8 * (k // 2)
        l_row = jnp.concatenate([l[s, at_8 : at_8 + 1, half], l[s, at_8 + 1 : at_8 + 2, half]], axis=1)
        pairs = dot(c_out[at, :], jnp.concatenate([bc, bc], axis=0), ((1,), (1,)))
        gap = jnp.exp(jnp.where(seen, wide[at, 0:128] - l_row, -jnp.inf))
        mv[at, :] = (pairs * gap).astype(bf16)
    state = jnp.zeros((128, 128), f32)
    for k, at in chunks[:-1]:
        late = (rows_of(u0, u, k, at).astype(f32) * wide[at, 256:384]).astype(bf16)
        fresh = dot(rows_of(b0, b, k, at), late, ((0,), (0,)))
        state = state * wide[k * T + T - 1 : k * T + T, 128:256] + fresh
        sv[k + 1] = state.astype(bf16)
    for k, at in chunks:
        uc = rows_of(u0, u, k, at)
        zero = jnp.zeros_like(uc)
        blocks = jnp.concatenate([jnp.where(left, uc, zero), jnp.where(left, zero, uc)], axis=0)
        y = dot(mv[at, :], blocks)
        if k > 0:
            y = y + dot(c_out[at, :], sv[k]) * wide[at, 128:256]
        gate = silu(zr[s, at, :].astype(f32))
        e_out[at, :] = (gate * wide[at, 384:512]).astype(bf16)
        y_out[at, :] = (y * gate).astype(bf16)


def span_own_0(*refs):
    span_own(0, *refs)


def span_own_1(*refs):
    span_own(1, *refs)


def combine_y(mine, other, total, before, l_before):
    late = lax.axis_index("yh") == 1
    for s in range(SEQS):
        log_0, log_1 = log_of(mine, s), log_of(other, s)
        state_0, state_1 = mine[s, 0:128, :].astype(f32), other[s, 0:128, :].astype(f32)
        ahead = state_0 * jnp.exp(log_1) + state_1
        behind = state_1 * jnp.exp(log_0) + state_0
        total[s, 0:128, :] = jnp.where(late, behind, ahead).astype(bf16)
        total[s, 128:144, :] = two_parts(log_0 + log_1)
        before[s] = jnp.where(late, state_1, jnp.zeros_like(state_1))
        l_before[s] = jnp.broadcast_to(jnp.where(late, log_1, jnp.zeros_like(log_1)), (8, 128))


def finish(*refs):
    packs, (before, l_before), own, (gain, out) = refs[:3], refs[3:5], refs[5:11], refs[11:]
    z = lax.axis_index("z")
    for s in range(SEQS):
        y_own, cc, decay = own[3 * s : 3 * s + 3]
        log = l_before[s, 0:1, :]
        state = before[s]
        for d in range(1, 4):
            past = packs[d - 1][s, 0:128, :].astype(f32)
            state = state + jnp.where(d <= z, past * jnp.exp(log), jnp.zeros_like(past))
            log = log + log_of(packs[d - 1], s)
        g = y_own[...].astype(f32) + dot(cc[...], state.astype(bf16)) * decay[...].astype(f32)
        g = g * lax.rsqrt(jnp.mean(g * g, axis=1, keepdims=True) + EPS) * gain[...]
        g = g.astype(bf16)
        for k in range(PIECES):
            out[k, s] = g[k * PIECE : k * PIECE + PIECE, :]


def order_out(*refs):
    ins, out, held, sems = refs[:8], refs[8], refs[9], refs[10]
    moves = fetch([(r, held.at[k]) for k, r in enumerate(ins)], sems)
    _, _, _, x, c = place()
    for core in range(2):
        half = lax.rem(c + core, 2)
        for d in range(4):
            at = pl.multiple_of((2 * lax.rem(x - d + 4, 4) + half) * 128, 128)
            moves[4 * core + d].wait()
            out[pl.ds(at, 128), :] = held[4 * core + d].astype(f32).T.astype(bf16)


def project_out(g, w, out):
    for k in range(2):
        rows = jnp.concatenate([g[8 * k + j].reshape(SEQS * PIECE, 128) for j in range(8)], axis=1)
        out[128 * k : 128 * k + 128, :] = dot(rows, w[...]).astype(bf16)


def struct(shape, kind=bf16):
    return jax.ShapeDtypeStruct(shape, kind)


def local(
    tokens,
    norm_gain,
    x_weight,
    z_weight,
    b_weight,
    c_weight,
    dt_weight,
    x_conv,
    b_conv,
    c_conv,
    dt_bias,
    decay_rate,
    out_gain,
    out_weight,
):
    even = lax.axis_index("yl") == 0
    keep = jnp.where(even, tokens[0:2], tokens[2:4])
    give = jnp.where(even, tokens[2:4], tokens[0:2])
    got = shift(give, "yl", 1)
    left_a = shift(keep, "x", 1)
    right_a = shift(keep, "x", -1)
    left_b = shift(got, "x", 1)
    right_b = shift(got, "x", -1)
    far_a = shift(left_a, "x", 1)
    far_b = shift(right_b, "x", -1)
    here = (keep, left_a, right_a, got, left_b, right_b, far_a, far_b)
    there = tuple(shift(v, "c", 1) for v in here)

    weights = [x_weight, b_weight, c_weight, z_weight]
    weights = weights + [dt_weight.T, norm_gain.reshape(8, 128), out_weight.T]
    (w_own,) = call(
        prepare,
        (struct((88, 512)),),
        weights,
        [pltpu.VMEM(w.shape, w.dtype) for w in weights] + [DMA((7,))],
        hbm=range(7),
    )
    y_parts = [w_own] + [shift(w_own, ("yh", "yl"), d) for d in (1, 2, 3)]
    (w_line,) = call(gather_y, (struct((4, 88, 512)),), y_parts)
    w_back = shift(w_line, "z", 1)
    w_front = shift(w_line, "z", -1)
    w_far_a = shift(w_back[0:2], "z", 1)
    w_far_b = shift(w_front[2:4], "z", -1)
    w_in, steps, o_here = call(
        order_in,
        (struct((1024, 512)), struct((32, 1024)), struct((1024, 128))),
        [w_line, w_back, w_front, w_far_a, w_far_b],
    )

    half = struct((SEQS, SPAN, 128))
    first = struct((SEQS, T, 128))
    state = struct((SEQS, 128, 128), f32)
    far_s = pltpu.HBM(half.shape, bf16)
    lines = struct((SEQS, 64, 128), f32)
    totals_s = struct((SEQS, 8, 128), f32)
    first_s = struct((SEQS, T, 256), f32)
    (tail,) = call(
        project_tail,
        (struct((SEQS, HALO, 384)),),
        [*here, *there, w_in],
        [pltpu.VMEM((SEQS, HALO, 1024), bf16)],
        us=1,
    )
    halo = shift(tail, LINE, 1)
    xb, cr, zr, raw, x0 = call(
        project_all,
        (
            struct((SEQS, SPAN, 256)),
            half,
            half,
            struct((SEQS, PIECES, 2, PIECE), f32),
            struct((SEQS, T, 256)),
        ),
        [*here, *there, w_in, steps],
        us=5,
    )
    outs = [o_here] + [shift(o_here, "x", d) for d in (1, 2, 3)]
    outs = outs + [shift(v, "c", 1) for v in outs]
    (w_out,) = call(
        order_out,
        (struct((1024, 1024)),),
        outs,
        [pltpu.VMEM((8, 1024, 128), bf16), DMA((8,))],
        hbm=range(8),
    )
    u, b, l, dt0, totals, part = call(
        span_state,
        (half, half, lines, first_s, totals_s, state),
        [dt_bias, decay_rate, xb, raw, x_conv, b_conv],
        [pltpu.VMEM((SPAN, 128), bf16), pltpu.VMEM((SPAN, 256), f32)],
        us=4,
        scalars=2,
    )
    u0, b0, pack = call(
        span_first,
        (first, first, struct((SEQS, 144, 128))),
        [x0, halo, x_conv, b_conv, dt0, totals, part],
    )
    near_pack = shift(pack, "yh", 1)
    one = struct((SPAN, 128))
    own = []
    for k in range(SEQS):
        own.append(
            call(
                (span_own_0, span_own_1)[k],
                (one, one, one),
                [u, b, u0, b0, l, cr, zr, halo, c_conv],
                [
                    pltpu.VMEM((SPAN, 128), bf16),
                    pltpu.VMEM((PIECES, 128, 128), bf16),
                    pltpu.VMEM((SPAN, 512), f32),
                ],
                us=2,
            )
        )
    total, before, l_before = call(
        combine_y,
        (struct((SEQS, 144, 128)), state, struct((SEQS, 8, 128), f32)),
        [pack, near_pack],
    )
    packs = [shift(total, "z", d) for d in (1, 2, 3)]
    (gated,) = call(
        finish,
        (struct((PIECES, SEQS, PIECE, 128)),),
        [*packs, before, l_before, *own[0], *own[1], out_gain[None]],
    )
    back = exchange(gated, GROUP)
    (out,) = call(project_out, (struct((256, 1024)),), [back, w_out])
    return out.reshape(2 * SEQS, PIECE, 1024)


def solution(mesh):
    torus = Mesh(mesh.devices.reshape(4, 2, 2, 4, 2), AXES)
    return jax.shard_map(
        local,
        mesh=torus,
        in_specs=(
            P(None, AXES, None),
            P(),
            P(SP, TP),
            P(SP, TP),
            P(SP, TP),
            P(SP, TP),
            P(SP, TP),
            P(None, TP),
            P(None, TP),
            P(None, TP),
            P(TP),
            P(TP),
            P(TP),
            P(TP, SP),
        ),
        out_specs=P(None, AXES, None),
        check_vma=False,
    )
```

```python
import jax
import jax.numpy as jnp
from jax import lax
from jax.experimental import pallas as pl
from jax.experimental.pallas import tpu as pltpu
from jax.sharding import Mesh
from jax.sharding import PartitionSpec as P


LENGTH = 8192
HEAD_P = 64
SEQS = 2
SPAN = 1024
PIECE = 64
PIECES = 16
T = 64
HALO = 16
EPS = 1e-05
AXES = ("z", "yh", "yl", "x", "c")
SP = ("z", "yh", "yl")
TP = ("x", "c")
LINE = ("z", "yh")
GROUP = ("yl", "x", "c")
bf16 = jnp.bfloat16
f32 = jnp.float32
VM = pl.BlockSpec(memory_space=pltpu.VMEM)
SM = pl.BlockSpec(memory_space=pltpu.SMEM)


HB = pl.BlockSpec(memory_space=pltpu.HBM)
DMA = pltpu.SemaphoreType.DMA


def call(body, outs, ins, scratch=(), mib=16, us=2, scalars=0, hbm=()):
    ins = [pltpu.with_memory_space_constraint(v, pltpu.HBM) if k in hbm else v for k, v in enumerate(ins)]
    return pl.pallas_call(
        body,
        out_shape=outs,
        in_specs=[SM if k < scalars else HB if k in hbm else VM for k in range(len(ins))],
        out_specs=tuple(VM if isinstance(o, jax.ShapeDtypeStruct) else HB for o in outs),
        scratch_shapes=list(scratch),
        compiler_params=pltpu.CompilerParams(vmem_limit_bytes=mib * 1024 * 1024),
        cost_estimate=pl.CostEstimate(
            flops=us * 1000000000, bytes_accessed=1 << 20, transcendentals=0
        ),
    )(*ins)


def fetch(pairs, sems):
    moves = [pltpu.make_async_copy(a, b, sems.at[k]) for k, (a, b) in enumerate(pairs)]
    for m in moves:
        m.start()
    return moves


def place():
    return [lax.axis_index(a) for a in AXES]


def shift(value, axis, d):
    n = lax.axis_size(axis)
    return lax.ppermute(value, axis, [(i, (i + d) % n) for i in range(n)])


def exchange(value, axes):
    return lax.all_to_all(value, axes, 0, 0, tiled=True)


def silu(v):
    h = 0.5 * v
    return h + h * jnp.tanh(h)


def softplus(v):
    return jnp.maximum(v, 0.0) + jnp.log1p(jnp.exp(-jnp.abs(v)))


def dot(a, b, dims=((1,), (0,))):
    return lax.dot_general(a, b, (dims, ((), ())), preferred_element_type=f32)


def prepare(*refs):
    ins, w_out, held, sems = refs[:7], refs[7], refs[8:15], refs[15]
    moves = fetch(list(zip(ins, held)), sems)
    for m in moves:
        m.wait()
    xw, bw, cw, zw, dw, gain, ow = held
    z, yh, yl, _, _ = place()
    sp = z * 4 + yh * 2 + yl
    row = gain[pl.ds(lax.div(sp, 2), 1), :]
    first = lax.rem(sp, 2) == 0
    row = jnp.where(first, row[:, 0:64], row[:, 64:128])
    row = jnp.concatenate([row, row], axis=1)
    g = jnp.broadcast_to(row, (128, 128)).T[0:64]
    dt = dw[...].astype(f32)
    dt = jnp.concatenate([dt[0:1], dt[1:2]], axis=1) * row
    dt = jnp.broadcast_to(dt, (8, 128)).astype(bf16)
    ws = [(v[...].astype(f32) * g).astype(bf16) for v in (xw, bw, cw, zw)]
    o = ow[...]
    for j in range(4):
        w_out[0:64, 128 * j : 128 * j + 128] = ws[j]
    w_out[64:72, 0:128] = dt
    w_out[64:72, 128:512] = jnp.zeros((8, 384), bf16)
    for j in range(4):
        w_out[72:88, 128 * j : 128 * j + 128] = o[16 * j : 16 * j + 16]


def gather_y(p0, p1, p2, p3, out):
    _, yh, yl, _, _ = place()
    for d, p in enumerate((p0, p1, p2, p3)):
        out[lax.rem(2 * yh + yl - d + 4, 4)] = p[...]


def order_in(p0, p1, p3, p2a, p2b, w, steps, o_out):
    z = lax.axis_index("z")
    for d in range(4):
        parts = [(p0, k) for k in range(4)]
        if d > 0:
            whole = {1: p1, 3: p3}.get(d)
            parts = [(whole, k) for k in range(4)] if whole is not None else [(p2a, 0), (p2a, 1), (p2b, 0), (p2b, 1)]
        first = lax.rem(z - d + 4, 4) * 256
        for k, (p, j) in enumerate(parts):
            at = pl.multiple_of(first + 64 * k, 64)
            w[pl.ds(at, 64), :] = p[j, 0:64, :]
            for n in range(4):
                o_out[pl.ds(at + 16 * n, 16), :] = p[j, 72:88, 128 * n : 128 * n + 128]
        at = pl.ds(pl.multiple_of(first, 256), 256)
        rows = [p[j, 64:72, 0:128].astype(f32)[0:1] for p, j in parts]
        for h in range(2):
            row = jnp.concatenate([v[:, 64 * h : 64 * h + 64] for v in rows], axis=1)
            steps[16 * h : 16 * h + 16, at] = jnp.broadcast_to(row, (16, 256)).astype(bf16)


def slots():
    _, _, yl, x, c = place()
    return [
        (half * 4 + lax.rem(x - d + 4, 4)) * 2 + core
        for core in (c, 1 - c)
        for half, d in ((yl, 0), (yl, 1), (yl, 3), (1 - yl, 0), (1 - yl, 1), (1 - yl, 3), (yl, 2), (1 - yl, 2))
    ]


def columns(d):
    return pl.ds(pl.multiple_of(lax.rem(lax.axis_index("z") - d + 4, 4) * 256, 256), 256)


def project_part(*refs):
    groups, parts, out, scale = (refs[:8], refs[8:16]), refs[16:19], refs[19], refs[20]
    for g, pieces in enumerate(groups):
        total = None
        for d, p in zip((0, 1, 3), parts):
            at = columns(d)
            rows = jnp.concatenate([v[:, :, at].reshape(SEQS * PIECE, 256) for v in pieces], axis=0)
            more = dot(rows, jnp.concatenate([p[k, 0:64, :] for k in range(4)], axis=0))
            total = more if total is None else total + more
        out[g] = total
        wide = jnp.concatenate([v[...].reshape(SEQS * PIECE, 1024) for v in pieces], axis=0).astype(f32)
        r = lax.rsqrt(jnp.mean(wide * wide, axis=1, keepdims=True) + EPS)
        scale[g] = jnp.broadcast_to(r, (1024, 128))


def project_tail(*refs):
    pieces, w, tail, rows = refs[:16], refs[16], refs[17], refs[18]
    for slot, piece in zip(slots(), pieces):

        @pl.when(slot == PIECES - 1)
        def _(piece=piece):
            rows[...] = piece[:, PIECE - HALO :, :]

    v = rows[...].reshape(SEQS * HALO, 1024)
    wide = v.astype(f32)
    r = lax.rsqrt(jnp.mean(wide * wide, axis=1, keepdims=True) + EPS)
    tail[...] = (dot(v, w[:, 0:384]) * r).astype(bf16).reshape(SEQS, HALO, 384)


def project_all(*refs):
    here, there, (w, steps, begun, scale) = refs[:8], refs[8:16], refs[16:20]
    xb, cr, zr, dt_out, x0 = refs[20:]
    places = slots()
    lane = lax.broadcasted_iota(jnp.int32, (128, 128), 1)
    for k in range(2):
        pieces = [v[...] for v in (here, there)[k]]
        rows = jnp.concatenate([p.reshape(SEQS * PIECE, 1024) for p in pieces], axis=0)
        wide = rows.astype(f32)
        r = scale[k]
        at = columns(2)
        last = [v[:, :, at].reshape(SEQS * PIECE, 256) for v in (here, there)[k]]
        part = begun[k] + dot(jnp.concatenate(last, axis=0), w[at, :])
        part = part * jnp.concatenate([r] * 4, axis=1)
        part = part.astype(bf16).reshape(8, SEQS, PIECE, 512)
        d0, d1 = (
            jnp.sum(wide * jnp.concatenate([steps[16 * h : 16 * h + 16, :]] * 64, axis=0).astype(f32), axis=1, keepdims=True)
            for h in range(2)
        )
        for j in range(8):
            slot = places[8 * k + j]
            at = pl.ds(pl.multiple_of(slot * PIECE, PIECE), PIECE)
            for s in range(SEQS):
                for ref, lo, n in ((xb, 0, 256), (cr, 256, 128), (zr, 384, 128)):
                    ref[s, at, :] = part[j, s, :, lo : lo + n]
            one = slice(128 * j, 128 * j + 128)
            turned = (jnp.where(lane < 64, d0[one], d1[one]) * r[one]).T
            both = jnp.concatenate([turned[0:1], turned[64:65]], axis=0)
            for s in range(SEQS):
                dt_out[s, slot] = both[:, 64 * s : 64 * s + 64]
    x0[...] = xb[:, 0:T, :]


def entering(halo, s, lane, end):
    z, yh, _, _, _ = place()
    v = halo[s, :, lane:end].astype(f32)
    return jnp.where(2 * z + yh == 0, jnp.zeros_like(v), v)


def convolve(rows, taps):
    part = (0.5 * taps[0:1, :]) * rows
    for k in range(1, 4):
        part = (0.5 * taps[k : k + 1, :]) * rows + pltpu.roll(part, 1, 0)
    half = part[HALO:]
    return half + half * jnp.tanh(half)


def halves(v):
    hi = v.astype(bf16)
    return [hi, (v - hi.astype(f32)).astype(bf16)]


def spread(rows, groups):
    count = max(groups) + 1
    source = lax.broadcasted_iota(jnp.int32, (8 * len(rows), 128 * count), 0)
    lane = lax.broadcasted_iota(jnp.int32, (8 * len(rows), 128 * count), 1)
    hit = None
    for k, g in enumerate(groups):
        want = lane // HEAD_P - 2 * g + 8 * k
        mine = jnp.logical_and(lane // 128 == g, source == want)
        hit = mine if hit is None else jnp.logical_or(hit, mine)
    return dot(jnp.concatenate(rows, axis=0), hit.astype(f32).astype(bf16), ((0,), (0,)))


def offsets(lines):
    total, ahead = jnp.zeros((8, 1), f32), []
    for k in range(SPAN // T):
        ahead.append(total)
        end = (k % 2) * T + T - 1
        total = total + lines[8 * (k // 2) : 8 * (k // 2) + 8, end : end + 1]
    return ahead, total


def absolute(lines, ahead):
    first = lax.broadcasted_iota(jnp.int32, (8, 128), 1) < T
    parts = []
    for b in range(SPAN // 128):
        parts.append(lines[8 * b : 8 * b + 8] + jnp.where(first, ahead[2 * b], ahead[2 * b + 1]))
    return jnp.concatenate(parts, axis=0)


def span_state(
    bias, rates, xb, raw, x_taps, b_taps, u_v, b_v, l_out, d_out, t_out, s_out, late_v, wide
):
    row = lax.rem(lax.broadcasted_iota(jnp.int32, (64, 1), 0), 8)
    dtb = jnp.where(row == 0, bias[0], jnp.where(row == 1, bias[1], 0.0))
    rate = jnp.where(row == 0, rates[0], jnp.where(row == 1, rates[1], 0.0))
    row = lax.broadcasted_iota(jnp.int32, (128, 128), 0)
    col = lax.broadcasted_iota(jnp.int32, (128, 128), 1)
    sums = jnp.logical_and(row <= col, row // T == col // T).astype(f32).astype(bf16)
    none = jnp.zeros((6, 128), f32)
    for s in range(SEQS):
        steps = []
        for b in range(SPAN // 128):
            steps += [jnp.concatenate([raw[s, 2 * b], raw[s, 2 * b + 1]], axis=1), none]
        dt = softplus(jnp.concatenate(steps, axis=0) + dtb)
        ld = -(dt * rate) / LENGTH
        both = dot(jnp.concatenate(halves(ld), axis=0), sums)
        lines = both[0:64] + both[64:128]
        l_out[s] = lines
        ahead, total = offsets(lines)
        total_all = jnp.concatenate([total] * 8, axis=0)
        late = dt * jnp.exp(total_all - absolute(lines, ahead))
        rows = halves(dt) + halves(late)
        for b in range(SPAN // 128):
            block = [v[8 * b : 8 * b + 8] for v in rows]
            wide[128 * b : 128 * b + 128, :] = spread(block, (0, 0, 1, 1))
        d_out[s] = wide[0:T]
        head = lax.broadcasted_iota(jnp.int32, (1, 128), 1) < HEAD_P
        t_out[s] = jnp.broadcast_to(jnp.where(head, total[0:1], total[1:2]), (8, 128))
        for first in range(T, SPAN, 128):
            last = min(first + 128, SPAN)
            rows = xb[s, first - HALO : last, :].astype(f32)
            x = convolve(rows[:, 0:128], x_taps)
            u_v[s, first:last, :] = (x * wide[first:last, 0:128]).astype(bf16)
            late_v[first:last, :] = (x * wide[first:last, 128:256]).astype(bf16)
            b_v[s, first:last, :] = convolve(rows[:, 128:256], b_taps).astype(bf16)
        s_out[s] = dot(b_v[s, T:, :], late_v[T:, :], ((0,), (0,)))


def two_parts(row):
    high = row.astype(bf16).astype(f32)
    which = lax.broadcasted_iota(jnp.int32, (16, 128), 0)
    return jnp.where(which == 0, high, jnp.where(which == 1, row - high, 0.0)).astype(bf16)


def log_of(pack, s):
    return pack[s, 128:129, :].astype(f32) + pack[s, 129:130, :].astype(f32)


def span_first(x0, halo, x_taps, b_taps, dt, totals, part, u_out, b_out, pack):
    for s in range(SEQS):
        rows = jnp.concatenate([entering(halo, s, 0, 256), x0[s].astype(f32)], axis=0)
        total = totals[s, 0:1, :]
        x = convolve(rows[:, 0:128], x_taps)
        b = convolve(rows[:, 128:256], b_taps).astype(bf16)
        u_out[s] = (x * dt[s, :, 0:128]).astype(bf16)
        b_out[s] = b
        late = (x * dt[s, :, 128:256]).astype(bf16)
        state = (part[s] + dot(b, late, ((0,), (0,)))).astype(bf16)
        pack[s, 0:128, :] = state
        pack[s, 128:144, :] = two_parts(total)


def span_own(s, u, b, u0, b0, l, cr, zr, halo, taps, y_out, c_out, e_out, mv, sv, wide):
    row = lax.broadcasted_iota(jnp.int32, (T, 128), 0)
    col = lax.rem(lax.broadcasted_iota(jnp.int32, (T, 128), 1), T)
    seen = col <= row
    left = lax.broadcasted_iota(jnp.int32, (T, 128), 1) < T
    first = lax.broadcasted_iota(jnp.int32, (8, 128), 1) < T
    lines = l[s]
    ahead, _ = offsets(lines)
    past = absolute(lines, ahead)
    for k in range(SPAN // 128):
        v = lines[8 * k : 8 * k + 8]
        rest = jnp.where(first, v[:, T - 1 : T], v[:, 2 * T - 1 : 2 * T]) - v
        rows = halves(v)
        rows += [jnp.exp(r).astype(bf16) for r in (v, rest, past[8 * k : 8 * k + 8])]
        wide[128 * k : 128 * k + 128, :] = spread(rows, (0, 0, 1, 2, 3))
    for k in range(0, SPAN, 128):
        if k == 0:
            rows = jnp.concatenate([entering(halo, s, 256, 384), cr[s, 0:128, :].astype(f32)], axis=0)
        else:
            rows = cr[s, k - HALO : k + 128, :].astype(f32)
        c_out[k : k + 128, :] = convolve(rows, taps).astype(bf16)
    chunks = [(k, slice(k * T, k * T + T)) for k in range(SPAN // T)]

    def rows_of(start, later, k, at):
        return start[s] if k == 0 else later[s, at, :]

    for k, at in chunks:
        bc = rows_of(b0, b, k, at)
        half = slice((k % 2) * T, (k % 2) * T + T)
        at_8 = 8 * (k // 2)
        l_row = jnp.concatenate([l[s, at_8 : at_8 + 1, half], l[s, at_8 + 1 : at_8 + 2, half]], axis=1)
        pairs = dot(c_out[at, :], jnp.concatenate([bc, bc], axis=0), ((1,), (1,)))
        gap = jnp.exp(jnp.where(seen, wide[at, 0:128] - l_row, -jnp.inf))
        mv[at, :] = (pairs * gap).astype(bf16)
    state = jnp.zeros((128, 128), f32)
    for k, at in chunks[:-1]:
        late = (rows_of(u0, u, k, at).astype(f32) * wide[at, 256:384]).astype(bf16)
        fresh = dot(rows_of(b0, b, k, at), late, ((0,), (0,)))
        state = state * wide[k * T + T - 1 : k * T + T, 128:256] + fresh
        sv[k + 1] = state.astype(bf16)
    for k, at in chunks:
        uc = rows_of(u0, u, k, at)
        zero = jnp.zeros_like(uc)
        blocks = jnp.concatenate([jnp.where(left, uc, zero), jnp.where(left, zero, uc)], axis=0)
        y = dot(mv[at, :], blocks)
        if k > 0:
            y = y + dot(c_out[at, :], sv[k]) * wide[at, 128:256]
        gate = silu(zr[s, at, :].astype(f32))
        e_out[at, :] = (gate * wide[at, 384:512]).astype(bf16)
        y_out[at, :] = (y * gate).astype(bf16)


def span_own_0(*refs):
    span_own(0, *refs)


def span_own_1(*refs):
    span_own(1, *refs)


def combine_y(mine, other, total, before, l_before):
    late = lax.axis_index("yh") == 1
    for s in range(SEQS):
        log_0, log_1 = log_of(mine, s), log_of(other, s)
        state_0, state_1 = mine[s, 0:128, :].astype(f32), other[s, 0:128, :].astype(f32)
        ahead = state_0 * jnp.exp(log_1) + state_1
        behind = state_1 * jnp.exp(log_0) + state_0
        total[s, 0:128, :] = jnp.where(late, behind, ahead).astype(bf16)
        total[s, 128:144, :] = two_parts(log_0 + log_1)
        before[s] = jnp.where(late, state_1, jnp.zeros_like(state_1))
        l_before[s] = jnp.broadcast_to(jnp.where(late, log_1, jnp.zeros_like(log_1)), (8, 128))


def finish(*refs):
    packs, (before, l_before), own, (gain, out) = refs[:3], refs[3:5], refs[5:11], refs[11:]
    z = lax.axis_index("z")
    for s in range(SEQS):
        y_own, cc, decay = own[3 * s : 3 * s + 3]
        log = l_before[s, 0:1, :]
        state = before[s]
        for d in range(1, 4):
            past = packs[d - 1][s, 0:128, :].astype(f32)
            state = state + jnp.where(d <= z, past * jnp.exp(log), jnp.zeros_like(past))
            log = log + log_of(packs[d - 1], s)
        g = y_own[...].astype(f32) + dot(cc[...], state.astype(bf16)) * decay[...].astype(f32)
        g = g * lax.rsqrt(jnp.mean(g * g, axis=1, keepdims=True) + EPS) * gain[...]
        g = g.astype(bf16)
        for k in range(PIECES):
            out[k, s] = g[k * PIECE : k * PIECE + PIECE, :]


def order_out(*refs):
    ins, out, held, sems = refs[:8], refs[8], refs[9], refs[10]
    moves = fetch([(r, held.at[k]) for k, r in enumerate(ins)], sems)
    _, _, _, x, c = place()
    for core in range(2):
        half = lax.rem(c + core, 2)
        for d in range(4):
            at = pl.multiple_of((2 * lax.rem(x - d + 4, 4) + half) * 128, 128)
            moves[4 * core + d].wait()
            out[pl.ds(at, 128), :] = held[4 * core + d].astype(f32).T.astype(bf16)


def project_out(g, w, out):
    for k in range(2):
        rows = jnp.concatenate([g[8 * k + j].reshape(SEQS * PIECE, 128) for j in range(8)], axis=1)
        out[128 * k : 128 * k + 128, :] = dot(rows, w[...]).astype(bf16)


def struct(shape, kind=bf16):
    return jax.ShapeDtypeStruct(shape, kind)


def local(
    tokens,
    norm_gain,
    x_weight,
    z_weight,
    b_weight,
    c_weight,
    dt_weight,
    x_conv,
    b_conv,
    c_conv,
    dt_bias,
    decay_rate,
    out_gain,
    out_weight,
):
    even = lax.axis_index("yl") == 0
    keep = jnp.where(even, tokens[0:2], tokens[2:4])
    give = jnp.where(even, tokens[2:4], tokens[0:2])
    got = shift(give, "yl", 1)
    left_a = shift(keep, "x", 1)
    right_a = shift(keep, "x", -1)
    left_b = shift(got, "x", 1)
    right_b = shift(got, "x", -1)
    far_a = shift(left_a, "x", 1)
    far_b = shift(right_b, "x", -1)
    here = (keep, left_a, right_a, got, left_b, right_b, far_a, far_b)
    there = tuple(shift(v, "c", 1) for v in here)

    weights = [x_weight, b_weight, c_weight, z_weight]
    weights = weights + [dt_weight.T, norm_gain.reshape(8, 128), out_weight.T]
    (w_own,) = call(
        prepare,
        (struct((88, 512)),),
        weights,
        [pltpu.VMEM(w.shape, w.dtype) for w in weights] + [DMA((7,))],
        hbm=range(7),
    )
    y_parts = [w_own] + [shift(w_own, ("yh", "yl"), d) for d in (1, 2, 3)]
    (w_line,) = call(gather_y, (struct((4, 88, 512)),), y_parts)
    w_back = shift(w_line, "z", 1)
    w_front = shift(w_line, "z", -1)
    w_far_a = shift(w_back[0:2], "z", 1)
    w_far_b = shift(w_front[2:4], "z", -1)
    w_in, steps, o_here = call(
        order_in,
        (struct((1024, 512)), struct((32, 1024)), struct((1024, 128))),
        [w_line, w_back, w_front, w_far_a, w_far_b],
    )

    half = struct((SEQS, SPAN, 128))
    first = struct((SEQS, T, 128))
    state = struct((SEQS, 128, 128), f32)
    far_s = pltpu.HBM(half.shape, bf16)
    lines = struct((SEQS, 64, 128), f32)
    totals_s = struct((SEQS, 8, 128), f32)
    first_s = struct((SEQS, T, 256), f32)
    begun, scale = call(
        project_part,
        (struct((2, 1024, 512), f32), struct((2, 1024, 128), f32)),
        [*here, *there, w_line, w_back, w_front],
        us=2,
    )
    (tail,) = call(
        project_tail,
        (struct((SEQS, HALO, 384)),),
        [*here, *there, w_in],
        [pltpu.VMEM((SEQS, HALO, 1024), bf16)],
        us=1,
    )
    halo = shift(tail, LINE, 1)
    xb, cr, zr, raw, x0 = call(
        project_all,
        (
            struct((SEQS, SPAN, 256)),
            half,
            half,
            struct((SEQS, PIECES, 2, PIECE), f32),
            struct((SEQS, T, 256)),
        ),
        [*here, *there, w_in, steps, begun, scale],
        us=5,
    )
    outs = [o_here] + [shift(o_here, "x", d) for d in (1, 2, 3)]
    outs = outs + [shift(v, "c", 1) for v in outs]
    (w_out,) = call(
        order_out,
        (struct((1024, 1024)),),
        outs,
        [pltpu.VMEM((8, 1024, 128), bf16), DMA((8,))],
        hbm=range(8),
    )
    u, b, l, dt0, totals, part = call(
        span_state,
        (half, half, lines, first_s, totals_s, state),
        [dt_bias, decay_rate, xb, raw, x_conv, b_conv],
        [pltpu.VMEM((SPAN, 128), bf16), pltpu.VMEM((SPAN, 256), f32)],
        us=4,
        scalars=2,
    )
    u0, b0, pack = call(
        span_first,
        (first, first, struct((SEQS, 144, 128))),
        [x0, halo, x_conv, b_conv, dt0, totals, part],
    )
    near_pack = shift(pack, "yh", 1)
    one = struct((SPAN, 128))
    own = []
    for k in range(SEQS):
        own.append(
            call(
                (span_own_0, span_own_1)[k],
                (one, one, one),
                [u, b, u0, b0, l, cr, zr, halo, c_conv],
                [
                    pltpu.VMEM((SPAN, 128), bf16),
                    pltpu.VMEM((PIECES, 128, 128), bf16),
                    pltpu.VMEM((SPAN, 512), f32),
                ],
                us=2,
            )
        )
    total, before, l_before = call(
        combine_y,
        (struct((SEQS, 144, 128)), state, struct((SEQS, 8, 128), f32)),
        [pack, near_pack],
    )
    packs = [shift(total, "z", d) for d in (1, 2, 3)]
    (gated,) = call(
        finish,
        (struct((PIECES, SEQS, PIECE, 128)),),
        [*packs, before, l_before, *own[0], *own[1], out_gain[None]],
    )
    back = exchange(gated, GROUP)
    (out,) = call(project_out, (struct((256, 1024)),), [back, w_out])
    return out.reshape(2 * SEQS, PIECE, 1024)


def solution(mesh):
    torus = Mesh(mesh.devices.reshape(4, 2, 2, 4, 2), AXES)
    return jax.shard_map(
        local,
        mesh=torus,
        in_specs=(
            P(None, AXES, None),
            P(),
            P(SP, TP),
            P(SP, TP),
            P(SP, TP),
            P(SP, TP),
            P(SP, TP),
            P(None, TP),
            P(None, TP),
            P(None, TP),
            P(TP),
            P(TP),
            P(TP),
            P(TP, SP),
        ),
        out_specs=P(None, AXES, None),
        check_vma=False,
    )
```

```python
import jax
import jax.numpy as jnp
from jax import lax
from jax.experimental import pallas as pl
from jax.experimental.pallas import tpu as pltpu
from jax.sharding import Mesh
from jax.sharding import PartitionSpec as P


LENGTH = 8192
HEAD_P = 64
SEQS = 2
SPAN = 1024
PIECE = 64
PIECES = 16
T = 64
HALO = 16
EPS = 1e-05
AXES = ("z", "yh", "yl", "x", "c")
SP = ("z", "yh", "yl")
TP = ("x", "c")
LINE = ("z", "yh")
GROUP = ("yl", "x", "c")
bf16 = jnp.bfloat16
f32 = jnp.float32
VM = pl.BlockSpec(memory_space=pltpu.VMEM)
SM = pl.BlockSpec(memory_space=pltpu.SMEM)


HB = pl.BlockSpec(memory_space=pltpu.HBM)
DMA = pltpu.SemaphoreType.DMA


def call(body, outs, ins, scratch=(), mib=16, us=2, scalars=0, hbm=()):
    ins = [pltpu.with_memory_space_constraint(v, pltpu.HBM) if k in hbm else v for k, v in enumerate(ins)]
    return pl.pallas_call(
        body,
        out_shape=outs,
        in_specs=[SM if k < scalars else HB if k in hbm else VM for k in range(len(ins))],
        out_specs=tuple(VM if isinstance(o, jax.ShapeDtypeStruct) else HB for o in outs),
        scratch_shapes=list(scratch),
        compiler_params=pltpu.CompilerParams(vmem_limit_bytes=mib * 1024 * 1024),
        cost_estimate=pl.CostEstimate(
            flops=us * 1000000000, bytes_accessed=1 << 20, transcendentals=0
        ),
    )(*ins)


def fetch(pairs, sems):
    moves = [pltpu.make_async_copy(a, b, sems.at[k]) for k, (a, b) in enumerate(pairs)]
    for m in moves:
        m.start()
    return moves


def place():
    return [lax.axis_index(a) for a in AXES]


def shift(value, axis, d):
    n = lax.axis_size(axis)
    return lax.ppermute(value, axis, [(i, (i + d) % n) for i in range(n)])


def exchange(value, axes):
    return lax.all_to_all(value, axes, 0, 0, tiled=True)


def silu(v):
    h = 0.5 * v
    return h + h * jnp.tanh(h)


def softplus(v):
    return jnp.maximum(v, 0.0) + jnp.log1p(jnp.exp(-jnp.abs(v)))


def dot(a, b, dims=((1,), (0,))):
    return lax.dot_general(a, b, (dims, ((), ())), preferred_element_type=f32)


def prepare(*refs):
    ins, tokens, (w_out, keep, give), held, sems = refs[:7], refs[7], refs[8:11], refs[11:18], refs[18]
    yl = lax.axis_index("yl")
    halves_of = [(tokens.at[pl.ds(2 * yl, 2)], keep), (tokens.at[pl.ds(2 - 2 * yl, 2)], give)]
    stay = fetch(halves_of, sems.at[pl.ds(7, 2)])
    moves = fetch(list(zip(ins, held)), sems.at[pl.ds(0, 7)])
    for m in moves:
        m.wait()
    xw, bw, cw, zw, dw, gain, ow = held
    z, yh, yl, _, _ = place()
    sp = z * 4 + yh * 2 + yl
    row = gain[pl.ds(lax.div(sp, 2), 1), :]
    first = lax.rem(sp, 2) == 0
    row = jnp.where(first, row[:, 0:64], row[:, 64:128])
    row = jnp.concatenate([row, row], axis=1)
    g = jnp.broadcast_to(row, (128, 128)).T[0:64]
    dt = dw[...].astype(f32)
    dt = jnp.concatenate([dt[0:1], dt[1:2]], axis=1) * row
    dt = jnp.broadcast_to(dt, (8, 128)).astype(bf16)
    ws = [(v[...].astype(f32) * g).astype(bf16) for v in (xw, bw, cw, zw)]
    o = ow[...]
    for j in range(4):
        w_out[0:64, 128 * j : 128 * j + 128] = ws[j]
    w_out[64:72, 0:128] = dt
    w_out[64:72, 128:512] = jnp.zeros((8, 384), bf16)
    for j in range(4):
        w_out[72:88, 128 * j : 128 * j + 128] = o[16 * j : 16 * j + 16]
    for m in stay:
        m.wait()


def gather_y(p0, p1, p2, p3, out):
    _, yh, yl, _, _ = place()
    for d, p in enumerate((p0, p1, p2, p3)):
        out[lax.rem(2 * yh + yl - d + 4, 4)] = p[...]


def order_in(p0, p1, p3, p2a, p2b, w, steps, o_out):
    z = lax.axis_index("z")
    for d in range(4):
        parts = [(p0, k) for k in range(4)]
        if d > 0:
            whole = {1: p1, 3: p3}.get(d)
            parts = [(whole, k) for k in range(4)] if whole is not None else [(p2a, 0), (p2a, 1), (p2b, 0), (p2b, 1)]
        first = lax.rem(z - d + 4, 4) * 256
        for k, (p, j) in enumerate(parts):
            at = pl.multiple_of(first + 64 * k, 64)
            w[pl.ds(at, 64), :] = p[j, 0:64, :]
            for n in range(4):
                o_out[pl.ds(at + 16 * n, 16), :] = p[j, 72:88, 128 * n : 128 * n + 128]
        at = pl.ds(pl.multiple_of(first, 256), 256)
        rows = [p[j, 64:72, 0:128].astype(f32)[0:1] for p, j in parts]
        for h in range(2):
            row = jnp.concatenate([v[:, 64 * h : 64 * h + 64] for v in rows], axis=1)
            steps[16 * h : 16 * h + 16, at] = jnp.broadcast_to(row, (16, 256)).astype(bf16)


def slots():
    _, _, yl, x, c = place()
    return [
        (half * 4 + lax.rem(x - d + 4, 4)) * 2 + core
        for core in (c, 1 - c)
        for half, d in ((yl, 0), (yl, 1), (yl, 3), (1 - yl, 0), (1 - yl, 1), (1 - yl, 3), (yl, 2), (1 - yl, 2))
    ]


def columns(d):
    return pl.ds(pl.multiple_of(lax.rem(lax.axis_index("z") - d + 4, 4) * 256, 256), 256)


def project_part(*refs):
    groups, parts, out, scale = (refs[:8], refs[8:16]), refs[16:19], refs[19], refs[20]
    for g, pieces in enumerate(groups):
        total = None
        for d, p in zip((0, 1, 3), parts):
            at = columns(d)
            rows = jnp.concatenate([v[:, :, at].reshape(SEQS * PIECE, 256) for v in pieces], axis=0)
            more = dot(rows, jnp.concatenate([p[k, 0:64, :] for k in range(4)], axis=0))
            total = more if total is None else total + more
        out[g] = total
        wide = jnp.concatenate([v[...].reshape(SEQS * PIECE, 1024) for v in pieces], axis=0).astype(f32)
        r = lax.rsqrt(jnp.mean(wide * wide, axis=1, keepdims=True) + EPS)
        scale[g] = jnp.broadcast_to(r, (1024, 128))


def project_tail(*refs):
    parts, pieces, (w, steps, o_out, tail, rows) = refs[:5], refs[5:21], refs[21:]
    order_in(*parts, w, steps, o_out)
    for slot, piece in zip(slots(), pieces):

        @pl.when(slot == PIECES - 1)
        def _(piece=piece):
            rows[...] = piece[:, PIECE - HALO :, :]

    v = rows[...].reshape(SEQS * HALO, 1024)
    wide = v.astype(f32)
    r = lax.rsqrt(jnp.mean(wide * wide, axis=1, keepdims=True) + EPS)
    tail[...] = (dot(v, w[:, 0:384]) * r).astype(bf16).reshape(SEQS, HALO, 384)


def project_all(*refs):
    here, there, (w, steps, begun, scale) = refs[:8], refs[8:16], refs[16:20]
    xb, cr, zr, dt_out, x0 = refs[20:]
    places = slots()
    lane = lax.broadcasted_iota(jnp.int32, (128, 128), 1)
    for k in range(2):
        pieces = [v[...] for v in (here, there)[k]]
        rows = jnp.concatenate([p.reshape(SEQS * PIECE, 1024) for p in pieces], axis=0)
        wide = rows.astype(f32)
        r = scale[k]
        at = columns(2)
        last = [v[:, :, at].reshape(SEQS * PIECE, 256) for v in (here, there)[k]]
        part = begun[k] + dot(jnp.concatenate(last, axis=0), w[at, :])
        part = part * jnp.concatenate([r] * 4, axis=1)
        part = part.astype(bf16).reshape(8, SEQS, PIECE, 512)
        d0, d1 = (
            jnp.sum(wide * jnp.concatenate([steps[16 * h : 16 * h + 16, :]] * 64, axis=0).astype(f32), axis=1, keepdims=True)
            for h in range(2)
        )
        for j in range(8):
            slot = places[8 * k + j]
            at = pl.ds(pl.multiple_of(slot * PIECE, PIECE), PIECE)
            for s in range(SEQS):
                for ref, lo, n in ((xb, 0, 256), (cr, 256, 128), (zr, 384, 128)):
                    ref[s, at, :] = part[j, s, :, lo : lo + n]
            one = slice(128 * j, 128 * j + 128)
            turned = (jnp.where(lane < 64, d0[one], d1[one]) * r[one]).T
            both = jnp.concatenate([turned[0:1], turned[64:65]], axis=0)
            for s in range(SEQS):
                dt_out[s, slot] = both[:, 64 * s : 64 * s + 64]
    x0[...] = xb[:, 0:T, :]


def entering(halo, s, lane, end):
    z, yh, _, _, _ = place()
    v = halo[s, :, lane:end].astype(f32)
    return jnp.where(2 * z + yh == 0, jnp.zeros_like(v), v)


def convolve(rows, taps):
    part = (0.5 * taps[0:1, :]) * rows
    for k in range(1, 4):
        part = (0.5 * taps[k : k + 1, :]) * rows + pltpu.roll(part, 1, 0)
    half = part[HALO:]
    return half + half * jnp.tanh(half)


def halves(v):
    hi = v.astype(bf16)
    return [hi, (v - hi.astype(f32)).astype(bf16)]


def spread(rows, groups):
    count = max(groups) + 1
    source = lax.broadcasted_iota(jnp.int32, (8 * len(rows), 128 * count), 0)
    lane = lax.broadcasted_iota(jnp.int32, (8 * len(rows), 128 * count), 1)
    hit = None
    for k, g in enumerate(groups):
        want = lane // HEAD_P - 2 * g + 8 * k
        mine = jnp.logical_and(lane // 128 == g, source == want)
        hit = mine if hit is None else jnp.logical_or(hit, mine)
    return dot(jnp.concatenate(rows, axis=0), hit.astype(f32).astype(bf16), ((0,), (0,)))


def offsets(lines):
    total, ahead = jnp.zeros((8, 1), f32), []
    for k in range(SPAN // T):
        ahead.append(total)
        end = (k % 2) * T + T - 1
        total = total + lines[8 * (k // 2) : 8 * (k // 2) + 8, end : end + 1]
    return ahead, total


def absolute(lines, ahead):
    first = lax.broadcasted_iota(jnp.int32, (8, 128), 1) < T
    parts = []
    for b in range(SPAN // 128):
        parts.append(lines[8 * b : 8 * b + 8] + jnp.where(first, ahead[2 * b], ahead[2 * b + 1]))
    return jnp.concatenate(parts, axis=0)


def span_state(
    bias, rates, xb, raw, x_taps, b_taps, u_v, b_v, l_out, d_out, t_out, s_out, late_v, wide
):
    row = lax.rem(lax.broadcasted_iota(jnp.int32, (64, 1), 0), 8)
    dtb = jnp.where(row == 0, bias[0], jnp.where(row == 1, bias[1], 0.0))
    rate = jnp.where(row == 0, rates[0], jnp.where(row == 1, rates[1], 0.0))
    row = lax.broadcasted_iota(jnp.int32, (128, 128), 0)
    col = lax.broadcasted_iota(jnp.int32, (128, 128), 1)
    sums = jnp.logical_and(row <= col, row // T == col // T).astype(f32).astype(bf16)
    none = jnp.zeros((6, 128), f32)
    for s in range(SEQS):
        steps = []
        for b in range(SPAN // 128):
            steps += [jnp.concatenate([raw[s, 2 * b], raw[s, 2 * b + 1]], axis=1), none]
        dt = softplus(jnp.concatenate(steps, axis=0) + dtb)
        ld = -(dt * rate) / LENGTH
        both = dot(jnp.concatenate(halves(ld), axis=0), sums)
        lines = both[0:64] + both[64:128]
        l_out[s] = lines
        ahead, total = offsets(lines)
        total_all = jnp.concatenate([total] * 8, axis=0)
        late = dt * jnp.exp(total_all - absolute(lines, ahead))
        rows = halves(dt) + halves(late)
        for b in range(SPAN // 128):
            block = [v[8 * b : 8 * b + 8] for v in rows]
            wide[128 * b : 128 * b + 128, :] = spread(block, (0, 0, 1, 1))
        d_out[s] = wide[0:T]
        head = lax.broadcasted_iota(jnp.int32, (1, 128), 1) < HEAD_P
        t_out[s] = jnp.broadcast_to(jnp.where(head, total[0:1], total[1:2]), (8, 128))
        for first in range(T, SPAN, 128):
            last = min(first + 128, SPAN)
            rows = xb[s, first - HALO : last, :].astype(f32)
            x = convolve(rows[:, 0:128], x_taps)
            u_v[s, first:last, :] = (x * wide[first:last, 0:128]).astype(bf16)
            late_v[first:last, :] = (x * wide[first:last, 128:256]).astype(bf16)
            b_v[s, first:last, :] = convolve(rows[:, 128:256], b_taps).astype(bf16)
        s_out[s] = dot(b_v[s, T:, :], late_v[T:, :], ((0,), (0,)))


def two_parts(row):
    high = row.astype(bf16).astype(f32)
    which = lax.broadcasted_iota(jnp.int32, (16, 128), 0)
    return jnp.where(which == 0, high, jnp.where(which == 1, row - high, 0.0)).astype(bf16)


def log_of(pack, s):
    return pack[s, 128:129, :].astype(f32) + pack[s, 129:130, :].astype(f32)


def span_first(x0, halo, x_taps, b_taps, dt, totals, part, u_out, b_out, pack):
    for s in range(SEQS):
        rows = jnp.concatenate([entering(halo, s, 0, 256), x0[s].astype(f32)], axis=0)
        total = totals[s, 0:1, :]
        x = convolve(rows[:, 0:128], x_taps)
        b = convolve(rows[:, 128:256], b_taps).astype(bf16)
        u_out[s] = (x * dt[s, :, 0:128]).astype(bf16)
        b_out[s] = b
        late = (x * dt[s, :, 128:256]).astype(bf16)
        state = (part[s] + dot(b, late, ((0,), (0,)))).astype(bf16)
        pack[s, 0:128, :] = state
        pack[s, 128:144, :] = two_parts(total)


def span_own(s, u, b, u0, b0, l, cr, zr, halo, taps, y_out, c_out, e_out, mv, sv, wide):
    row = lax.broadcasted_iota(jnp.int32, (T, 128), 0)
    col = lax.rem(lax.broadcasted_iota(jnp.int32, (T, 128), 1), T)
    seen = col <= row
    left = lax.broadcasted_iota(jnp.int32, (T, 128), 1) < T
    first = lax.broadcasted_iota(jnp.int32, (8, 128), 1) < T
    lines = l[s]
    ahead, _ = offsets(lines)
    past = absolute(lines, ahead)
    for k in range(SPAN // 128):
        v = lines[8 * k : 8 * k + 8]
        rest = jnp.where(first, v[:, T - 1 : T], v[:, 2 * T - 1 : 2 * T]) - v
        rows = halves(v)
        rows += [jnp.exp(r).astype(bf16) for r in (v, rest, past[8 * k : 8 * k + 8])]
        wide[128 * k : 128 * k + 128, :] = spread(rows, (0, 0, 1, 2, 3))
    for k in range(0, SPAN, 128):
        if k == 0:
            rows = jnp.concatenate([entering(halo, s, 256, 384), cr[s, 0:128, :].astype(f32)], axis=0)
        else:
            rows = cr[s, k - HALO : k + 128, :].astype(f32)
        c_out[k : k + 128, :] = convolve(rows, taps).astype(bf16)
    chunks = [(k, slice(k * T, k * T + T)) for k in range(SPAN // T)]

    def rows_of(start, later, k, at):
        return start[s] if k == 0 else later[s, at, :]

    for k, at in chunks:
        bc = rows_of(b0, b, k, at)
        half = slice((k % 2) * T, (k % 2) * T + T)
        at_8 = 8 * (k // 2)
        l_row = jnp.concatenate([l[s, at_8 : at_8 + 1, half], l[s, at_8 + 1 : at_8 + 2, half]], axis=1)
        pairs = dot(c_out[at, :], jnp.concatenate([bc, bc], axis=0), ((1,), (1,)))
        gap = jnp.exp(jnp.where(seen, wide[at, 0:128] - l_row, -jnp.inf))
        mv[at, :] = (pairs * gap).astype(bf16)
    state = jnp.zeros((128, 128), f32)
    for k, at in chunks[:-1]:
        late = (rows_of(u0, u, k, at).astype(f32) * wide[at, 256:384]).astype(bf16)
        fresh = dot(rows_of(b0, b, k, at), late, ((0,), (0,)))
        state = state * wide[k * T + T - 1 : k * T + T, 128:256] + fresh
        sv[k + 1] = state.astype(bf16)
    for k, at in chunks:
        uc = rows_of(u0, u, k, at)
        zero = jnp.zeros_like(uc)
        blocks = jnp.concatenate([jnp.where(left, uc, zero), jnp.where(left, zero, uc)], axis=0)
        y = dot(mv[at, :], blocks)
        if k > 0:
            y = y + dot(c_out[at, :], sv[k]) * wide[at, 128:256]
        gate = silu(zr[s, at, :].astype(f32))
        e_out[at, :] = (gate * wide[at, 384:512]).astype(bf16)
        y_out[at, :] = (y * gate).astype(bf16)


def span_own_0(*refs):
    span_own(0, *refs)


def span_own_1(*refs):
    span_own(1, *refs)


def combine_y(mine, other, total, before, l_before):
    late = lax.axis_index("yh") == 1
    for s in range(SEQS):
        log_0, log_1 = log_of(mine, s), log_of(other, s)
        state_0, state_1 = mine[s, 0:128, :].astype(f32), other[s, 0:128, :].astype(f32)
        ahead = state_0 * jnp.exp(log_1) + state_1
        behind = state_1 * jnp.exp(log_0) + state_0
        total[s, 0:128, :] = jnp.where(late, behind, ahead).astype(bf16)
        total[s, 128:144, :] = two_parts(log_0 + log_1)
        before[s] = jnp.where(late, state_1, jnp.zeros_like(state_1))
        l_before[s] = jnp.broadcast_to(jnp.where(late, log_1, jnp.zeros_like(log_1)), (8, 128))


def finish(*refs):
    packs, (before, l_before), own, (gain, out) = refs[:3], refs[3:5], refs[5:11], refs[11:]
    z = lax.axis_index("z")
    for s in range(SEQS):
        y_own, cc, decay = own[3 * s : 3 * s + 3]
        log = l_before[s, 0:1, :]
        state = before[s]
        for d in range(1, 4):
            past = packs[d - 1][s, 0:128, :].astype(f32)
            state = state + jnp.where(d <= z, past * jnp.exp(log), jnp.zeros_like(past))
            log = log + log_of(packs[d - 1], s)
        g = y_own[...].astype(f32) + dot(cc[...], state.astype(bf16)) * decay[...].astype(f32)
        g = g * lax.rsqrt(jnp.mean(g * g, axis=1, keepdims=True) + EPS) * gain[...]
        g = g.astype(bf16)
        for k in range(PIECES):
            out[k, s] = g[k * PIECE : k * PIECE + PIECE, :]


def order_out(*refs):
    ins, out, held, sems = refs[:8], refs[8], refs[9], refs[10]
    moves = fetch([(r, held.at[k]) for k, r in enumerate(ins)], sems)
    _, _, _, x, c = place()
    for core in range(2):
        half = lax.rem(c + core, 2)
        for d in range(4):
            at = pl.multiple_of((2 * lax.rem(x - d + 4, 4) + half) * 128, 128)
            moves[4 * core + d].wait()
            out[pl.ds(at, 128), :] = held[4 * core + d].astype(f32).T.astype(bf16)


def project_out(g, w, out, held, sem):
    away = []
    for k in range(2):
        rows = jnp.concatenate([g[8 * k + j].reshape(SEQS * PIECE, 128) for j in range(8)], axis=1)
        held[128 * k : 128 * k + 128, :] = dot(rows, w[...]).astype(bf16)
        at = pl.ds(128 * k, 128)
        away += fetch([(held.at[at, :], out.at[at, :])], sem.at[pl.ds(k, 1)])
    for m in away:
        m.wait()


def struct(shape, kind=bf16):
    return jax.ShapeDtypeStruct(shape, kind)


def local(
    tokens,
    norm_gain,
    x_weight,
    z_weight,
    b_weight,
    c_weight,
    dt_weight,
    x_conv,
    b_conv,
    c_conv,
    dt_bias,
    decay_rate,
    out_gain,
    out_weight,
):
    weights = [x_weight, b_weight, c_weight, z_weight]
    weights = weights + [dt_weight.T, norm_gain.reshape(8, 128), out_weight.T]
    piece = struct((SEQS, PIECE, 1024))
    w_own, keep, give = call(
        prepare,
        (struct((88, 512)), piece, piece),
        [*weights, tokens],
        [pltpu.VMEM(w.shape, w.dtype) for w in weights] + [DMA((9,))],
        hbm=range(8),
    )
    got = shift(give, "yl", 1)
    left_a = shift(keep, "x", 1)
    right_a = shift(keep, "x", -1)
    left_b = shift(got, "x", 1)
    right_b = shift(got, "x", -1)
    far_a = shift(left_a, "x", 1)
    far_b = shift(right_b, "x", -1)
    here = (keep, left_a, right_a, got, left_b, right_b, far_a, far_b)
    there = tuple(shift(v, "c", 1) for v in here)

    y_parts = [w_own] + [shift(w_own, ("yh", "yl"), d) for d in (1, 2, 3)]
    (w_line,) = call(gather_y, (struct((4, 88, 512)),), y_parts)
    w_back = shift(w_line, "z", 1)
    w_front = shift(w_line, "z", -1)
    w_far_a = shift(w_back[0:2], "z", 1)
    w_far_b = shift(w_front[2:4], "z", -1)
    half = struct((SEQS, SPAN, 128))
    first = struct((SEQS, T, 128))
    state = struct((SEQS, 128, 128), f32)
    far_s = pltpu.HBM(half.shape, bf16)
    lines = struct((SEQS, 64, 128), f32)
    totals_s = struct((SEQS, 8, 128), f32)
    first_s = struct((SEQS, T, 256), f32)
    begun, scale = call(
        project_part,
        (struct((2, 1024, 512), f32), struct((2, 1024, 128), f32)),
        [*here, *there, w_line, w_back, w_front],
        us=2,
    )
    w_in, steps, o_here, tail = call(
        project_tail,
        (
            struct((1024, 512)),
            struct((32, 1024)),
            struct((1024, 128)),
            struct((SEQS, HALO, 384)),
        ),
        [w_line, w_back, w_front, w_far_a, w_far_b, *here, *there],
        [pltpu.VMEM((SEQS, HALO, 1024), bf16)],
        us=1,
    )
    halo = shift(tail, LINE, 1)
    xb, cr, zr, raw, x0 = call(
        project_all,
        (
            struct((SEQS, SPAN, 256)),
            half,
            half,
            struct((SEQS, PIECES, 2, PIECE), f32),
            struct((SEQS, T, 256)),
        ),
        [*here, *there, w_in, steps, begun, scale],
        us=5,
    )
    outs = [o_here] + [shift(o_here, "x", d) for d in (1, 2, 3)]
    outs = outs + [shift(v, "c", 1) for v in outs]
    (w_out,) = call(
        order_out,
        (struct((1024, 1024)),),
        outs,
        [pltpu.VMEM((8, 1024, 128), bf16), DMA((8,))],
        hbm=range(8),
    )
    u, b, l, dt0, totals, part = call(
        span_state,
        (half, half, lines, first_s, totals_s, state),
        [dt_bias, decay_rate, xb, raw, x_conv, b_conv],
        [pltpu.VMEM((SPAN, 128), bf16), pltpu.VMEM((SPAN, 256), f32)],
        us=4,
        scalars=2,
    )
    u0, b0, pack = call(
        span_first,
        (first, first, struct((SEQS, 144, 128))),
        [x0, halo, x_conv, b_conv, dt0, totals, part],
    )
    near_pack = shift(pack, "yh", 1)
    one = struct((SPAN, 128))
    own = []
    for k in range(SEQS):
        own.append(
            call(
                (span_own_0, span_own_1)[k],
                (one, one, one),
                [u, b, u0, b0, l, cr, zr, halo, c_conv],
                [
                    pltpu.VMEM((SPAN, 128), bf16),
                    pltpu.VMEM((PIECES, 128, 128), bf16),
                    pltpu.VMEM((SPAN, 512), f32),
                ],
                us=2,
            )
        )
    total, before, l_before = call(
        combine_y,
        (struct((SEQS, 144, 128)), state, struct((SEQS, 8, 128), f32)),
        [pack, near_pack],
    )
    packs = [shift(total, "z", d) for d in (1, 2, 3)]
    (gated,) = call(
        finish,
        (struct((PIECES, SEQS, PIECE, 128)),),
        [*packs, before, l_before, *own[0], *own[1], out_gain[None]],
    )
    back = exchange(gated, GROUP)
    (out,) = call(
        project_out,
        (pltpu.HBM((256, 1024), bf16),),
        [back, w_out],
        [pltpu.VMEM((256, 1024), bf16), DMA((2,))],
    )
    return out.reshape(2 * SEQS, PIECE, 1024)


def solution(mesh):
    torus = Mesh(mesh.devices.reshape(4, 2, 2, 4, 2), AXES)
    return jax.shard_map(
        local,
        mesh=torus,
        in_specs=(
            P(None, AXES, None),
            P(),
            P(SP, TP),
            P(SP, TP),
            P(SP, TP),
            P(SP, TP),
            P(SP, TP),
            P(None, TP),
            P(None, TP),
            P(None, TP),
            P(TP),
            P(TP),
            P(TP),
            P(TP, SP),
        ),
        out_specs=P(None, AXES, None),
        check_vma=False,
    )
```

```python
import jax
import jax.numpy as jnp
from jax import lax
from jax.experimental import pallas as pl
from jax.experimental.pallas import tpu as pltpu
from jax.sharding import Mesh
from jax.sharding import PartitionSpec as P


LENGTH = 8192
HEAD_P = 64
SEQS = 2
SPAN = 1024
PIECE = 64
PIECES = 16
T = 64
HALO = 16
EPS = 1e-05
AXES = ("z", "yh", "yl", "x", "c")
SP = ("z", "yh", "yl")
TP = ("x", "c")
LINE = ("z", "yh")
GROUP = ("yl", "x", "c")
bf16 = jnp.bfloat16
f32 = jnp.float32
VM = pl.BlockSpec(memory_space=pltpu.VMEM)
SM = pl.BlockSpec(memory_space=pltpu.SMEM)


HB = pl.BlockSpec(memory_space=pltpu.HBM)
DMA = pltpu.SemaphoreType.DMA


def call(body, outs, ins, scratch=(), mib=16, us=2, scalars=0, hbm=()):
    ins = [pltpu.with_memory_space_constraint(v, pltpu.HBM) if k in hbm else v for k, v in enumerate(ins)]
    return pl.pallas_call(
        body,
        out_shape=outs,
        in_specs=[SM if k < scalars else HB if k in hbm else VM for k in range(len(ins))],
        out_specs=tuple(VM if isinstance(o, jax.ShapeDtypeStruct) else HB for o in outs),
        scratch_shapes=list(scratch),
        compiler_params=pltpu.CompilerParams(vmem_limit_bytes=mib * 1024 * 1024),
        cost_estimate=pl.CostEstimate(
            flops=us * 1000000000, bytes_accessed=1 << 20, transcendentals=0
        ),
    )(*ins)


def fetch(pairs, sems):
    moves = [pltpu.make_async_copy(a, b, sems.at[k]) for k, (a, b) in enumerate(pairs)]
    for m in moves:
        m.start()
    return moves


def place():
    return [lax.axis_index(a) for a in AXES]


def shift(value, axis, d):
    n = lax.axis_size(axis)
    return lax.ppermute(value, axis, [(i, (i + d) % n) for i in range(n)])


def exchange(value, axes):
    return lax.all_to_all(value, axes, 0, 0, tiled=True)


def silu(v):
    h = 0.5 * v
    return h + h * jnp.tanh(h)


def softplus(v):
    return jnp.maximum(v, 0.0) + jnp.log1p(jnp.exp(-jnp.abs(v)))


def dot(a, b, dims=((1,), (0,))):
    return lax.dot_general(a, b, (dims, ((), ())), preferred_element_type=f32)


def prepare(*refs):
    ins, tokens, (w_out, keep, give), held, sems = refs[:7], refs[7], refs[8:11], refs[11:18], refs[18]
    yl = lax.axis_index("yl")
    halves_of = [(tokens.at[pl.ds(2 * yl, 2)], keep), (tokens.at[pl.ds(2 - 2 * yl, 2)], give)]
    stay = fetch(halves_of, sems.at[pl.ds(7, 2)])
    moves = fetch(list(zip(ins, held)), sems.at[pl.ds(0, 7)])
    for m in moves:
        m.wait()
    xw, bw, cw, zw, dw, gain, ow = held
    z, yh, yl, _, _ = place()
    sp = z * 4 + yh * 2 + yl
    row = gain[pl.ds(lax.div(sp, 2), 1), :]
    first = lax.rem(sp, 2) == 0
    row = jnp.where(first, row[:, 0:64], row[:, 64:128])
    row = jnp.concatenate([row, row], axis=1)
    g = jnp.broadcast_to(row, (128, 128)).T[0:64]
    dt = dw[...].astype(f32)
    dt = jnp.concatenate([dt[0:1], dt[1:2]], axis=1) * row
    dt = jnp.broadcast_to(dt, (8, 128)).astype(bf16)
    ws = [(v[...].astype(f32) * g).astype(bf16) for v in (xw, bw, cw, zw)]
    o = ow[...]
    for j in range(4):
        w_out[0:64, 128 * j : 128 * j + 128] = ws[j]
    w_out[64:72, 0:128] = dt
    w_out[64:72, 128:512] = jnp.zeros((8, 384), bf16)
    for j in range(4):
        w_out[72:88, 128 * j : 128 * j + 128] = o[16 * j : 16 * j + 16]
    for m in stay:
        m.wait()


def gather_y(p0, p1, p2, p3, out):
    _, yh, yl, _, _ = place()
    for d, p in enumerate((p0, p1, p2, p3)):
        out[lax.rem(2 * yh + yl - d + 4, 4)] = p[...]


def order_in(p0, p1, p3, p2a, p2b, w, steps, o_out):
    z = lax.axis_index("z")
    for d in range(4):
        parts = [(p0, k) for k in range(4)]
        if d > 0:
            whole = {1: p1, 3: p3}.get(d)
            parts = [(whole, k) for k in range(4)] if whole is not None else [(p2a, 0), (p2a, 1), (p2b, 0), (p2b, 1)]
        first = lax.rem(z - d + 4, 4) * 256
        for k, (p, j) in enumerate(parts):
            at = pl.multiple_of(first + 64 * k, 64)
            w[pl.ds(at, 64), :] = p[j, 0:64, :]
            for n in range(4):
                o_out[pl.ds(at + 16 * n, 16), :] = p[j, 72:88, 128 * n : 128 * n + 128]
        at = pl.ds(pl.multiple_of(first, 256), 256)
        rows = [p[j, 64:72, 0:128].astype(f32)[0:1] for p, j in parts]
        for h in range(2):
            row = jnp.concatenate([v[:, 64 * h : 64 * h + 64] for v in rows], axis=1)
            steps[16 * h : 16 * h + 16, at] = jnp.broadcast_to(row, (16, 256)).astype(bf16)


def slots():
    _, _, yl, x, c = place()
    return [
        (half * 4 + lax.rem(x - d + 4, 4)) * 2 + core
        for core in (c, 1 - c)
        for half, d in ((yl, 0), (yl, 1), (yl, 3), (1 - yl, 0), (1 - yl, 1), (1 - yl, 3), (yl, 2), (1 - yl, 2))
    ]


def columns(d):
    return pl.ds(pl.multiple_of(lax.rem(lax.axis_index("z") - d + 4, 4) * 256, 256), 256)


def project_part(*refs):
    groups, parts, out, scale = (refs[:8], refs[8:16]), refs[16:19], refs[19], refs[20]
    for g, pieces in enumerate(groups):
        total = None
        for d, p in zip((0, 1, 3), parts):
            at = columns(d)
            rows = jnp.concatenate([v[:, :, at].reshape(SEQS * PIECE, 256) for v in pieces], axis=0)
            more = dot(rows, jnp.concatenate([p[k, 0:64, :] for k in range(4)], axis=0))
            total = more if total is None else total + more
        out[g] = total
        wide = jnp.concatenate([v[...].reshape(SEQS * PIECE, 1024) for v in pieces], axis=0).astype(f32)
        r = lax.rsqrt(jnp.mean(wide * wide, axis=1, keepdims=True) + EPS)
        scale[g] = jnp.broadcast_to(r, (1024, 128))


def project_tail(*refs):
    pieces, w, tail, rows = refs[:16], refs[16], refs[17], refs[18]
    for slot, piece in zip(slots(), pieces):

        @pl.when(slot == PIECES - 1)
        def _(piece=piece):
            rows[...] = piece[:, PIECE - HALO :, :]

    v = rows[...].reshape(SEQS * HALO, 1024)
    wide = v.astype(f32)
    r = lax.rsqrt(jnp.mean(wide * wide, axis=1, keepdims=True) + EPS)
    tail[...] = (dot(v, w[:, 0:384]) * r).astype(bf16).reshape(SEQS, HALO, 384)


def project_all(*refs):
    here, there, (w, steps, begun, scale) = refs[:8], refs[8:16], refs[16:20]
    xb, cr, zr, dt_out, x0 = refs[20:]
    places = slots()
    lane = lax.broadcasted_iota(jnp.int32, (128, 128), 1)
    for k in range(2):
        pieces = [v[...] for v in (here, there)[k]]
        rows = jnp.concatenate([p.reshape(SEQS * PIECE, 1024) for p in pieces], axis=0)
        wide = rows.astype(f32)
        r = scale[k]
        at = columns(2)
        last = [v[:, :, at].reshape(SEQS * PIECE, 256) for v in (here, there)[k]]
        part = begun[k] + dot(jnp.concatenate(last, axis=0), w[at, :])
        part = part * jnp.concatenate([r] * 4, axis=1)
        part = part.astype(bf16).reshape(8, SEQS, PIECE, 512)
        d0, d1 = (
            jnp.sum(wide * jnp.concatenate([steps[16 * h : 16 * h + 16, :]] * 64, axis=0).astype(f32), axis=1, keepdims=True)
            for h in range(2)
        )
        for j in range(8):
            slot = places[8 * k + j]
            at = pl.ds(pl.multiple_of(slot * PIECE, PIECE), PIECE)
            for s in range(SEQS):
                for ref, lo, n in ((xb, 0, 256), (cr, 256, 128), (zr, 384, 128)):
                    ref[s, at, :] = part[j, s, :, lo : lo + n]
            one = slice(128 * j, 128 * j + 128)
            turned = (jnp.where(lane < 64, d0[one], d1[one]) * r[one]).T
            both = jnp.concatenate([turned[0:1], turned[64:65]], axis=0)
            for s in range(SEQS):
                dt_out[s, slot] = both[:, 64 * s : 64 * s + 64]
    x0[...] = xb[:, 0:T, :]


def entering(halo, s, lane, end):
    z, yh, _, _, _ = place()
    v = halo[s, :, lane:end].astype(f32)
    return jnp.where(2 * z + yh == 0, jnp.zeros_like(v), v)


def convolve(rows, taps):
    part = (0.5 * taps[0:1, :]) * rows
    for k in range(1, 4):
        part = (0.5 * taps[k : k + 1, :]) * rows + pltpu.roll(part, 1, 0)
    half = part[HALO:]
    return half + half * jnp.tanh(half)


def halves(v):
    hi = v.astype(bf16)
    return [hi, (v - hi.astype(f32)).astype(bf16)]


def spread(rows, groups):
    count = max(groups) + 1
    source = lax.broadcasted_iota(jnp.int32, (8 * len(rows), 128 * count), 0)
    lane = lax.broadcasted_iota(jnp.int32, (8 * len(rows), 128 * count), 1)
    hit = None
    for k, g in enumerate(groups):
        want = lane // HEAD_P - 2 * g + 8 * k
        mine = jnp.logical_and(lane // 128 == g, source == want)
        hit = mine if hit is None else jnp.logical_or(hit, mine)
    return dot(jnp.concatenate(rows, axis=0), hit.astype(f32).astype(bf16), ((0,), (0,)))


def offsets(lines):
    total, ahead = jnp.zeros((8, 1), f32), []
    for k in range(SPAN // T):
        ahead.append(total)
        end = (k % 2) * T + T - 1
        total = total + lines[8 * (k // 2) : 8 * (k // 2) + 8, end : end + 1]
    return ahead, total


def absolute(lines, ahead):
    first = lax.broadcasted_iota(jnp.int32, (8, 128), 1) < T
    parts = []
    for b in range(SPAN // 128):
        parts.append(lines[8 * b : 8 * b + 8] + jnp.where(first, ahead[2 * b], ahead[2 * b + 1]))
    return jnp.concatenate(parts, axis=0)


def span_state(
    bias, rates, xb, raw, x_taps, b_taps, u_v, b_v, l_out, d_out, t_out, s_out, late_v, wide
):
    row = lax.rem(lax.broadcasted_iota(jnp.int32, (64, 1), 0), 8)
    dtb = jnp.where(row == 0, bias[0], jnp.where(row == 1, bias[1], 0.0))
    rate = jnp.where(row == 0, rates[0], jnp.where(row == 1, rates[1], 0.0))
    row = lax.broadcasted_iota(jnp.int32, (128, 128), 0)
    col = lax.broadcasted_iota(jnp.int32, (128, 128), 1)
    sums = jnp.logical_and(row <= col, row // T == col // T).astype(f32).astype(bf16)
    none = jnp.zeros((6, 128), f32)
    for s in range(SEQS):
        steps = []
        for b in range(SPAN // 128):
            steps += [jnp.concatenate([raw[s, 2 * b], raw[s, 2 * b + 1]], axis=1), none]
        dt = softplus(jnp.concatenate(steps, axis=0) + dtb)
        ld = -(dt * rate) / LENGTH
        both = dot(jnp.concatenate(halves(ld), axis=0), sums)
        lines = both[0:64] + both[64:128]
        l_out[s] = lines
        ahead, total = offsets(lines)
        total_all = jnp.concatenate([total] * 8, axis=0)
        late = dt * jnp.exp(total_all - absolute(lines, ahead))
        rows = halves(dt) + halves(late)
        for b in range(SPAN // 128):
            block = [v[8 * b : 8 * b + 8] for v in rows]
            wide[128 * b : 128 * b + 128, :] = spread(block, (0, 0, 1, 1))
        d_out[s] = wide[0:T]
        head = lax.broadcasted_iota(jnp.int32, (1, 128), 1) < HEAD_P
        t_out[s] = jnp.broadcast_to(jnp.where(head, total[0:1], total[1:2]), (8, 128))
        for first in range(T, SPAN, 128):
            last = min(first + 128, SPAN)
            rows = xb[s, first - HALO : last, :].astype(f32)
            x = convolve(rows[:, 0:128], x_taps)
            u_v[s, first:last, :] = (x * wide[first:last, 0:128]).astype(bf16)
            late_v[first:last, :] = (x * wide[first:last, 128:256]).astype(bf16)
            b_v[s, first:last, :] = convolve(rows[:, 128:256], b_taps).astype(bf16)
        s_out[s] = dot(b_v[s, T:, :], late_v[T:, :], ((0,), (0,)))


def two_parts(row):
    high = row.astype(bf16).astype(f32)
    which = lax.broadcasted_iota(jnp.int32, (16, 128), 0)
    return jnp.where(which == 0, high, jnp.where(which == 1, row - high, 0.0)).astype(bf16)


def log_of(pack, s):
    return pack[s, 128:129, :].astype(f32) + pack[s, 129:130, :].astype(f32)


def span_first(x0, halo, x_taps, b_taps, dt, totals, part, u_out, b_out, pack):
    for s in range(SEQS):
        rows = jnp.concatenate([entering(halo, s, 0, 256), x0[s].astype(f32)], axis=0)
        total = totals[s, 0:1, :]
        x = convolve(rows[:, 0:128], x_taps)
        b = convolve(rows[:, 128:256], b_taps).astype(bf16)
        u_out[s] = (x * dt[s, :, 0:128]).astype(bf16)
        b_out[s] = b
        late = (x * dt[s, :, 128:256]).astype(bf16)
        state = (part[s] + dot(b, late, ((0,), (0,)))).astype(bf16)
        pack[s, 0:128, :] = state
        pack[s, 128:144, :] = two_parts(total)


def span_own(s, u, b, u0, b0, l, cr, zr, halo, taps, y_out, c_out, e_out, mv, sv, wide):
    row = lax.broadcasted_iota(jnp.int32, (T, 128), 0)
    col = lax.rem(lax.broadcasted_iota(jnp.int32, (T, 128), 1), T)
    seen = col <= row
    left = lax.broadcasted_iota(jnp.int32, (T, 128), 1) < T
    first = lax.broadcasted_iota(jnp.int32, (8, 128), 1) < T
    lines = l[s]
    ahead, _ = offsets(lines)
    past = absolute(lines, ahead)
    for k in range(SPAN // 128):
        v = lines[8 * k : 8 * k + 8]
        rest = jnp.where(first, v[:, T - 1 : T], v[:, 2 * T - 1 : 2 * T]) - v
        rows = halves(v)
        rows += [jnp.exp(r).astype(bf16) for r in (v, rest, past[8 * k : 8 * k + 8])]
        wide[128 * k : 128 * k + 128, :] = spread(rows, (0, 0, 1, 2, 3))
    for k in range(0, SPAN, 128):
        if k == 0:
            rows = jnp.concatenate([entering(halo, s, 256, 384), cr[s, 0:128, :].astype(f32)], axis=0)
        else:
            rows = cr[s, k - HALO : k + 128, :].astype(f32)
        c_out[k : k + 128, :] = convolve(rows, taps).astype(bf16)
    chunks = [(k, slice(k * T, k * T + T)) for k in range(SPAN // T)]

    def rows_of(start, later, k, at):
        return start[s] if k == 0 else later[s, at, :]

    for k, at in chunks:
        bc = rows_of(b0, b, k, at)
        half = slice((k % 2) * T, (k % 2) * T + T)
        at_8 = 8 * (k // 2)
        l_row = jnp.concatenate([l[s, at_8 : at_8 + 1, half], l[s, at_8 + 1 : at_8 + 2, half]], axis=1)
        pairs = dot(c_out[at, :], jnp.concatenate([bc, bc], axis=0), ((1,), (1,)))
        gap = jnp.exp(jnp.where(seen, wide[at, 0:128] - l_row, -jnp.inf))
        mv[at, :] = (pairs * gap).astype(bf16)
    state = jnp.zeros((128, 128), f32)
    for k, at in chunks[:-1]:
        late = (rows_of(u0, u, k, at).astype(f32) * wide[at, 256:384]).astype(bf16)
        fresh = dot(rows_of(b0, b, k, at), late, ((0,), (0,)))
        state = state * wide[k * T + T - 1 : k * T + T, 128:256] + fresh
        sv[k + 1] = state.astype(bf16)
    for k, at in chunks:
        uc = rows_of(u0, u, k, at)
        zero = jnp.zeros_like(uc)
        blocks = jnp.concatenate([jnp.where(left, uc, zero), jnp.where(left, zero, uc)], axis=0)
        y = dot(mv[at, :], blocks)
        if k > 0:
            y = y + dot(c_out[at, :], sv[k]) * wide[at, 128:256]
        gate = silu(zr[s, at, :].astype(f32))
        e_out[at, :] = (gate * wide[at, 384:512]).astype(bf16)
        y_out[at, :] = (y * gate).astype(bf16)


def span_own_0(*refs):
    span_own(0, *refs)


def span_own_1(*refs):
    span_own(1, *refs)


def combine_y(mine, other, total, before, l_before):
    late = lax.axis_index("yh") == 1
    for s in range(SEQS):
        log_0, log_1 = log_of(mine, s), log_of(other, s)
        state_0, state_1 = mine[s, 0:128, :].astype(f32), other[s, 0:128, :].astype(f32)
        ahead = state_0 * jnp.exp(log_1) + state_1
        behind = state_1 * jnp.exp(log_0) + state_0
        total[s, 0:128, :] = jnp.where(late, behind, ahead).astype(bf16)
        total[s, 128:144, :] = two_parts(log_0 + log_1)
        before[s] = jnp.where(late, state_1, jnp.zeros_like(state_1))
        l_before[s] = jnp.broadcast_to(jnp.where(late, log_1, jnp.zeros_like(log_1)), (8, 128))


def finish(*refs):
    packs, (before, l_before), own, (gain, out) = refs[:3], refs[3:5], refs[5:11], refs[11:]
    z = lax.axis_index("z")
    for s in range(SEQS):
        y_own, cc, decay = own[3 * s : 3 * s + 3]
        log = l_before[s, 0:1, :]
        state = before[s]
        for d in range(1, 4):
            past = packs[d - 1][s, 0:128, :].astype(f32)
            state = state + jnp.where(d <= z, past * jnp.exp(log), jnp.zeros_like(past))
            log = log + log_of(packs[d - 1], s)
        g = y_own[...].astype(f32) + dot(cc[...], state.astype(bf16)) * decay[...].astype(f32)
        g = g * lax.rsqrt(jnp.mean(g * g, axis=1, keepdims=True) + EPS) * gain[...]
        g = g.astype(bf16)
        for k in range(PIECES):
            out[k, s] = g[k * PIECE : k * PIECE + PIECE, :]


def order_out(*refs):
    ins, out, held, sems = refs[:8], refs[8], refs[9], refs[10]
    moves = fetch([(r, held.at[k]) for k, r in enumerate(ins)], sems)
    _, _, _, x, c = place()
    for core in range(2):
        half = lax.rem(c + core, 2)
        for d in range(4):
            at = pl.multiple_of((2 * lax.rem(x - d + 4, 4) + half) * 128, 128)
            moves[4 * core + d].wait()
            out[pl.ds(at, 128), :] = held[4 * core + d].astype(f32).T.astype(bf16)


def project_out(g, w, out):
    for k in range(2):
        rows = jnp.concatenate([g[8 * k + j].reshape(SEQS * PIECE, 128) for j in range(8)], axis=1)
        out[128 * k : 128 * k + 128, :] = dot(rows, w[...]).astype(bf16)


def struct(shape, kind=bf16):
    return jax.ShapeDtypeStruct(shape, kind)


def local(
    tokens,
    norm_gain,
    x_weight,
    z_weight,
    b_weight,
    c_weight,
    dt_weight,
    x_conv,
    b_conv,
    c_conv,
    dt_bias,
    decay_rate,
    out_gain,
    out_weight,
):
    weights = [x_weight, b_weight, c_weight, z_weight]
    weights = weights + [dt_weight.T, norm_gain.reshape(8, 128), out_weight.T]
    piece = struct((SEQS, PIECE, 1024))
    w_own, keep, give = call(
        prepare,
        (struct((88, 512)), piece, piece),
        [*weights, tokens],
        [pltpu.VMEM(w.shape, w.dtype) for w in weights] + [DMA((9,))],
        hbm=range(8),
    )
    got = shift(give, "yl", 1)
    left_a = shift(keep, "x", 1)
    right_a = shift(keep, "x", -1)
    left_b = shift(got, "x", 1)
    right_b = shift(got, "x", -1)
    far_a = shift(left_a, "x", 1)
    far_b = shift(right_b, "x", -1)
    here = (keep, left_a, right_a, got, left_b, right_b, far_a, far_b)
    there = tuple(shift(v, "c", 1) for v in here)

    y_parts = [w_own] + [shift(w_own, ("yh", "yl"), d) for d in (1, 2, 3)]
    (w_line,) = call(gather_y, (struct((4, 88, 512)),), y_parts)
    w_back = shift(w_line, "z", 1)
    w_front = shift(w_line, "z", -1)
    w_far_a = shift(w_back[0:2], "z", 1)
    w_far_b = shift(w_front[2:4], "z", -1)
    w_in, steps, o_here = call(
        order_in,
        (struct((1024, 512)), struct((32, 1024)), struct((1024, 128))),
        [w_line, w_back, w_front, w_far_a, w_far_b],
    )

    half = struct((SEQS, SPAN, 128))
    first = struct((SEQS, T, 128))
    state = struct((SEQS, 128, 128), f32)
    far_s = pltpu.HBM(half.shape, bf16)
    lines = struct((SEQS, 64, 128), f32)
    totals_s = struct((SEQS, 8, 128), f32)
    first_s = struct((SEQS, T, 256), f32)
    begun, scale = call(
        project_part,
        (struct((2, 1024, 512), f32), struct((2, 1024, 128), f32)),
        [*here, *there, w_line, w_back, w_front],
        us=2,
    )
    (tail,) = call(
        project_tail,
        (struct((SEQS, HALO, 384)),),
        [*here, *there, w_in],
        [pltpu.VMEM((SEQS, HALO, 1024), bf16)],
        us=1,
    )
    halo = shift(tail, LINE, 1)
    xb, cr, zr, raw, x0 = call(
        project_all,
        (
            struct((SEQS, SPAN, 256)),
            half,
            half,
            struct((SEQS, PIECES, 2, PIECE), f32),
            struct((SEQS, T, 256)),
        ),
        [*here, *there, w_in, steps, begun, scale],
        us=5,
    )
    outs = [o_here] + [shift(o_here, "x", d) for d in (1, 2, 3)]
    outs = outs + [shift(v, "c", 1) for v in outs]
    (w_out,) = call(
        order_out,
        (struct((1024, 1024)),),
        outs,
        [pltpu.VMEM((8, 1024, 128), bf16), DMA((8,))],
        hbm=range(8),
    )
    u, b, l, dt0, totals, part = call(
        span_state,
        (half, half, lines, first_s, totals_s, state),
        [dt_bias, decay_rate, xb, raw, x_conv, b_conv],
        [pltpu.VMEM((SPAN, 128), bf16), pltpu.VMEM((SPAN, 256), f32)],
        us=4,
        scalars=2,
    )
    u0, b0, pack = call(
        span_first,
        (first, first, struct((SEQS, 144, 128))),
        [x0, halo, x_conv, b_conv, dt0, totals, part],
    )
    near_pack = shift(pack, "yh", 1)
    one = struct((SPAN, 128))
    own = []
    for k in range(SEQS):
        own.append(
            call(
                (span_own_0, span_own_1)[k],
                (one, one, one),
                [u, b, u0, b0, l, cr, zr, halo, c_conv],
                [
                    pltpu.VMEM((SPAN, 128), bf16),
                    pltpu.VMEM((PIECES, 128, 128), bf16),
                    pltpu.VMEM((SPAN, 512), f32),
                ],
                us=2,
            )
        )
    total, before, l_before = call(
        combine_y,
        (struct((SEQS, 144, 128)), state, struct((SEQS, 8, 128), f32)),
        [pack, near_pack],
    )
    packs = [shift(total, "z", d) for d in (1, 2, 3)]
    (gated,) = call(
        finish,
        (struct((PIECES, SEQS, PIECE, 128)),),
        [*packs, before, l_before, *own[0], *own[1], out_gain[None]],
    )
    back = exchange(gated, GROUP)
    (out,) = call(project_out, (struct((256, 1024)),), [back, w_out])
    return out.reshape(2 * SEQS, PIECE, 1024)


def solution(mesh):
    torus = Mesh(mesh.devices.reshape(4, 2, 2, 4, 2), AXES)
    return jax.shard_map(
        local,
        mesh=torus,
        in_specs=(
            P(None, AXES, None),
            P(),
            P(SP, TP),
            P(SP, TP),
            P(SP, TP),
            P(SP, TP),
            P(SP, TP),
            P(None, TP),
            P(None, TP),
            P(None, TP),
            P(TP),
            P(TP),
            P(TP),
            P(TP, SP),
        ),
        out_specs=P(None, AXES, None),
        check_vma=False,
    )
```
